32 devices in a mesh: rep: 2 (over x), fs: 8 (over z, y), tp: 2 (over core).
Axes of the slice: x: 2, y: 2, z: 4, core: 2. Of those that a mesh axis runs over, the one named last changes fastest.
Arguments:
- tokens: bfloat16 [16, 512, 2048], P(('rep', 'fs')), may hold values from -6 to 6
- gain_mix_pre: float32 [2048], P('fs'), may hold values from 0.1 to 1.9
- gain_mix_post: float32 [2048], P('fs'), may hold values from 0.1 to 1.9
- gain_mlp_pre: float32 [2048], P('fs'), may hold values from 0.1 to 1.9
- gain_mlp_post: float32 [2048], P('fs'), may hold values from 0.1 to 1.9
- x_weight: float32 [2048, 2048], P('fs', 'tp'), may hold values from -0.125 to 0.125
- gate_weight: float32 [2048, 2048], P('fs', 'tp'), may hold values from -0.125 to 0.125
- x_scale: float32 [2048], P('tp'), may hold values from 0.5 to 2
- gate_scale: float32 [2048], P('tp'), may hold values from 0.5 to 2
- conv_weight: float32 [4, 2048], P(None, 'tp'), may hold values from -3 to 3
- recur_map: bfloat16 [2048, 32], P('tp'), may hold values from -1 to 1
- input_map: bfloat16 [2048, 32], P('tp'), may hold values from -1 to 1
- decay_param: float32 [2048], P('tp'), may hold values from 3.9 to 10
- out_weight: float32 [2048, 2048], P('tp', 'fs'), may hold values from -0.125 to 0.125
- out_scale: float32 [2048], P('fs'), may hold values from 0.5 to 2
- up_weight: float32 [2048, 6144], P('fs', 'tp'), may hold values from -0.125 to 0.125
- up_scale: float32 [6144], P('tp'), may hold values from 0.5 to 2
- down_weight: float32 [6144, 2048], P('tp', 'fs'), may hold values from -0.078125 to 0.078125
- down_scale: float32 [2048], P('fs'), may hold values from 0.5 to 2
Outputs:
- layer_out: bfloat16 [16, 512, 2048], P(('rep', 'fs'), 'tp')
The draws below stay inside these ranges and needn't reach their ends.
All inputs are finite; a program needn't handle non-finite values.
Results may differ from the reference program's by a relative error of at most 0.025.
Values may be sent and summed in bfloat16 or wider, within the bound.
A program may use at most 128 MiB of HBM per device.

```python
import math
import jax
import jax.numpy as jnp
from jax import lax

D = 2048
W = 2048
FF = 6144
BLOCK = 32
CONV = 4
SEQ = 512
SEQS = 16
N_TP = 2


def draw_decay_param(key, part):
    keys = jax.random.split(jax.random.fold_in(key, 11), 2)
    slow_share = 0.5
    chooser = jax.random.uniform(keys[0], (W,), jnp.float32)
    spread = jax.random.uniform(keys[1], (W,), jnp.float32)
    slow_rate = jnp.minimum(jnp.exp(jnp.log(0.05 / SEQ) + spread * jnp.log(10.0)), 0.02)
    fast_rate = jnp.exp(jnp.log(0.004) + spread * jnp.log(5.0))
    rate = jnp.where(chooser < slow_share, slow_rate, fast_rate)
    return (-jnp.log(jnp.expm1(rate))).astype(jnp.float32)


def block_scale(key, shape, shards, low, largest):
    gain, own = 1.0, jax.random.fold_in(key, 6)
    for axis_at, blocks in shards:
        draws = jnp.exp(jax.random.uniform(jax.random.fold_in(own, axis_at), (blocks,), jnp.float32, low / len(shards), largest / len(shards)))
        gain = gain * jnp.repeat(draws, shape[axis_at] // blocks).reshape([-1 if axis == axis_at else 1 for axis in range(len(shape))])
    return gain


def normal_values(stream_key, shape, deviation, bound, cuts=(), dtype=jnp.bfloat16):
    level = block_scale(stream_key, shape, cuts, -0.22, 0.18) if cuts else 1.0
    result = jax.random.normal(stream_key, shape, jnp.float32) * deviation * level
    return jnp.minimum(jnp.maximum(result, -bound), bound).astype(dtype)


def setup_inputs(seed: int = 0) -> dict:
    streams_of = jax.random.split(jax.random.key(seed), 20)
    tokens = normal_values(streams_of[0], (SEQS, SEQ, D), 1.0, 6.0, ((0, 16),))
    gain_mix_pre = jnp.clip(1.0 + 0.18 * jax.random.normal(streams_of[1], (D,), jnp.float32), 0.1, 1.9)
    gain_mix_post = jnp.clip(1.0 + 0.18 * jax.random.normal(streams_of[2], (D,), jnp.float32), 0.1, 1.9)
    gain_mlp_pre = jnp.clip(1.0 + 0.18 * jax.random.normal(streams_of[3], (D,), jnp.float32), 0.1, 1.9)
    gain_mlp_post = jnp.clip(1.0 + 0.18 * jax.random.normal(streams_of[4], (D,), jnp.float32), 0.1, 1.9)
    x_weight = normal_values(streams_of[5], (D, W), D ** -0.5, 0.125, ((0, 8), (1, 2)), jnp.float32)
    gate_weight = normal_values(streams_of[6], (D, W), D ** -0.5, 0.125, ((0, 8), (1, 2)), jnp.float32)
    x_scale = jnp.clip(jnp.exp(math.log(2.0) - 1.3862944 * jax.random.uniform(streams_of[7], (W,), jnp.float32) ** block_scale(streams_of[7], (W,), ((0, 2),), -0.2, 0.2)), 0.5, 2.0)
    gate_scale = jnp.clip(jnp.exp(math.log(2.0) - 1.3862944 * jax.random.uniform(streams_of[8], (W,), jnp.float32) ** block_scale(streams_of[8], (W,), ((0, 2),), -0.2, 0.2)), 0.5, 2.0)
    conv_weight = normal_values(streams_of[9], (CONV, W), 0.5, 3.0, ((1, 2),), jnp.float32)
    recur_map = normal_values(streams_of[10], (W, BLOCK), BLOCK ** -0.5, 1.0, ((0, 2),))
    input_map = normal_values(streams_of[11], (W, BLOCK), BLOCK ** -0.5, 1.0, ((0, 2),))
    decay_param = draw_decay_param(jax.random.fold_in(streams_of[19], 71), 0)
    out_weight = normal_values(streams_of[13], (W, D), W ** -0.5, 0.125, ((0, 2), (1, 8)), jnp.float32)
    out_scale = jnp.clip(jnp.exp(math.log(2.0) - 1.3862944 * jax.random.uniform(streams_of[14], (D,), jnp.float32) ** block_scale(streams_of[14], (D,), ((0, 8),), -0.2, 0.2)), 0.5, 2.0)
    up_weight = normal_values(streams_of[15], (D, FF), D ** -0.5, 0.125, ((0, 8), (1, 2)), jnp.float32)
    up_scale = jnp.clip(jnp.exp(math.log(2.0) - 1.3862944 * jax.random.uniform(streams_of[16], (FF,), jnp.float32) ** block_scale(streams_of[16], (FF,), ((0, 2),), -0.2, 0.2)), 0.5, 2.0)
    down_weight = normal_values(streams_of[17], (FF, D), FF ** -0.5, 0.078125, ((0, 2), (1, 8)), jnp.float32)
    down_scale = jnp.clip(jnp.exp(math.log(2.0) - 1.3862944 * jax.random.uniform(streams_of[18], (D,), jnp.float32) ** block_scale(streams_of[18], (D,), ((0, 8),), -0.2, 0.2)), 0.5, 2.0)
    return dict(tokens=tokens, gain_mix_pre=gain_mix_pre, gain_mix_post=gain_mix_post, gain_mlp_pre=gain_mlp_pre, gain_mlp_post=gain_mlp_post, x_weight=x_weight, gate_weight=gate_weight, x_scale=x_scale, gate_scale=gate_scale, conv_weight=conv_weight, recur_map=recur_map, input_map=input_map, decay_param=decay_param, out_weight=out_weight, out_scale=out_scale, up_weight=up_weight, up_scale=up_scale, down_weight=down_weight, down_scale=down_scale)


EPSILON = 1e-06
DECAY_SCALE = 8.0

def rms_rows(values, gain_vector):
    return values * lax.rsqrt(lax.optimization_barrier(jnp.mean(values * values, axis=-1, keepdims=True)) + EPSILON) * gain_vector

def link_states(earlier, later):
    return (earlier[0] * later[0], later[0] * earlier[1] + later[1])

def reference(tokens, gain_mix_pre, gain_mix_post, gain_mlp_pre, gain_mlp_post, x_weight, gate_weight, x_scale, gate_scale, conv_weight, recur_map, input_map, decay_param, out_weight, out_scale, up_weight, up_scale, down_weight, down_scale):
    x_bf = x_weight.astype(jnp.bfloat16)
    gate_bf = gate_weight.astype(jnp.bfloat16)
    out_bf = out_weight.astype(jnp.bfloat16)
    up_bf = up_weight.astype(jnp.bfloat16)
    down_bf = down_weight.astype(jnp.bfloat16)
    blocks = W // BLOCK
    recur_blocks = recur_map.astype(jnp.float32).reshape(blocks, BLOCK, BLOCK)
    input_blocks = input_map.astype(jnp.float32).reshape(blocks, BLOCK, BLOCK)
    hidden_group = FF // N_TP
    channel_group = W // N_TP

    def one_sequence(seq_tokens):
        resid_in = seq_tokens.astype(jnp.float32)
        normed = rms_rows(resid_in, gain_mix_pre).astype(jnp.bfloat16)
        x_branch = (jnp.dot(normed, x_bf, preferred_element_type=jnp.float32) * x_scale).astype(jnp.bfloat16)
        gate_branch = (jnp.dot(normed, gate_bf, preferred_element_type=jnp.float32) * gate_scale).astype(jnp.bfloat16)
        padded = jnp.concatenate([jnp.zeros((CONV - 1, W), jnp.bfloat16), x_branch], axis=0)
        conv_sum = jnp.zeros((SEQ, W), jnp.float32)
        for tap_index in range(CONV):
            conv_sum = conv_sum + conv_weight[tap_index] * padded[tap_index:tap_index + SEQ].astype(jnp.float32)
        conv_out = lax.optimization_barrier(conv_sum.astype(jnp.bfloat16)).astype(jnp.float32)
        conv_blocks = conv_out.reshape(SEQ, blocks, BLOCK)
        recur_logit = jnp.einsum('tnc,ncd->tnd', conv_blocks, recur_blocks, precision=lax.Precision.HIGHEST).reshape(SEQ, W)
        input_logit = jnp.einsum('tnc,ncd->tnd', conv_blocks, input_blocks, precision=lax.Precision.HIGHEST).reshape(SEQ, W)
        log_decay = -DECAY_SCALE * jax.nn.sigmoid(recur_logit) * jax.nn.softplus(-decay_param)
        drive = jnp.sqrt(-jnp.expm1(2.0 * log_decay)) * jax.nn.sigmoid(input_logit) * conv_out
        _, states = lax.associative_scan(link_states, (jnp.exp(log_decay), drive), axis=0)
        mixed = (states * jax.nn.gelu(gate_branch.astype(jnp.float32))).astype(jnp.bfloat16)
        mix_sum = jnp.zeros((SEQ, D), jnp.float32)
        for group_index in range(N_TP):
            first_col = group_index * channel_group
            mix_part = jnp.dot(mixed[:, first_col:first_col + channel_group], out_bf[first_col:first_col + channel_group], preferred_element_type=jnp.float32) * out_scale
            mix_sum = mix_sum + lax.optimization_barrier(mix_part.astype(jnp.bfloat16)).astype(jnp.float32)
        hidden_state = (resid_in + rms_rows(mix_sum, gain_mix_post)).astype(jnp.bfloat16)
        normed_mlp = rms_rows(hidden_state.astype(jnp.float32), gain_mlp_pre).astype(jnp.bfloat16)
        up_proj = jnp.dot(normed_mlp, up_bf, preferred_element_type=jnp.float32) * up_scale
        activated = jnp.square(jax.nn.relu(up_proj)).astype(jnp.bfloat16)
        mlp_sum = jnp.zeros((SEQ, D), jnp.float32)
        for group_index in range(N_TP):
            first_col = group_index * hidden_group
            partial_value = jnp.dot(activated[:, first_col:first_col + hidden_group], down_bf[first_col:first_col + hidden_group], preferred_element_type=jnp.float32) * down_scale
            mlp_sum = mlp_sum + lax.optimization_barrier(partial_value.astype(jnp.bfloat16)).astype(jnp.float32)
        return (hidden_state.astype(jnp.float32) + rms_rows(mlp_sum, gain_mlp_post)).astype(jnp.bfloat16)
    return lax.map(one_sequence, tokens)
```

```python
import functools

import jax
import jax.numpy as jnp
from jax import lax
from jax.experimental import pallas as pl
from jax.experimental.pallas import tpu as pltpu
from jax.sharding import PartitionSpec as P

BLOCK = 32
LANES = 128
EPSILON = 1e-06
DECAY_SCALE = 8.0
F32 = jnp.float32
BF16 = jnp.bfloat16


def unit_rows(values):
    return values * lax.rsqrt(jnp.mean(values * values, axis=-1, keepdims=True) + EPSILON)


def shifted(values, distance, fill):
    head = jnp.full((distance, values.shape[1]), fill, values.dtype)
    return jnp.concatenate([head, values[: values.shape[0] - distance]], axis=0)


def mixer_kernel(x_ref, gate_ref, taps_ref, recur_ref, input_ref, rate_ref, mixed_ref):
    length = x_ref.shape[0]
    x_branch = x_ref[...].astype(F32)
    taps = taps_ref.shape[0]
    total = taps_ref[taps - 1 : taps, :] * x_branch
    for tap in range(taps - 1):
        total += taps_ref[tap : tap + 1, :] * shifted(x_branch, taps - 1 - tap, 0.0)
    conv = total.astype(BF16)
    recur = jax.nn.sigmoid(jnp.dot(conv, recur_ref[...], preferred_element_type=F32))
    gate_in = jax.nn.sigmoid(jnp.dot(conv, input_ref[...], preferred_element_type=F32))
    log_decay = recur * rate_ref[0:1, :]
    decay = jnp.exp(log_decay)
    z = -2.0 * log_decay
    series = z * (1.0 - z * (1 / 2) * (1.0 - z * (1 / 3) * (1.0 - z * (1 / 4) * (1.0 - z * (1 / 5)))))
    power = jnp.where(z < 0.1, series, 1.0 - decay * decay)
    state = jnp.sqrt(power) * gate_in * conv.astype(F32)
    distance = 1
    while distance < length:
        state = state + decay * shifted(state, distance, 0.0)
        decay = decay * shifted(decay, distance, 1.0)
        distance *= 2
    mixed_ref[...] = (state * jax.nn.gelu(gate_ref[...].astype(F32))).astype(BF16)


def mixer(branches, taps, recur_dense, input_dense, rate, sequences):
    rows, width = branches.shape[0], branches.shape[1] // 2
    length = rows // sequences
    groups = width // LANES
    return pl.pallas_call(
        mixer_kernel,
        grid=(sequences, groups),
        in_specs=[
            pl.BlockSpec((length, LANES), lambda s, g: (s, g)),
            pl.BlockSpec((length, LANES), lambda s, g: (s, g + groups)),
            pl.BlockSpec((taps.shape[0], LANES), lambda s, g: (0, g)),
            pl.BlockSpec((LANES, LANES), lambda s, g: (g, 0)),
            pl.BlockSpec((LANES, LANES), lambda s, g: (g, 0)),
            pl.BlockSpec((1, LANES), lambda s, g: (0, g)),
        ],
        out_specs=pl.BlockSpec((length, LANES), lambda s, g: (s, g)),
        out_shape=jax.ShapeDtypeStruct((rows, width), BF16),
        cost_estimate=pl.CostEstimate(
            flops=rows * width * 100, bytes_accessed=rows * width * 6, transcendentals=rows * width * 4
        ),
        name="mixer",
    )(branches, branches, taps, recur_dense, input_dense, rate)


MESH_IDS = pl.DeviceIdType.MESH


def greet(peers):
    barrier = pltpu.get_barrier_semaphore()
    for peer in peers:
        pl.semaphore_signal(barrier, inc=1, device_id=peer, device_id_type=MESH_IDS)
    pl.semaphore_wait(barrier, len(peers))


def push(source, target, sent, landed, peer):
    return pltpu.make_async_remote_copy(
        src_ref=source, dst_ref=target, send_sem=sent, recv_sem=landed,
        device_id=peer, device_id_type=MESH_IDS,
    )


def others(axis, count):
    me = lax.axis_index(axis)
    return [lax.rem(me + step, count) for step in range(1, count)]


def row_block(ref, index, rows):
    return ref.at[pl.ds(pl.multiple_of(index * rows, rows), rows)]


def team_gather_kernel(reps, tps, x_ref, out_ref, own_sem, sent, landed):
    rep, core = lax.axis_index("rep"), lax.axis_index("tp")
    rows = x_ref.shape[0]
    rep_peers, tp_peers = others("rep", reps), others("tp", tps)
    greet([{"rep": peer} for peer in rep_peers] + [{"tp": peer} for peer in tp_peers])
    mine = row_block(out_ref, rep * tps + core, rows)
    flights = []
    for step, peer in enumerate(rep_peers):
        copy = push(x_ref, mine, sent.at[step + 1, 0], landed.at[step + 1, 0], {"rep": peer})
        copy.start()
        flights.append(copy)
    own = pltpu.make_async_copy(x_ref, mine, own_sem)
    own.start()
    local = []
    for slot, peer in enumerate(tp_peers):
        copy = push(x_ref, mine, sent.at[0, slot + 1], landed.at[0, slot + 1], {"tp": peer})
        copy.start()
        local.append(copy)
    for step in range(1, reps):
        flights[step - 1].wait_recv()
        source = lax.rem(rep + reps - step, reps)
        block = row_block(out_ref, source * tps + core, rows)
        for slot, peer in enumerate(tp_peers):
            copy = push(block, block, sent.at[step, slot + 1], landed.at[step, slot + 1], {"tp": peer})
            copy.start()
            local.append(copy)
    for copy in flights:
        copy.wait_send()
    for copy in local:
        copy.wait()
    own.wait()


def team_gather(values):
    reps, tps = lax.axis_size("rep"), lax.axis_size("tp")
    rows, width = values.shape
    return pl.pallas_call(
        functools.partial(team_gather_kernel, reps, tps),
        out_shape=jax.ShapeDtypeStruct((rows * reps * tps, width), values.dtype),
        in_specs=[pl.BlockSpec(memory_space=pltpu.VMEM)],
        out_specs=pl.BlockSpec(memory_space=pltpu.VMEM),
        scratch_shapes=[
            pltpu.SemaphoreType.DMA,
            pltpu.SemaphoreType.DMA((reps, tps)),
            pltpu.SemaphoreType.DMA((reps, tps)),
        ],
        compiler_params=pltpu.CompilerParams(collective_id=0, has_side_effects=True),
        cost_estimate=pl.CostEstimate(flops=0, bytes_accessed=80_000_000, transcendentals=0),
        name="team_gather",
    )(values)


def team_sum_kernel(reps, tps, part_ref, out_ref, got, stage, last, sent, landed, sent_far, landed_far):
    rep, core = lax.axis_index("rep"), lax.axis_index("tp")
    rows = out_ref.shape[0]
    step_rows = 16
    rep_peers, tp_peers = others("rep", reps), others("tp", tps)
    greet([{"rep": peer} for peer in rep_peers] + [{"tp": peer} for peer in tp_peers])
    near = []
    for slot, peer in enumerate(tp_peers):
        for group in range(reps):
            copy = push(
                row_block(part_ref, group * tps + peer, rows), got.at[slot, group],
                sent.at[slot, group], landed.at[slot, group], {"tp": peer},
            )
            copy.start()
            near.append(copy)
    for copy in near:
        copy.wait()

    def total(group, start):
        base = pl.multiple_of((group * tps + core) * rows + start, step_rows)
        value = part_ref[pl.ds(base, step_rows)].astype(F32)
        for slot in range(tps - 1):
            value += got[slot, group, pl.ds(start, step_rows)].astype(F32)
        return value

    far = []
    for step, peer in enumerate(rep_peers):

        def fill(index, carry):
            start = pl.multiple_of(index * step_rows, step_rows)
            stage[step, pl.ds(start, step_rows)] = total(peer, start).astype(BF16)
            return carry

        lax.fori_loop(0, rows // step_rows, fill, 0)
        copy = push(stage.at[step], last.at[step], sent_far.at[step], landed_far.at[step], {"rep": peer})
        copy.start()
        far.append(copy)
    for copy in far:
        copy.wait()

    def finish(index, carry):
        start = pl.multiple_of(index * step_rows, step_rows)
        value = total(rep, start)
        for step in range(reps - 1):
            value += last[step, pl.ds(start, step_rows)].astype(F32)
        out_ref[pl.ds(start, step_rows)] = value
        return carry

    lax.fori_loop(0, rows // step_rows, finish, 0)


def team_sum(parts):
    reps, tps = lax.axis_size("rep"), lax.axis_size("tp")
    rows, width = parts.shape[0] // (reps * tps), parts.shape[1]
    return pl.pallas_call(
        functools.partial(team_sum_kernel, reps, tps),
        out_shape=jax.ShapeDtypeStruct((rows, width), F32),
        in_specs=[pl.BlockSpec(memory_space=pltpu.VMEM)],
        out_specs=pl.BlockSpec(memory_space=pltpu.VMEM),
        scratch_shapes=[
            pltpu.VMEM((tps - 1, reps, rows, width), BF16),
            pltpu.VMEM((reps - 1, rows, width), BF16),
            pltpu.VMEM((reps - 1, rows, width), BF16),
            pltpu.SemaphoreType.DMA((tps - 1, reps)),
            pltpu.SemaphoreType.DMA((tps - 1, reps)),
            pltpu.SemaphoreType.DMA((reps - 1,)),
            pltpu.SemaphoreType.DMA((reps - 1,)),
        ],
        compiler_params=pltpu.CompilerParams(collective_id=1, has_side_effects=True),
        cost_estimate=pl.CostEstimate(flops=0, bytes_accessed=80_000_000, transcendentals=0),
        name="team_sum",
    )(parts)


def shard_gather_kernel(shards, x_ref, out_ref, own_sem, sent, landed, sent_pass, landed_pass):
    me = lax.axis_index("fs")
    rows = x_ref.shape[0]
    pairs = shards // 2
    pair, parity = me // 2, lax.rem(me, 2)
    partner = {"fs": pair * 2 + 1 - parity}
    peers = [{"fs": lax.rem(pair + step, pairs) * 2 + parity} for step in range(1, pairs)]
    greet([partner] + peers)
    mine = row_block(out_ref, me, rows)
    passed = [push(x_ref, mine, sent_pass.at[0], landed_pass.at[0], partner)]
    passed[0].start()
    direct = []
    for step, peer in enumerate(peers):
        copy = push(x_ref, mine, sent.at[step], landed.at[step], peer)
        copy.start()
        direct.append(copy)
    own = pltpu.make_async_copy(x_ref, mine, own_sem)
    own.start()
    for step in range(1, pairs):
        direct[step - 1].wait_recv()
        block = row_block(out_ref, lax.rem(pair + pairs - step, pairs) * 2 + parity, rows)
        copy = push(block, block, sent_pass.at[step], landed_pass.at[step], partner)
        copy.start()
        passed.append(copy)
    for copy in direct:
        copy.wait_send()
    for copy in passed:
        copy.wait()
    own.wait()


def shard_gather(values, collective_id):
    shards = lax.axis_size("fs")
    rows, width = values.shape
    return pl.pallas_call(
        functools.partial(shard_gather_kernel, shards),
        out_shape=jax.ShapeDtypeStruct((rows * shards, width), values.dtype),
        in_specs=[pl.BlockSpec(memory_space=pltpu.VMEM)],
        out_specs=pl.BlockSpec(memory_space=pltpu.VMEM),
        scratch_shapes=[
            pltpu.SemaphoreType.DMA,
            pltpu.SemaphoreType.DMA((shards // 2,)),
            pltpu.SemaphoreType.DMA((shards // 2,)),
            pltpu.SemaphoreType.DMA((shards // 2,)),
            pltpu.SemaphoreType.DMA((shards // 2,)),
        ],
        compiler_params=pltpu.CompilerParams(collective_id=collective_id, has_side_effects=True),
        cost_estimate=pl.CostEstimate(flops=0, bytes_accessed=200_000_000, transcendentals=0),
        name="shard_gather",
    )(values)


def on_device(
    tokens, gain_mix_pre, gain_mix_post, gain_mlp_pre, gain_mlp_post,
    x_weight, gate_weight, x_scale, gate_scale, conv_weight, recur_map, input_map,
    decay_param, out_weight, out_scale, up_weight, up_scale, down_weight, down_scale,
):
    reps = lax.axis_size("rep")
    rep = lax.axis_index("rep")

    def part(values, axis):
        size = values.shape[axis] // reps
        return lax.dynamic_slice_in_dim(values, rep * size, size, axis)

    length = tokens.shape[1]
    share_rows = length // lax.axis_size("tp")
    offset_row = lax.axis_index("tp") * share_rows
    resid_share = lax.dynamic_slice_in_dim(tokens[0], offset_row, share_rows, 0).astype(F32)
    normed_share = unit_rows(resid_share).astype(BF16)

    pre = gain_mix_pre[:, None]
    branch_rows = jnp.concatenate(
        [(part(x_weight, 1) * pre).astype(BF16), (part(gate_weight, 1) * pre).astype(BF16)], axis=1
    )
    branch_rows, out_weight = lax.optimization_barrier((branch_rows, out_weight))
    branch_full = lax.all_gather(branch_rows, "fs", axis=0, tiled=True)
    post = jnp.stack([gain_mix_post, gain_mlp_post])
    post_high = post.astype(BF16)
    post_low = (post - post_high.astype(F32)).astype(BF16)
    pad_rows = jnp.zeros((12, post.shape[1]), BF16)
    out_cols = jnp.concatenate(
        [(part(out_weight, 0) * out_scale).astype(BF16), post_high, post_low, pad_rows], axis=0
    )
    out_cols, down_weight = lax.optimization_barrier((out_cols, down_weight))
    out_all = lax.all_gather(out_cols, "fs", axis=1, tiled=True)
    down_full = lax.all_gather((part(down_weight, 0) * down_scale).astype(BF16), "fs", axis=1, tiled=True)
    up_rows = (part(up_weight, 1) * gain_mlp_pre[:, None]).astype(BF16)
    normed = team_gather(normed_share)
    normed, up_rows = lax.optimization_barrier((normed, up_rows))
    up_full = shard_gather(up_rows, 2)
    normed, up_full = lax.optimization_barrier((normed, up_full))

    scales = jnp.concatenate([part(x_scale, 0), part(gate_scale, 0)])
    branches = (jnp.dot(normed, branch_full, preferred_element_type=F32) * scales).astype(BF16)
    width = branches.shape[1] // 2

    def dense(block_map):
        rows = lax.broadcasted_iota(jnp.int32, (width, LANES), 0)
        columns = lax.broadcasted_iota(jnp.int32, (width, LANES), 1)
        spread = jnp.tile(part(block_map, 0), (1, LANES // BLOCK))
        return jnp.where(rows % LANES // BLOCK == columns // BLOCK, spread, 0).astype(BF16)

    rate = -DECAY_SCALE * jax.nn.softplus(-part(decay_param, 0))
    mixed = mixer(
        branches, part(conv_weight, 1), dense(recur_map), dense(input_map), rate[None], reps
    )
    out_full = out_all[:width]
    gains = out_all[width : width + 2].astype(F32) + out_all[width + 2 : width + 4].astype(F32)
    mix_share = team_sum(jnp.dot(mixed, out_full, preferred_element_type=F32).astype(BF16))
    hidden_state = (resid_share + unit_rows(mix_share) * gains[0]).astype(BF16)
    mlp_input = team_gather(unit_rows(hidden_state.astype(F32)).astype(BF16))
    up_proj = jnp.dot(mlp_input, up_full, preferred_element_type=F32)
    activated = jnp.square(jax.nn.relu(up_proj * part(up_scale, 0))).astype(BF16)
    mlp_share = team_sum(jnp.dot(activated, down_full, preferred_element_type=F32).astype(BF16))
    return (hidden_state.astype(F32) + unit_rows(mlp_share) * gains[1]).astype(BF16)[None]


WEIGHTS = 4
PIECE = 256


def mixer_group(x_branch, gate, taps, recur_map, input_map, rate):
    length, count = x_branch.shape[0], taps.shape[0]
    total = taps[count - 1 : count, :] * x_branch
    for tap in range(count - 1):
        total += taps[tap : tap + 1, :] * shifted(x_branch, count - 1 - tap, 0.0)
    conv = total.astype(BF16)
    recur = jax.nn.sigmoid(jnp.dot(conv, recur_map, preferred_element_type=F32))
    gate_in = jax.nn.sigmoid(jnp.dot(conv, input_map, preferred_element_type=F32))
    log_decay = recur * rate
    decay = jnp.exp(log_decay)
    z = -2.0 * log_decay
    series = z * (1.0 - z * (1 / 2) * (1.0 - z * (1 / 3) * (1.0 - z * (1 / 4) * (1.0 - z * (1 / 5)))))
    power = jnp.where(z < 0.1, series, 1.0 - decay * decay)
    state = jnp.sqrt(power) * gate_in * conv.astype(F32)
    distance = 1
    while distance < length:
        state = state + decay * shifted(state, distance, 0.0)
        decay = decay * shifted(decay, distance, 1.0)
        distance *= 2
    return (state * jax.nn.gelu(gate)).astype(BF16)


def aligned(start, unit):
    return pl.multiple_of(start, unit)


def layer_kernel(
    shards, tokens, gains, b_parts, o_parts, u_parts, d_parts, scales, up_scale, taps, recur_map, input_map, rate,
    out, b_full, o_full, u_full, d_full, gains_full, tok_got, normed, branches, mixed, mlp_in, active, hidden,
    give, got_near, keep, total, stage, got_far,
    own_sem, y_sent, y_land, z_sent, z_land, zf_sent, x_sent, x_land, g_own, g_sent, g_land,
    t_sent, t_land, n_sent, n_land, f_sent, f_land, m_sent, m_land, mn_sent, mn_land, mf_sent, mf_land,
):
    lines = shards // 2
    others = lines - 1
    rep, me, core = lax.axis_index("rep"), lax.axis_index("fs"), lax.axis_index("tp")
    z, y = me // 2, lax.rem(me, 2)
    x_peer, core_peer, y_peer = {"rep": 1 - rep}, {"tp": 1 - core}, {"fs": z * 2 + 1 - y}
    upper = z // (lines // 2)
    depth = z + upper * (lines - 1 - 2 * z)

    def other(k):
        place = k + (k + lines - depth) // lines
        return place + upper * (lines - 1 - 2 * place)

    greet(
        [{"fs": lax.rem(me + step, shards)} for step in range(1, shards)] + [x_peer, core_peer]
    )
    parts = (b_parts, o_parts, u_parts, d_parts)
    fulls = (b_full, o_full, u_full, d_full)

    def half(w, slot, side):
        rows = parts[w].shape[1]
        return fulls[w].at[pl.ds(aligned(slot * rows + side * (rows // 2), 64), rows // 2)]

    def whole(w, slot):
        rows = parts[w].shape[1]
        return fulls[w].at[pl.ds(aligned(slot * rows, 64), rows)]

    def y_copy(w):
        return push(parts[w].at[1 - y], whole(w, me), y_sent.at[w], y_land.at[w], y_peer)

    def y_arrival(w):
        block = whole(w, z * 2 + 1 - y)
        return push(block, block, y_sent.at[w], y_land.at[w], y_peer)

    def own_copy(w):
        return pltpu.make_async_copy(parts[w].at[y], whole(w, me), own_sem.at[w])

    def z_copy(w, kind, k):
        slot = z * 2 + lax.rem(y + kind, 2)
        target = half(w, slot, rep)
        rows = parts[w].shape[1] // 2
        source = parts[w].at[y, pl.ds(aligned(rep * rows, 64), rows)] if kind == 0 else target
        return push(source, target, z_sent.at[w, kind, k], z_land.at[w, slot], {"fs": other(k) * 2 + y})

    def start_z(w, kind):
        for k in range(others - 1):
            z_copy(w, kind, k).start()

        @pl.when(depth > 0)
        def _():
            z_copy(w, kind, others - 1).start()

    def item_slot(kind, k):
        return other(k) * 2 + lax.rem(y + kind, 2)

    def zf_copy(w, kind):
        block = half(w, item_slot(kind, others - 1), rep)
        ends = upper * (lines - 1)
        return push(block, block, zf_sent.at[w, kind], z_land.at[w, item_slot(kind, others - 1)], {"fs": ends * 2 + y})

    def x_copy(w, kind, k):
        slot = item_slot(kind, k)
        block = half(w, slot, rep)
        return push(block, block, x_sent.at[w, kind, k], x_land.at[w, slot], x_peer)

    def serve(w, kind, k):
        slot = item_slot(kind, k)
        block = half(w, slot, rep)
        push(block, block, x_sent.at[w, kind, k], z_land.at[w, slot], x_peer).wait_recv()
        x_copy(w, kind, k).start()

        def onward():
            zf_copy(w, kind).start()

        if isinstance(k, int):
            if k == others - 1:
                pl.when(depth == 1)(onward)
        else:
            pl.when((k == others - 1) & (depth == 1))(onward)

    def x_arrival(w, kind, k):
        slot = item_slot(kind, k)
        block = half(w, slot, 1 - rep)
        push(block, block, x_sent.at[w, kind, k], x_land.at[w, slot], x_peer).wait_recv()

    def all_x_arrivals(w):
        def body(index, carry):
            x_arrival(w, index // others, lax.rem(index, others))
            return carry

        lax.fori_loop(0, 2 * others, body, 0)

    def serve_step(w, index, count=2 * others):
        @pl.when((index >= 0) & (index < count))
        def _():
            serve(w, index // others, lax.rem(index, others))

    seq = tokens.shape[0]
    share = seq // 2
    width = tokens.shape[1]
    mine = pl.ds(aligned(core * share, 64), share)
    t_near = push(tokens.at[mine], tok_got.at[mine], t_sent.at[0], t_land.at[0], y_peer)
    t_pass = push(tok_got.at[mine], tok_got.at[mine], t_sent.at[1], t_land.at[1], core_peer)

    y_copy(0).start()
    start_z(0, 0)
    t_near.start()
    for w in range(1, WEIGHTS):
        y_copy(w).start()
    for w in range(WEIGHTS):
        own_copy(w).start()
    own_gains = pltpu.make_async_copy(gains, gains_full.at[me], g_own)
    own_gains.start()

    def gain_copy(step):
        return push(gains, gains_full.at[me], g_sent.at[step - 1], g_land.at[me], {"fs": lax.rem(me + step, shards)})

    for step in range(1, shards):
        gain_copy(step).start()

    rows = 16

    def normalize(source, base):
        def body(index, carry):
            start = aligned(index * rows, rows)
            values = source[pl.ds(start, rows), :].astype(F32)
            normed[pl.ds(aligned(base + start, rows), rows), :] = unit_rows(values).astype(BF16)
            return carry

        lax.fori_loop(0, seq // rows, body, 0)

    normalize(tokens, 0)
    y_arrival(0).wait_recv()
    start_z(0, 1)
    start_z(1, 0)
    for k in range(others):
        serve(0, 0, k)
    for k in range(others):
        serve(0, 1, k)
    t_near.wait_recv()
    t_pass.start()
    y_arrival(1).wait_recv()
    start_z(1, 1)
    start_z(2, 0)
    t_pass.wait_recv()
    normalize(tok_got, seq)
    all_x_arrivals(0)
    own_copy(0).wait()

    columns = branches.shape[1]
    col_tiles = columns // PIECE

    def branch_step(index, carry):
        row = aligned((index // col_tiles) * seq, 64)
        col = aligned(lax.rem(index, col_tiles) * PIECE, PIECE)
        value = jnp.dot(normed[pl.ds(row, seq), :], b_full[:, pl.ds(col, PIECE)], preferred_element_type=F32)
        branches[pl.ds(row, seq), pl.ds(col, PIECE)] = (value * scales[:, pl.ds(col, PIECE)]).astype(BF16)
        serve_step(1, index)
        return carry

    lax.fori_loop(0, 2 * col_tiles, branch_step, 0)

    groups = columns // 2 // LANES

    def mixer_step(index, carry):
        row = aligned((index // groups) * seq, 64)
        group = lax.rem(index, groups)
        col = aligned(group * LANES, LANES)
        lanes = pl.ds(col, LANES)
        mixed[pl.ds(row, seq), lanes] = mixer_group(
            branches[pl.ds(row, seq), lanes].astype(F32),
            branches[pl.ds(row, seq), pl.ds(aligned(columns // 2 + col, LANES), LANES)].astype(F32),
            taps[:, lanes], recur_map[lanes, :], input_map[lanes, :], rate[:, lanes],
        )

        @pl.when(index == groups)
        def _():
            y_arrival(2).wait_recv()
            start_z(2, 1)
            start_z(3, 0)

        @pl.when(index > groups)
        def _():
            serve_step(2, index - groups - 1, others)

        return carry

    lax.fori_loop(0, 2 * groups, mixer_step, 0)
    y_arrival(3).wait_recv()
    start_z(3, 1)

    def block_of(index):
        item = index - 2
        kind = (item + 2 * others) // others - 2
        far = item_slot(lax.rem(kind + 2, 2), lax.rem(item + 2 * others, others))
        near = z * 2 + lax.rem(y + index, 2)
        late = (index + shards - 2) // shards
        return near + late * (far - near)

    def near_copy(phase, block):
        return push(give.at[block], got_near.at[block], n_sent.at[phase, block], n_land.at[phase, block], core_peer)

    def far_copy(phase, block):
        return push(stage.at[block], got_far.at[block], f_sent.at[phase, block], f_land.at[phase, block], y_peer)

    def project(phase, w, lhs, before):
        depth_rows = parts[w].shape[1]

        def combine(index):
            block = block_of(index)
            near_copy(phase, block).wait_recv()
            stage[block] = (keep[block] + got_near[block, 1].astype(F32)).astype(BF16)
            total[block] += got_near[block, 0].astype(F32)
            far_copy(phase, block).start()

        def body(index, carry):
            before(index)
            block = block_of(index)
            weight = fulls[w][pl.ds(aligned(block * depth_rows, 64), depth_rows), :]
            for side in range(2):
                left = lhs[pl.ds(aligned(side * seq + (1 - core) * share, 64), share), :]
                give[block, side] = jnp.dot(left, weight, preferred_element_type=F32).astype(BF16)
            own = lhs[pl.ds(aligned(core * share, 64), share), :]
            total[block] = jnp.dot(own, weight, preferred_element_type=F32)
            near_copy(phase, block).start()
            own = lhs[pl.ds(aligned(seq + core * share, 64), share), :]
            keep[block] = jnp.dot(own, weight, preferred_element_type=F32)

            @pl.when(index > 0)
            def _():
                combine(index - 1)

            return carry

        lax.fori_loop(0, shards, body, 0)
        combine(shards - 1)

    def collect(phase, between):
        def body(index, carry):
            block = block_of(index)
            far_copy(phase, block).wait_recv()
            total[block] += got_far[block].astype(F32)
            between(index)
            return carry

        lax.fori_loop(0, shards, body, 0)

        def drain(index, carry):
            far_copy(phase, index).wait_send()
            near_copy(phase, index).wait_send()
            return carry

        lax.fori_loop(0, shards, drain, 0)

    all_x_arrivals(1)
    own_copy(1).wait()
    project(0, 1, mixed, lambda index: None)

    def serve_up(index):
        @pl.when(lax.rem(index, 2) == 1)
        def _():
            serve_step(2, others + index // 2)

    collect(0, serve_up)

    own_gains.wait()
    for step in range(1, shards):
        source = lax.rem(me + step, shards)
        push(gains, gains_full.at[source], g_sent.at[step - 1], g_land.at[source], y_peer).wait_recv()

    def summed(start):
        values = [total[block, pl.ds(start, rows), :] for block in range(shards)]
        squares = sum(jnp.sum(value * value, axis=-1, keepdims=True) for value in values)
        return values, lax.rsqrt(squares * (1.0 / width) + EPSILON)

    pieces = m_sent.shape[0]
    piece_rows = share // pieces

    def piece(ref, base, index):
        return ref.at[pl.ds(aligned(base + index * piece_rows, 16), piece_rows)]

    def to_far(index):
        return push(
            piece(mlp_in, core * share, index), piece(mlp_in, seq + core * share, index),
            m_sent.at[index], m_land.at[index], y_peer,
        )

    def to_near(index):
        block = piece(mlp_in, core * share, index)
        return push(block, block, mn_sent.at[index], mn_land.at[index], core_peer)

    def onward(index):
        block = piece(mlp_in, seq + core * share, index)
        return push(block, block, mf_sent.at[index], mf_land.at[index], core_peer)

    def entry_piece(index, carry):
        def entry_rows(inner, inner_carry):
            start = aligned(index * piece_rows + inner * rows, rows)
            values, factor = summed(start)
            place = aligned(core * share + start, rows)
            squares = jnp.zeros((rows, 1), F32)
            kept = []
            for block in range(shards):
                cols = pl.ds(block * PIECE, PIECE)
                value = tokens[pl.ds(place, rows), cols].astype(F32) + values[block] * factor * gains_full[block, 0:1, :]
                value = value.astype(BF16)
                hidden[pl.ds(start, rows), cols] = value
                value = value.astype(F32)
                kept.append(value)
                squares += jnp.sum(value * value, axis=-1, keepdims=True)
            scale = lax.rsqrt(squares * (1.0 / width) + EPSILON)
            for block in range(shards):
                mlp_in[pl.ds(place, rows), pl.ds(block * PIECE, PIECE)] = (kept[block] * scale).astype(BF16)
            return inner_carry

        lax.fori_loop(0, piece_rows // rows, entry_rows, 0)
        to_far(index).start()
        to_near(index).start()
        return carry

    lax.fori_loop(0, pieces, entry_piece, 0)
    all_x_arrivals(2)
    own_copy(2).wait()

    def wait_near(index, carry):
        to_near(index).wait_recv()
        return carry

    lax.fori_loop(0, pieces, wait_near, 0)
    up_tiles = active.shape[1] // PIECE

    def up_rows(base):
        def body(index, carry):
            col = aligned(index * PIECE, PIECE)
            value = jnp.dot(mlp_in[pl.ds(base, seq), :], u_full[:, pl.ds(col, PIECE)], preferred_element_type=F32)
            value = jnp.maximum(value * up_scale[:, pl.ds(col, PIECE)], 0.0)
            active[pl.ds(base, seq), pl.ds(col, PIECE)] = (value * value).astype(BF16)
            return carry

        lax.fori_loop(0, up_tiles, body, 0)

    up_rows(0)

    def pass_on(index, carry):
        to_far(index).wait_recv()
        onward(index).start()
        return carry

    lax.fori_loop(0, pieces, pass_on, 0)

    def wait_far(index, carry):
        onward(index).wait_recv()
        return carry

    lax.fori_loop(0, pieces, wait_far, 0)
    up_rows(seq)

    def before_down(index):
        serve_step(3, index)

        @pl.when(index >= 2)
        def _():
            item = index - 2
            x_arrival(3, item // others, lax.rem(item, others))

    own_copy(3).wait()
    project(1, 3, active, before_down)
    collect(1, lambda index: None)

    def last_rows(index, carry):
        start = aligned(index * rows, rows)
        values, factor = summed(start)
        for block in range(shards):
            cols = pl.ds(block * PIECE, PIECE)
            value = hidden[pl.ds(start, rows), cols].astype(F32) + values[block] * factor * gains_full[block, 1:2, :]
            out[pl.ds(start, rows), cols] = value.astype(BF16)
        return carry

    lax.fori_loop(0, share // rows, last_rows, 0)

    for w in range(WEIGHTS):
        y_copy(w).wait_send()
        for kind in range(2):
            for k in range(others - 1):
                z_copy(w, kind, k).wait_send()

            @pl.when(depth > 0)
            def _():
                z_copy(w, kind, others - 1).wait_send()

            @pl.when(depth == 1)
            def _():
                zf_copy(w, kind).wait_send()

            for k in range(others):
                x_copy(w, kind, k).wait_send()
    t_near.wait_send()
    t_pass.wait_send()
    for step in range(1, shards):
        gain_copy(step).wait_send()

    def drain(index, carry):
        to_far(index).wait_send()
        to_near(index).wait_send()
        onward(index).wait_send()
        return carry

    lax.fori_loop(0, pieces, drain, 0)


def layer(shards, tokens, gains, weight_parts, scales, up_scale, taps, recur_map, input_map, rate):
    seq, width = tokens.shape
    share = seq // 2
    lines = shards // 2
    pieces = 4
    branch_width, hidden_units = scales.shape[1], up_scale.shape[1]
    dma = pltpu.SemaphoreType.DMA
    vmem = pl.BlockSpec(memory_space=pltpu.VMEM)
    anywhere = pl.BlockSpec(memory_space=pl.ANY)
    fulls = [pltpu.VMEM((shards * part.shape[1], part.shape[2]), BF16) for part in weight_parts]
    return pl.pallas_call(
        functools.partial(layer_kernel, shards),
        out_shape=jax.ShapeDtypeStruct((share, width), BF16),
        in_specs=[vmem, vmem] + [anywhere] * WEIGHTS + [vmem] * 6,
        out_specs=vmem,
        scratch_shapes=fulls + [
            pltpu.VMEM((shards,) + gains.shape, F32),
            pltpu.VMEM((seq, width), BF16),
            pltpu.VMEM((2 * seq, width), BF16),
            pltpu.VMEM((2 * seq, branch_width), BF16),
            pltpu.VMEM((2 * seq, branch_width // 2), BF16),
            pltpu.VMEM((2 * seq, width), BF16),
            pltpu.VMEM((2 * seq, hidden_units), BF16),
            pltpu.VMEM((share, width), BF16),
            pltpu.VMEM((shards, 2, share, width // shards), BF16),
            pltpu.VMEM((shards, 2, share, width // shards), BF16),
            pltpu.VMEM((shards, share, width // shards), F32),
            pltpu.VMEM((shards, share, width // shards), F32),
            pltpu.VMEM((shards, share, width // shards), BF16),
            pltpu.VMEM((shards, share, width // shards), BF16),
            dma((WEIGHTS,)), dma((WEIGHTS,)), dma((WEIGHTS,)),
            dma((WEIGHTS, 2, lines - 1)), dma((WEIGHTS, shards)), dma((WEIGHTS, 2)),
            dma((WEIGHTS, 2, lines - 1)), dma((WEIGHTS, shards)),
            dma, dma((shards - 1,)), dma((shards,)),
            dma((2,)), dma((2,)),
            dma((2, shards)), dma((2, shards)), dma((2, shards)), dma((2, shards)),
            dma((pieces,)), dma((pieces,)), dma((pieces,)), dma((pieces,)), dma((pieces,)), dma((pieces,)),
        ],
        compiler_params=pltpu.CompilerParams(
            collective_id=4, has_side_effects=True, vmem_limit_bytes=66_000_000
        ),
        cost_estimate=pl.CostEstimate(flops=20_000_000_000, bytes_accessed=80_000_000, transcendentals=0),
        name="layer",
    )(tokens, gains, *weight_parts, scales, up_scale, taps, recur_map, input_map, rate)


def on_device_paired(
    tokens, gain_mix_pre, gain_mix_post, gain_mlp_pre, gain_mlp_post,
    x_weight, gate_weight, x_scale, gate_scale, conv_weight, recur_map, input_map,
    decay_param, out_weight, out_scale, up_weight, up_scale, down_weight, down_scale,
):
    shards = lax.axis_size("fs")
    side = lax.rem(lax.axis_index("fs"), 2)

    def part(values, axis):
        size = values.shape[axis] // 2
        return lax.dynamic_slice_in_dim(values, side * size, size, axis)

    def by_columns(*arrays):
        halves = [jnp.split(array, 2, axis=1) for array in arrays]
        return jnp.stack([jnp.concatenate([pair[p] for pair in halves], axis=1) for p in range(2)])

    def by_rows(array):
        return array.reshape(2, array.shape[0] // 2, array.shape[1])

    pre, mlp_pre = gain_mix_pre[:, None], gain_mlp_pre[:, None]
    weight_parts = (
        by_columns((x_weight * pre).astype(BF16), (gate_weight * pre).astype(BF16)),
        by_rows((out_weight * out_scale).astype(BF16)),
        by_columns((up_weight * mlp_pre).astype(BF16)),
        by_rows((down_weight * down_scale).astype(BF16)),
    )
    gains = jnp.stack([gain_mix_post, gain_mlp_post])
    scales = jnp.concatenate([part(x_scale, 0), part(gate_scale, 0)])[None]
    width = scales.shape[1] // 2

    def dense(block_map):
        rows = lax.broadcasted_iota(jnp.int32, (width, LANES), 0)
        columns = lax.broadcasted_iota(jnp.int32, (width, LANES), 1)
        spread = jnp.tile(part(block_map, 0), (1, LANES // BLOCK))
        return jnp.where(rows % LANES // BLOCK == columns // BLOCK, spread, 0).astype(BF16)

    rate = (-DECAY_SCALE * jax.nn.softplus(-part(decay_param, 0)))[None]
    return layer(
        shards, tokens[0], gains, weight_parts, scales, part(up_scale, 0)[None], part(conv_weight, 1),
        dense(recur_map), dense(input_map), rate,
    )[None]


def solution(mesh):
    in_specs = (
        P(("rep", "fs"), None, None),
        P("fs"), P("fs"), P("fs"), P("fs"),
        P("fs", "tp"), P("fs", "tp"),
        P("tp"), P("tp"),
        P(None, "tp"), P("tp", None), P("tp", None), P("tp"),
        P("tp", "fs"), P("fs"),
        P("fs", "tp"), P("tp"),
        P("tp", "fs"), P("fs"),
    )
    out_specs = P(("rep", "fs"), "tp", None)
    paired = (
        mesh.shape["rep"] == 2 and mesh.shape["tp"] == 2
        and mesh.shape["fs"] % 4 == 0 and mesh.shape["fs"] > 4
    )
    return jax.shard_map(
        on_device_paired if paired else on_device, mesh=mesh, in_specs=in_specs, out_specs=out_specs, check_vma=False
    )
```

```python
import functools

import jax
import jax.numpy as jnp
from jax import lax
from jax.experimental import pallas as pl
from jax.experimental.pallas import tpu as pltpu
from jax.sharding import PartitionSpec as P

BLOCK = 32
LANES = 128
EPSILON = 1e-06
DECAY_SCALE = 8.0
F32 = jnp.float32
BF16 = jnp.bfloat16


def unit_rows(values):
    return values * lax.rsqrt(jnp.mean(values * values, axis=-1, keepdims=True) + EPSILON)


def shifted(values, distance, fill):
    head = jnp.full((distance, values.shape[1]), fill, values.dtype)
    return jnp.concatenate([head, values[: values.shape[0] - distance]], axis=0)


def mixer_kernel(x_ref, gate_ref, taps_ref, recur_ref, input_ref, rate_ref, mixed_ref):
    length = x_ref.shape[0]
    x_branch = x_ref[...].astype(F32)
    taps = taps_ref.shape[0]
    total = taps_ref[taps - 1 : taps, :] * x_branch
    for tap in range(taps - 1):
        total += taps_ref[tap : tap + 1, :] * shifted(x_branch, taps - 1 - tap, 0.0)
    conv = total.astype(BF16)
    recur = jax.nn.sigmoid(jnp.dot(conv, recur_ref[...], preferred_element_type=F32))
    gate_in = jax.nn.sigmoid(jnp.dot(conv, input_ref[...], preferred_element_type=F32))
    log_decay = recur * rate_ref[0:1, :]
    decay = jnp.exp(log_decay)
    z = -2.0 * log_decay
    series = z * (1.0 - z * (1 / 2) * (1.0 - z * (1 / 3) * (1.0 - z * (1 / 4) * (1.0 - z * (1 / 5)))))
    power = jnp.where(z < 0.1, series, 1.0 - decay * decay)
    state = jnp.sqrt(power) * gate_in * conv.astype(F32)
    distance = 1
    while distance < length:
        state = state + decay * shifted(state, distance, 0.0)
        decay = decay * shifted(decay, distance, 1.0)
        distance *= 2
    mixed_ref[...] = (state * jax.nn.gelu(gate_ref[...].astype(F32))).astype(BF16)


def mixer(branches, taps, recur_dense, input_dense, rate, sequences):
    rows, width = branches.shape[0], branches.shape[1] // 2
    length = rows // sequences
    groups = width // LANES
    return pl.pallas_call(
        mixer_kernel,
        grid=(sequences, groups),
        in_specs=[
            pl.BlockSpec((length, LANES), lambda s, g: (s, g)),
            pl.BlockSpec((length, LANES), lambda s, g: (s, g + groups)),
            pl.BlockSpec((taps.shape[0], LANES), lambda s, g: (0, g)),
            pl.BlockSpec((LANES, LANES), lambda s, g: (g, 0)),
            pl.BlockSpec((LANES, LANES), lambda s, g: (g, 0)),
            pl.BlockSpec((1, LANES), lambda s, g: (0, g)),
        ],
        out_specs=pl.BlockSpec((length, LANES), lambda s, g: (s, g)),
        out_shape=jax.ShapeDtypeStruct((rows, width), BF16),
        cost_estimate=pl.CostEstimate(
            flops=rows * width * 100, bytes_accessed=rows * width * 6, transcendentals=rows * width * 4
        ),
        name="mixer",
    )(branches, branches, taps, recur_dense, input_dense, rate)


MESH_IDS = pl.DeviceIdType.MESH


def greet(peers):
    barrier = pltpu.get_barrier_semaphore()
    for peer in peers:
        pl.semaphore_signal(barrier, inc=1, device_id=peer, device_id_type=MESH_IDS)
    pl.semaphore_wait(barrier, len(peers))


def push(source, target, sent, landed, peer):
    return pltpu.make_async_remote_copy(
        src_ref=source, dst_ref=target, send_sem=sent, recv_sem=landed,
        device_id=peer, device_id_type=MESH_IDS,
    )


def others(axis, count):
    me = lax.axis_index(axis)
    return [lax.rem(me + step, count) for step in range(1, count)]


def row_block(ref, index, rows):
    return ref.at[pl.ds(pl.multiple_of(index * rows, rows), rows)]


def team_gather_kernel(reps, tps, x_ref, out_ref, own_sem, sent, landed):
    rep, core = lax.axis_index("rep"), lax.axis_index("tp")
    rows = x_ref.shape[0]
    rep_peers, tp_peers = others("rep", reps), others("tp", tps)
    greet([{"rep": peer} for peer in rep_peers] + [{"tp": peer} for peer in tp_peers])
    mine = row_block(out_ref, rep * tps + core, rows)
    flights = []
    for step, peer in enumerate(rep_peers):
        copy = push(x_ref, mine, sent.at[step + 1, 0], landed.at[step + 1, 0], {"rep": peer})
        copy.start()
        flights.append(copy)
    own = pltpu.make_async_copy(x_ref, mine, own_sem)
    own.start()
    local = []
    for slot, peer in enumerate(tp_peers):
        copy = push(x_ref, mine, sent.at[0, slot + 1], landed.at[0, slot + 1], {"tp": peer})
        copy.start()
        local.append(copy)
    for step in range(1, reps):
        flights[step - 1].wait_recv()
        source = lax.rem(rep + reps - step, reps)
        block = row_block(out_ref, source * tps + core, rows)
        for slot, peer in enumerate(tp_peers):
            copy = push(block, block, sent.at[step, slot + 1], landed.at[step, slot + 1], {"tp": peer})
            copy.start()
            local.append(copy)
    for copy in flights:
        copy.wait_send()
    for copy in local:
        copy.wait()
    own.wait()


def team_gather(values):
    reps, tps = lax.axis_size("rep"), lax.axis_size("tp")
    rows, width = values.shape
    return pl.pallas_call(
        functools.partial(team_gather_kernel, reps, tps),
        out_shape=jax.ShapeDtypeStruct((rows * reps * tps, width), values.dtype),
        in_specs=[pl.BlockSpec(memory_space=pltpu.VMEM)],
        out_specs=pl.BlockSpec(memory_space=pltpu.VMEM),
        scratch_shapes=[
            pltpu.SemaphoreType.DMA,
            pltpu.SemaphoreType.DMA((reps, tps)),
            pltpu.SemaphoreType.DMA((reps, tps)),
        ],
        compiler_params=pltpu.CompilerParams(collective_id=0, has_side_effects=True),
        cost_estimate=pl.CostEstimate(flops=0, bytes_accessed=80_000_000, transcendentals=0),
        name="team_gather",
    )(values)


def team_sum_kernel(reps, tps, part_ref, out_ref, got, stage, last, sent, landed, sent_far, landed_far):
    rep, core = lax.axis_index("rep"), lax.axis_index("tp")
    rows = out_ref.shape[0]
    step_rows = 16
    rep_peers, tp_peers = others("rep", reps), others("tp", tps)
    greet([{"rep": peer} for peer in rep_peers] + [{"tp": peer} for peer in tp_peers])
    near = []
    for slot, peer in enumerate(tp_peers):
        for group in range(reps):
            copy = push(
                row_block(part_ref, group * tps + peer, rows), got.at[slot, group],
                sent.at[slot, group], landed.at[slot, group], {"tp": peer},
            )
            copy.start()
            near.append(copy)
    for copy in near:
        copy.wait()

    def total(group, start):
        base = pl.multiple_of((group * tps + core) * rows + start, step_rows)
        value = part_ref[pl.ds(base, step_rows)].astype(F32)
        for slot in range(tps - 1):
            value += got[slot, group, pl.ds(start, step_rows)].astype(F32)
        return value

    far = []
    for step, peer in enumerate(rep_peers):

        def fill(index, carry):
            start = pl.multiple_of(index * step_rows, step_rows)
            stage[step, pl.ds(start, step_rows)] = total(peer, start).astype(BF16)
            return carry

        lax.fori_loop(0, rows // step_rows, fill, 0)
        copy = push(stage.at[step], last.at[step], sent_far.at[step], landed_far.at[step], {"rep": peer})
        copy.start()
        far.append(copy)
    for copy in far:
        copy.wait()

    def finish(index, carry):
        start = pl.multiple_of(index * step_rows, step_rows)
        value = total(rep, start)
        for step in range(reps - 1):
            value += last[step, pl.ds(start, step_rows)].astype(F32)
        out_ref[pl.ds(start, step_rows)] = value
        return carry

    lax.fori_loop(0, rows // step_rows, finish, 0)


def team_sum(parts):
    reps, tps = lax.axis_size("rep"), lax.axis_size("tp")
    rows, width = parts.shape[0] // (reps * tps), parts.shape[1]
    return pl.pallas_call(
        functools.partial(team_sum_kernel, reps, tps),
        out_shape=jax.ShapeDtypeStruct((rows, width), F32),
        in_specs=[pl.BlockSpec(memory_space=pltpu.VMEM)],
        out_specs=pl.BlockSpec(memory_space=pltpu.VMEM),
        scratch_shapes=[
            pltpu.VMEM((tps - 1, reps, rows, width), BF16),
            pltpu.VMEM((reps - 1, rows, width), BF16),
            pltpu.VMEM((reps - 1, rows, width), BF16),
            pltpu.SemaphoreType.DMA((tps - 1, reps)),
            pltpu.SemaphoreType.DMA((tps - 1, reps)),
            pltpu.SemaphoreType.DMA((reps - 1,)),
            pltpu.SemaphoreType.DMA((reps - 1,)),
        ],
        compiler_params=pltpu.CompilerParams(collective_id=1, has_side_effects=True),
        cost_estimate=pl.CostEstimate(flops=0, bytes_accessed=80_000_000, transcendentals=0),
        name="team_sum",
    )(parts)


def shard_gather_kernel(shards, x_ref, out_ref, own_sem, sent, landed, sent_pass, landed_pass):
    me = lax.axis_index("fs")
    rows = x_ref.shape[0]
    pairs = shards // 2
    pair, parity = me // 2, lax.rem(me, 2)
    partner = {"fs": pair * 2 + 1 - parity}
    peers = [{"fs": lax.rem(pair + step, pairs) * 2 + parity} for step in range(1, pairs)]
    greet([partner] + peers)
    mine = row_block(out_ref, me, rows)
    passed = [push(x_ref, mine, sent_pass.at[0], landed_pass.at[0], partner)]
    passed[0].start()
    direct = []
    for step, peer in enumerate(peers):
        copy = push(x_ref, mine, sent.at[step], landed.at[step], peer)
        copy.start()
        direct.append(copy)
    own = pltpu.make_async_copy(x_ref, mine, own_sem)
    own.start()
    for step in range(1, pairs):
        direct[step - 1].wait_recv()
        block = row_block(out_ref, lax.rem(pair + pairs - step, pairs) * 2 + parity, rows)
        copy = push(block, block, sent_pass.at[step], landed_pass.at[step], partner)
        copy.start()
        passed.append(copy)
    for copy in direct:
        copy.wait_send()
    for copy in passed:
        copy.wait()
    own.wait()


def shard_gather(values, collective_id):
    shards = lax.axis_size("fs")
    rows, width = values.shape
    return pl.pallas_call(
        functools.partial(shard_gather_kernel, shards),
        out_shape=jax.ShapeDtypeStruct((rows * shards, width), values.dtype),
        in_specs=[pl.BlockSpec(memory_space=pltpu.VMEM)],
        out_specs=pl.BlockSpec(memory_space=pltpu.VMEM),
        scratch_shapes=[
            pltpu.SemaphoreType.DMA,
            pltpu.SemaphoreType.DMA((shards // 2,)),
            pltpu.SemaphoreType.DMA((shards // 2,)),
            pltpu.SemaphoreType.DMA((shards // 2,)),
            pltpu.SemaphoreType.DMA((shards // 2,)),
        ],
        compiler_params=pltpu.CompilerParams(collective_id=collective_id, has_side_effects=True),
        cost_estimate=pl.CostEstimate(flops=0, bytes_accessed=200_000_000, transcendentals=0),
        name="shard_gather",
    )(values)


def on_device(
    tokens, gain_mix_pre, gain_mix_post, gain_mlp_pre, gain_mlp_post,
    x_weight, gate_weight, x_scale, gate_scale, conv_weight, recur_map, input_map,
    decay_param, out_weight, out_scale, up_weight, up_scale, down_weight, down_scale,
):
    reps = lax.axis_size("rep")
    rep = lax.axis_index("rep")

    def part(values, axis):
        size = values.shape[axis] // reps
        return lax.dynamic_slice_in_dim(values, rep * size, size, axis)

    length = tokens.shape[1]
    share_rows = length // lax.axis_size("tp")
    offset_row = lax.axis_index("tp") * share_rows
    resid_share = lax.dynamic_slice_in_dim(tokens[0], offset_row, share_rows, 0).astype(F32)
    normed_share = unit_rows(resid_share).astype(BF16)

    pre = gain_mix_pre[:, None]
    branch_rows = jnp.concatenate(
        [(part(x_weight, 1) * pre).astype(BF16), (part(gate_weight, 1) * pre).astype(BF16)], axis=1
    )
    branch_rows, out_weight = lax.optimization_barrier((branch_rows, out_weight))
    branch_full = lax.all_gather(branch_rows, "fs", axis=0, tiled=True)
    post = jnp.stack([gain_mix_post, gain_mlp_post])
    post_high = post.astype(BF16)
    post_low = (post - post_high.astype(F32)).astype(BF16)
    pad_rows = jnp.zeros((12, post.shape[1]), BF16)
    out_cols = jnp.concatenate(
        [(part(out_weight, 0) * out_scale).astype(BF16), post_high, post_low, pad_rows], axis=0
    )
    out_cols, down_weight = lax.optimization_barrier((out_cols, down_weight))
    out_all = lax.all_gather(out_cols, "fs", axis=1, tiled=True)
    down_full = lax.all_gather((part(down_weight, 0) * down_scale).astype(BF16), "fs", axis=1, tiled=True)
    up_rows = (part(up_weight, 1) * gain_mlp_pre[:, None]).astype(BF16)
    normed = team_gather(normed_share)
    normed, up_rows = lax.optimization_barrier((normed, up_rows))
    up_full = shard_gather(up_rows, 2)
    normed, up_full = lax.optimization_barrier((normed, up_full))

    scales = jnp.concatenate([part(x_scale, 0), part(gate_scale, 0)])
    branches = (jnp.dot(normed, branch_full, preferred_element_type=F32) * scales).astype(BF16)
    width = branches.shape[1] // 2

    def dense(block_map):
        rows = lax.broadcasted_iota(jnp.int32, (width, LANES), 0)
        columns = lax.broadcasted_iota(jnp.int32, (width, LANES), 1)
        spread = jnp.tile(part(block_map, 0), (1, LANES // BLOCK))
        return jnp.where(rows % LANES // BLOCK == columns // BLOCK, spread, 0).astype(BF16)

    rate = -DECAY_SCALE * jax.nn.softplus(-part(decay_param, 0))
    mixed = mixer(
        branches, part(conv_weight, 1), dense(recur_map), dense(input_map), rate[None], reps
    )
    out_full = out_all[:width]
    gains = out_all[width : width + 2].astype(F32) + out_all[width + 2 : width + 4].astype(F32)
    mix_share = team_sum(jnp.dot(mixed, out_full, preferred_element_type=F32).astype(BF16))
    hidden_state = (resid_share + unit_rows(mix_share) * gains[0]).astype(BF16)
    mlp_input = team_gather(unit_rows(hidden_state.astype(F32)).astype(BF16))
    up_proj = jnp.dot(mlp_input, up_full, preferred_element_type=F32)
    activated = jnp.square(jax.nn.relu(up_proj * part(up_scale, 0))).astype(BF16)
    mlp_share = team_sum(jnp.dot(activated, down_full, preferred_element_type=F32).astype(BF16))
    return (hidden_state.astype(F32) + unit_rows(mlp_share) * gains[1]).astype(BF16)[None]


WEIGHTS = 4
PIECE = 256


def log_decay_and_drive(conv, logits, rate):
    lanes = conv.shape[1]
    log_decay = jax.nn.sigmoid(logits[:, :lanes]) * rate
    decay = jnp.exp(log_decay)
    z = -2.0 * log_decay
    series = z * (1.0 - z * (1 / 2) * (1.0 - z * (1 / 3) * (1.0 - z * (1 / 4) * (1.0 - z * (1 / 5)))))
    power = jnp.where(z < 0.1, series, 1.0 - decay * decay)
    return decay, jnp.sqrt(power) * jax.nn.sigmoid(logits[:, lanes:]) * conv.astype(F32)


def mixer_group(x_branch, gate, taps, maps, rate):
    length, count = x_branch.shape[0], taps.shape[0]
    total = taps[count - 1 : count, :] * x_branch
    for tap in range(count - 1):
        total += taps[tap : tap + 1, :] * shifted(x_branch, count - 1 - tap, 0.0)
    conv = total.astype(BF16)
    logits = lax.dot_general(conv, maps, (((1,), (1,)), ((), ())), preferred_element_type=F32)
    decay, state = log_decay_and_drive(conv, logits, rate)
    distance = 1
    while distance < length:
        state = state + decay * shifted(state, distance, 0.0)
        decay = decay * shifted(decay, distance, 1.0)
        distance *= 2
    return (state * jax.nn.gelu(gate)).astype(BF16)


def softplus_of_negative(values):
    small = jnp.exp(-jnp.abs(values))
    series = jnp.zeros_like(small)
    for term in range(8, 0, -1):
        series = small * (1.0 / term - series)
    return jnp.maximum(-values, 0.0) + jnp.where(small < 0.1, series, jnp.log(1.0 + small))


def aligned(start, unit):
    return pl.multiple_of(start, unit)


def layer_kernel(
    shards, tokens, mix_pre, mix_post, mlp_pre, mlp_post, out_scale, down_scale,
    x_scale, gate_scale, up_scale, conv_weight, recur_map, input_map, decay_param,
    x_weight, gate_weight, out_weight, up_weight, down_weight, out,
    b_full, o_full, u_full, d_full, b_give, o_give, u_give, d_give,
    x_raw, gate_raw, o_raw, u_raw, d_raw, gains_full, gain_rows, scales, maps, rate,
    tok_got, normed, branches, mixed, mlp_in, active, hidden,
    give, got_near, keep, total, stage, got_far,
    raw_sem, y_sent, y_land, z_sent, z_land, zf_sent, x_sent, x_land, g_sent, g_land,
    t_sent, t_land, n_sent, n_land, f_sent, f_land, m_sent, m_land, mn_sent, mn_land, mf_sent, mf_land,
):
    lines = shards // 2
    others = lines - 1
    rep, me, core = lax.axis_index("rep"), lax.axis_index("fs"), lax.axis_index("tp")
    z, y = me // 2, lax.rem(me, 2)
    x_peer, core_peer, y_peer = {"rep": 1 - rep}, {"tp": 1 - core}, {"fs": z * 2 + 1 - y}
    upper = z // (lines // 2)
    depth = z + upper * (lines - 1 - 2 * z)
    inner = (depth + lines - 1) // lines

    def other(k):
        turned = lax.rem(k + inner * (others - 1), others)
        place = turned + (turned + lines - depth) // lines
        return place + upper * (lines - 1 - 2 * place)

    seq, width = tokens.shape
    share = seq // 2
    columns = branches.shape[1]
    channels = columns // 2
    units = active.shape[1]
    gives = (b_give, o_give, u_give, d_give)
    fulls = (b_full, o_full, u_full, d_full)

    raw_copies = [
        pltpu.make_async_copy(x_weight, x_raw, raw_sem.at[0]),
        pltpu.make_async_copy(gate_weight, gate_raw, raw_sem.at[1]),
        pltpu.make_async_copy(out_weight, o_raw, raw_sem.at[2]),
        pltpu.make_async_copy(up_weight, u_raw, raw_sem.at[3]),
        pltpu.make_async_copy(down_weight, d_raw, raw_sem.at[4]),
    ]
    for copy in raw_copies:
        copy.start()
    peers = [{"fs": lax.rem(me + step, shards)} for step in range(1, shards)] + [x_peer, core_peer]
    barrier = pltpu.get_barrier_semaphore()
    for peer in peers:
        pl.semaphore_signal(barrier, inc=1, device_id=peer, device_id_type=MESH_IDS)
    for row, gain in enumerate((mix_pre, mix_post, mlp_pre, mlp_post)):
        gains_full[me, row : row + 1, :] = gain[...]
    chunk = 32

    def cast(count, move):
        def body(index, carry):
            move(aligned(index * chunk, chunk))
            return carry

        lax.fori_loop(0, count // chunk, body, 0)

    def branch_rows(start):
        rows = pl.ds(start, chunk)
        home = pl.ds(aligned(me * b_give.shape[0] + start, chunk), chunk)
        for at, raw in enumerate((x_raw, gate_raw)):
            place = pl.ds(at * channels, channels)
            b_full[home, place] = raw[rows, pl.ds(aligned(y * channels, LANES), channels)].astype(BF16)
            b_give[rows, place] = raw[rows, pl.ds(aligned((1 - y) * channels, LANES), channels)].astype(BF16)

    def up_rows_cast(start):
        rows = pl.ds(start, chunk)
        home = pl.ds(aligned(me * u_give.shape[0] + start, chunk), chunk)
        u_full[home, :] = u_raw[rows, pl.ds(aligned(y * units, LANES), units)].astype(BF16)
        u_give[rows, :] = u_raw[rows, pl.ds(aligned((1 - y) * units, LANES), units)].astype(BF16)

    def column_rows(full, spare, raw, scale):
        size = spare.shape[0]

        def move(start):
            home = pl.ds(aligned(me * size + start, chunk), chunk)
            full[home, :] = (raw[pl.ds(aligned(y * size + start, chunk), chunk), :] * scale[...]).astype(BF16)
            rows = pl.ds(start, chunk)
            spare[rows, :] = (raw[pl.ds(aligned((1 - y) * size + start, chunk), chunk), :] * scale[...]).astype(BF16)

        return move

    def half(w, slot, side):
        rows = gives[w].shape[0]
        return fulls[w].at[pl.ds(aligned(slot * rows + side * (rows // 2), 64), rows // 2)]

    def whole(w, slot):
        rows = gives[w].shape[0]
        return fulls[w].at[pl.ds(aligned(slot * rows, 64), rows)]

    def y_copy(w):
        return push(gives[w], whole(w, me), y_sent.at[w], y_land.at[w], y_peer)

    def y_arrival(w):
        block = whole(w, z * 2 + 1 - y)
        return push(block, block, y_sent.at[w], y_land.at[w], y_peer)

    def z_copy(w, kind, k):
        slot = z * 2 + lax.rem(y + kind, 2)
        block = half(w, slot, rep)
        return push(block, block, z_sent.at[w, kind, k], z_land.at[w, slot], {"fs": other(k) * 2 + y})

    def start_z(w, kind):
        z_copy(w, kind, 1).start()
        z_copy(w, kind, 0).start()
        for k in range(2, others):

            @pl.when((inner == 1) | (k < others - 1))
            def _():
                z_copy(w, kind, k).start()

    def item_slot(kind, k):
        return other(k) * 2 + lax.rem(y + kind, 2)

    def zf_copy(w, kind):
        slot = item_slot(kind, 0)
        block = half(w, slot, rep)
        return push(block, block, zf_sent.at[w, kind], z_land.at[w, slot], {"fs": upper * (lines - 1) * 2 + y})

    def x_copy(w, kind, k):
        slot = item_slot(kind, k)
        block = half(w, slot, rep)
        return push(block, block, x_sent.at[w, kind, k], x_land.at[w, slot], x_peer)

    def serve(w, item):
        kind, k = item // others, lax.rem(item, others)
        slot = item_slot(kind, k)
        block = half(w, slot, rep)
        push(block, block, x_sent.at[w, kind, k], z_land.at[w, slot], x_peer).wait_recv()

        @pl.when((k == 0) & (depth == 1))
        def _():
            zf_copy(w, kind).start()

        x_copy(w, kind, k).start()

    def x_arrival(w, item):
        slot = item_slot(item // others, lax.rem(item, others))
        block = half(w, slot, 1 - rep)
        push(block, block, x_sent.at[w, 0, 0], x_land.at[w, slot], x_peer).wait_recv()

    items = 2 * others

    def all_x_arrivals(w):
        def body(index, carry):
            x_arrival(w, index)
            return carry

        lax.fori_loop(0, items, body, 0)

    def when(condition, act):
        pl.when(condition)(act)

    mine = pl.ds(aligned(core * share, 64), share)
    t_near = push(tokens.at[mine], tok_got.at[mine], t_sent.at[0], t_land.at[0], y_peer)
    t_pass = push(tok_got.at[mine], tok_got.at[mine], t_sent.at[1], t_land.at[1], core_peer)

    def gain_copy(step):
        block = gains_full.at[me]
        return push(block, block, g_sent.at[step - 1], g_land.at[me], {"fs": lax.rem(me + step, shards)})

    raw_copies[0].wait()
    raw_copies[1].wait()
    cast(b_give.shape[0], branch_rows)
    pl.semaphore_wait(barrier, len(peers))
    y_copy(0).start()
    start_z(0, 0)
    for step in range(1, shards):
        gain_copy(step).start()
    raw_copies[2].wait()
    cast(o_give.shape[0], column_rows(o_full, o_give, o_raw, out_scale))
    raw_copies[3].wait()
    cast(u_give.shape[0], up_rows_cast)
    raw_copies[4].wait()
    cast(d_give.shape[0], column_rows(d_full, d_give, d_raw, down_scale))
    y_copy(1).start()
    t_near.start()
    y_copy(2).start()
    y_copy(3).start()

    part = pl.ds(aligned(y * channels, LANES), channels)
    scales[:, :channels] = x_scale[:, part]
    scales[:, channels:] = gate_scale[:, part]
    rate[...] = -DECAY_SCALE * softplus_of_negative(decay_param[:, part])
    block_rows = recur_map.shape[0]
    groups = channels // LANES
    same = (
        lax.broadcasted_iota(jnp.int32, (LANES, LANES), 0) // block_rows
        == lax.broadcasted_iota(jnp.int32, (LANES, LANES), 1) // block_rows
    )
    for group in range(groups):
        lanes = pl.ds(aligned(y * channels + group * LANES, LANES), LANES)
        for at, block_map in enumerate((recur_map, input_map)):
            spread = jnp.concatenate([block_map[:, lanes].astype(F32)] * (LANES // block_rows), axis=0)
            first = (group * 2 + at) * LANES
            maps[first : first + LANES, :] = jnp.where(same, spread, 0.0).astype(BF16)

    for step in range(1, shards):
        source = lax.rem(me + step, shards)
        block = gains_full.at[source]
        push(block, block, g_sent.at[step - 1], g_land.at[source], y_peer).wait_recv()
    piece_cols = width // shards
    for block in range(shards):
        gain_rows[:, block * piece_cols : (block + 1) * piece_cols] = gains_full[block]

    rows = 16

    def normalize(source, base):
        def body(index, carry):
            start = aligned(index * rows, rows)
            values = source[pl.ds(start, rows), :].astype(F32)
            values = unit_rows(values) * gain_rows[0:1, :]
            normed[pl.ds(aligned(base + start, rows), rows), :] = values.astype(BF16)
            return carry

        lax.fori_loop(0, seq // rows, body, 0)

    normalize(tokens, 0)
    serve(0, 0)
    y_arrival(0).wait_recv()
    start_z(0, 1)
    start_z(1, 0)
    serve(0, 1)
    serve(0, 2)
    y_arrival(1).wait_recv()
    start_z(1, 1)
    serve(0, 3)
    serve(0, 4)
    serve(0, 5)
    t_near.wait_recv()
    t_pass.start()
    all_x_arrivals(0)

    col_tiles = columns // PIECE

    def branch_step(index, carry):
        row = aligned((index // col_tiles) * seq, 64)
        col = aligned(lax.rem(index, col_tiles) * PIECE, PIECE)
        value = jnp.dot(normed[pl.ds(row, seq), :], b_full[:, pl.ds(col, PIECE)], preferred_element_type=F32)
        branches[pl.ds(row, seq), pl.ds(col, PIECE)] = (value * scales[:, pl.ds(col, PIECE)]).astype(BF16)
        when(index >= 2, lambda: serve(1, index - 2))
        return carry

    lax.fori_loop(0, col_tiles, branch_step, 0)
    t_pass.wait_recv()
    normalize(tok_got, seq)
    lax.fori_loop(col_tiles, 2 * col_tiles, branch_step, 0)
    start_z(2, 0)

    def up_sends():
        y_arrival(2).wait_recv()
        start_z(2, 1)

    def mixer_step(index, carry):
        row = aligned((index // groups) * seq, 64)
        group = lax.rem(index, groups)
        col = aligned(group * LANES, LANES)
        lanes = pl.ds(col, LANES)
        mixed[pl.ds(row, seq), lanes] = mixer_group(
            branches[pl.ds(row, seq), lanes].astype(F32),
            branches[pl.ds(row, seq), pl.ds(aligned(channels + col, LANES), LANES)].astype(F32),
            conv_weight[:, pl.ds(aligned(y * channels + col, LANES), LANES)],
            maps[pl.ds(aligned(group * 2 * LANES, LANES), 2 * LANES), :], rate[:, lanes],
        )
        when(index == groups, up_sends)
        when(index == 2 * groups - 2, lambda: serve(2, 0))
        return carry

    lax.fori_loop(0, 2 * groups, mixer_step, 0)

    def block_of(index):
        item = index - 2
        safe = lax.rem(item + items, items)
        far = item_slot(safe // others, lax.rem(safe, others))
        near = z * 2 + lax.rem(y + index, 2)
        late = (index + shards - 2) // shards
        return near + late * (far - near)

    def near_copy(phase, block):
        return push(give.at[block], got_near.at[block], n_sent.at[phase, block], n_land.at[phase, block], core_peer)

    def far_copy(phase, block):
        return push(stage.at[block], got_far.at[block], f_sent.at[phase, block], f_land.at[phase, block], y_peer)

    def project(phase, w, lhs, before):
        depth_rows = gives[w].shape[0]

        def combine(index):
            block = block_of(index)
            near_copy(phase, block).wait_recv()
            stage[block] = (keep[block] + got_near[block, 1].astype(F32)).astype(BF16)
            total[block] += got_near[block, 0].astype(F32)
            far_copy(phase, block).start()

        def body(index, carry):
            before(index)
            block = block_of(index)
            weight = fulls[w][pl.ds(aligned(block * depth_rows, 64), depth_rows), :]
            for side in range(2):
                left = lhs[pl.ds(aligned(side * seq + (1 - core) * share, 64), share), :]
                give[block, side] = jnp.dot(left, weight, preferred_element_type=F32).astype(BF16)
            own = lhs[pl.ds(aligned(core * share, 64), share), :]
            total[block] = jnp.dot(own, weight, preferred_element_type=F32)
            near_copy(phase, block).start()
            own = lhs[pl.ds(aligned(seq + core * share, 64), share), :]
            keep[block] = jnp.dot(own, weight, preferred_element_type=F32)
            when(index > 0, lambda: combine(index - 1))
            return carry

        lax.fori_loop(0, shards, body, 0)
        combine(shards - 1)

    def collect(phase, between):
        def body(index, carry):
            block = block_of(index)
            far_copy(phase, block).wait_recv()
            total[block] += got_far[block].astype(F32)
            between(index)
            return carry

        lax.fori_loop(0, shards, body, 0)

        def drain(index, carry):
            far_copy(phase, index).wait_send()
            near_copy(phase, index).wait_send()
            return carry

        lax.fori_loop(0, shards, drain, 0)

    def during_sum(index):
        when(index == 1, lambda: serve(2, 2))

        @pl.when(index == 5)
        def _():
            serve(2, 3)
            start_z(3, 0)

    all_x_arrivals(1)
    project(0, 1, mixed, lambda index: when(index == 4, lambda: serve(2, 1)))
    collect(0, during_sum)

    def summed(start):
        values = [total[block, pl.ds(start, rows), :] for block in range(shards)]
        squares = sum(jnp.sum(value * value, axis=-1, keepdims=True) for value in values)
        return values, lax.rsqrt(squares * (1.0 / width) + EPSILON)

    pieces = m_sent.shape[0]
    piece_rows = share // pieces

    def piece(ref, base, index):
        return ref.at[pl.ds(aligned(base + index * piece_rows, 16), piece_rows)]

    def to_far(index):
        return push(
            piece(mlp_in, core * share, index), piece(mlp_in, seq + core * share, index),
            m_sent.at[index], m_land.at[index], y_peer,
        )

    def to_near(index):
        block = piece(mlp_in, core * share, index)
        return push(block, block, mn_sent.at[index], mn_land.at[index], core_peer)

    def onward(index):
        block = piece(mlp_in, seq + core * share, index)
        return push(block, block, mf_sent.at[index], mf_land.at[index], core_peer)

    def entry_piece(index, carry):
        def entry_rows(inner_index, inner_carry):
            start = aligned(index * piece_rows + inner_index * rows, rows)
            values, factor = summed(start)
            place = aligned(core * share + start, rows)
            squares = jnp.zeros((rows, 1), F32)
            kept = []
            for block in range(shards):
                cols = pl.ds(block * piece_cols, piece_cols)
                value = tokens[pl.ds(place, rows), cols].astype(F32) + values[block] * factor * gain_rows[1:2, cols]
                value = value.astype(BF16)
                hidden[pl.ds(start, rows), cols] = value
                value = value.astype(F32)
                kept.append(value)
                squares += jnp.sum(value * value, axis=-1, keepdims=True)
            scale = lax.rsqrt(squares * (1.0 / width) + EPSILON)
            for block in range(shards):
                cols = pl.ds(block * piece_cols, piece_cols)
                mlp_in[pl.ds(place, rows), cols] = (kept[block] * scale * gain_rows[2:3, cols]).astype(BF16)
            return inner_carry

        lax.fori_loop(0, piece_rows // rows, entry_rows, 0)
        to_far(index).start()
        to_near(index).start()
        return carry

    lax.fori_loop(0, pieces, entry_piece, 0)
    serve(2, 4)
    y_arrival(3).wait_recv()
    start_z(3, 1)
    serve(2, 5)
    all_x_arrivals(2)

    def wait_near(index, carry):
        to_near(index).wait_recv()
        return carry

    lax.fori_loop(0, pieces, wait_near, 0)
    up_tiles = units // PIECE

    def up_rows(base):
        def body(index, carry):
            col = aligned(index * PIECE, PIECE)
            value = jnp.dot(mlp_in[pl.ds(base, seq), :], u_full[:, pl.ds(col, PIECE)], preferred_element_type=F32)
            value = jnp.maximum(value * up_scale[:, pl.ds(aligned(y * units + col, PIECE), PIECE)], 0.0)
            active[pl.ds(base, seq), pl.ds(col, PIECE)] = (value * value).astype(BF16)
            return carry

        lax.fori_loop(0, up_tiles, body, 0)

    up_rows(0)
    serve(3, 0)

    def pass_on(index, carry):
        to_far(index).wait_recv()
        onward(index).start()
        return carry

    lax.fori_loop(0, pieces, pass_on, 0)
    serve(3, 1)

    def wait_far(index, carry):
        onward(index).wait_recv()
        return carry

    lax.fori_loop(0, pieces, wait_far, 0)
    up_rows(seq)

    def before_down(index):
        when((index >= 2) & (index < items), lambda: serve(3, index))
        when(index >= 2, lambda: x_arrival(3, index - 2))

    project(1, 3, active, before_down)
    collect(1, lambda index: None)

    def last_rows(index, carry):
        start = aligned(index * rows, rows)
        values, factor = summed(start)
        for block in range(shards):
            cols = pl.ds(block * piece_cols, piece_cols)
            value = hidden[pl.ds(start, rows), cols].astype(F32) + values[block] * factor * gain_rows[3:4, cols]
            out[pl.ds(start, rows), cols] = value.astype(BF16)
        return carry

    lax.fori_loop(0, share // rows, last_rows, 0)

    for w in range(WEIGHTS):
        y_copy(w).wait_send()
        for kind in range(2):
            for k in range(others):
                x_copy(w, kind, k).wait_send()

                @pl.when((inner == 1) | (k < others - 1))
                def _():
                    z_copy(w, kind, k).wait_send()

            @pl.when(depth == 1)
            def _():
                zf_copy(w, kind).wait_send()

    t_near.wait_send()
    t_pass.wait_send()
    for step in range(1, shards):
        gain_copy(step).wait_send()

    def drain(index, carry):
        to_far(index).wait_send()
        to_near(index).wait_send()
        onward(index).wait_send()
        return carry

    lax.fori_loop(0, pieces, drain, 0)


def on_device_paired(
    tokens, gain_mix_pre, gain_mix_post, gain_mlp_pre, gain_mlp_post,
    x_weight, gate_weight, x_scale, gate_scale, conv_weight, recur_map, input_map,
    decay_param, out_weight, out_scale, up_weight, up_scale, down_weight, down_scale,
):
    shards = lax.axis_size("fs")
    seq, width = tokens.shape[1:]
    share, lines, pieces = seq // 2, shards // 2, 4
    fan_in, channels, units = x_weight.shape[0], x_weight.shape[1] // 2, up_weight.shape[1] // 2
    piece_cols = width // shards
    dma = pltpu.SemaphoreType.DMA
    vmem = pl.BlockSpec(memory_space=pltpu.VMEM)
    anywhere = pl.BlockSpec(memory_space=pl.ANY)
    part_shapes = ((fan_in, 2 * channels), (channels, piece_cols), (fan_in, units), (units, piece_cols))
    raws = (x_weight, gate_weight, out_weight, up_weight, down_weight)
    rows = [
        value[None] for value in (
            gain_mix_pre, gain_mix_post, gain_mlp_pre, gain_mlp_post, out_scale, down_scale,
            x_scale, gate_scale, up_scale,
        )
    ]
    result = pl.pallas_call(
        functools.partial(layer_kernel, shards),
        out_shape=jax.ShapeDtypeStruct((share, width), BF16),
        in_specs=[vmem] * 14 + [anywhere] * len(raws),
        out_specs=vmem,
        scratch_shapes=[pltpu.VMEM((shards * shape[0], shape[1]), BF16) for shape in part_shapes]
        + [pltpu.VMEM(shape, BF16) for shape in part_shapes]
        + [pltpu.VMEM(raw.shape, F32) for raw in raws]
        + [
            pltpu.VMEM((shards, 4, piece_cols), F32),
            pltpu.VMEM((4, width), F32),
            pltpu.VMEM((1, 2 * channels), F32),
            pltpu.VMEM((2 * channels, LANES), BF16),
            pltpu.VMEM((1, channels), F32),
            pltpu.VMEM((seq, width), BF16),
            pltpu.VMEM((2 * seq, width), BF16),
            pltpu.VMEM((2 * seq, 2 * channels), BF16),
            pltpu.VMEM((2 * seq, channels), BF16),
            pltpu.VMEM((2 * seq, width), BF16),
            pltpu.VMEM((2 * seq, units), BF16),
            pltpu.VMEM((share, width), BF16),
            pltpu.VMEM((shards, 2, share, piece_cols), BF16),
            pltpu.VMEM((shards, 2, share, piece_cols), BF16),
            pltpu.VMEM((shards, share, piece_cols), F32),
            pltpu.VMEM((shards, share, piece_cols), F32),
            pltpu.VMEM((shards, share, piece_cols), BF16),
            pltpu.VMEM((shards, share, piece_cols), BF16),
            dma((len(raws),)), dma((WEIGHTS,)), dma((WEIGHTS,)),
            dma((WEIGHTS, 2, lines - 1)), dma((WEIGHTS, shards)), dma((WEIGHTS, 2)),
            dma((WEIGHTS, 2, lines - 1)), dma((WEIGHTS, shards)),
            dma((shards - 1,)), dma((shards,)),
            dma((2,)), dma((2,)),
            dma((2, shards)), dma((2, shards)), dma((2, shards)), dma((2, shards)),
            dma((pieces,)), dma((pieces,)), dma((pieces,)), dma((pieces,)), dma((pieces,)), dma((pieces,)),
        ],
        compiler_params=pltpu.CompilerParams(
            collective_id=4, has_side_effects=True, vmem_limit_bytes=67_000_000
        ),
        cost_estimate=pl.CostEstimate(flops=20_000_000_000, bytes_accessed=80_000_000, transcendentals=0),
        name="layer",
    )(tokens[0], *rows, conv_weight, recur_map.T, input_map.T, decay_param[None], *raws)
    return result[None]


def solution(mesh):
    in_specs = (
        P(("rep", "fs"), None, None),
        P("fs"), P("fs"), P("fs"), P("fs"),
        P("fs", "tp"), P("fs", "tp"),
        P("tp"), P("tp"),
        P(None, "tp"), P("tp", None), P("tp", None), P("tp"),
        P("tp", "fs"), P("fs"),
        P("fs", "tp"), P("tp"),
        P("tp", "fs"), P("fs"),
    )
    out_specs = P(("rep", "fs"), "tp", None)
    paired = (
        mesh.shape["rep"] == 2 and mesh.shape["tp"] == 2
        and mesh.shape["fs"] % 4 == 0 and mesh.shape["fs"] > 4
    )
    return jax.shard_map(
        on_device_paired if paired else on_device, mesh=mesh, in_specs=in_specs, out_specs=out_specs, check_vma=False
    )
```

```python
import functools

import jax
import jax.numpy as jnp
from jax import lax
from jax.experimental import pallas as pl
from jax.experimental.pallas import tpu as pltpu
from jax.sharding import PartitionSpec as P

BLOCK = 32
LANES = 128
EPSILON = 1e-06
DECAY_SCALE = 8.0
F32 = jnp.float32
BF16 = jnp.bfloat16


def unit_rows(values):
    return values * lax.rsqrt(jnp.mean(values * values, axis=-1, keepdims=True) + EPSILON)


def shifted(values, distance, fill):
    head = jnp.full((distance, values.shape[1]), fill, values.dtype)
    return jnp.concatenate([head, values[: values.shape[0] - distance]], axis=0)


def mixer_kernel(x_ref, gate_ref, taps_ref, recur_ref, input_ref, rate_ref, mixed_ref):
    length = x_ref.shape[0]
    x_branch = x_ref[...].astype(F32)
    taps = taps_ref.shape[0]
    total = taps_ref[taps - 1 : taps, :] * x_branch
    for tap in range(taps - 1):
        total += taps_ref[tap : tap + 1, :] * shifted(x_branch, taps - 1 - tap, 0.0)
    conv = total.astype(BF16)
    recur = jax.nn.sigmoid(jnp.dot(conv, recur_ref[...], preferred_element_type=F32))
    gate_in = jax.nn.sigmoid(jnp.dot(conv, input_ref[...], preferred_element_type=F32))
    log_decay = recur * rate_ref[0:1, :]
    decay = jnp.exp(log_decay)
    z = -2.0 * log_decay
    series = z * (1.0 - z * (1 / 2) * (1.0 - z * (1 / 3) * (1.0 - z * (1 / 4) * (1.0 - z * (1 / 5)))))
    power = jnp.where(z < 0.1, series, 1.0 - decay * decay)
    state = jnp.sqrt(power) * gate_in * conv.astype(F32)
    distance = 1
    while distance < length:
        state = state + decay * shifted(state, distance, 0.0)
        decay = decay * shifted(decay, distance, 1.0)
        distance *= 2
    mixed_ref[...] = (state * jax.nn.gelu(gate_ref[...].astype(F32))).astype(BF16)


def mixer(branches, taps, recur_dense, input_dense, rate, sequences):
    rows, width = branches.shape[0], branches.shape[1] // 2
    length = rows // sequences
    groups = width // LANES
    return pl.pallas_call(
        mixer_kernel,
        grid=(sequences, groups),
        in_specs=[
            pl.BlockSpec((length, LANES), lambda s, g: (s, g)),
            pl.BlockSpec((length, LANES), lambda s, g: (s, g + groups)),
            pl.BlockSpec((taps.shape[0], LANES), lambda s, g: (0, g)),
            pl.BlockSpec((LANES, LANES), lambda s, g: (g, 0)),
            pl.BlockSpec((LANES, LANES), lambda s, g: (g, 0)),
            pl.BlockSpec((1, LANES), lambda s, g: (0, g)),
        ],
        out_specs=pl.BlockSpec((length, LANES), lambda s, g: (s, g)),
        out_shape=jax.ShapeDtypeStruct((rows, width), BF16),
        cost_estimate=pl.CostEstimate(
            flops=rows * width * 100, bytes_accessed=rows * width * 6, transcendentals=rows * width * 4
        ),
        name="mixer",
    )(branches, branches, taps, recur_dense, input_dense, rate)


MESH_IDS = pl.DeviceIdType.MESH


def greet(peers):
    barrier = pltpu.get_barrier_semaphore()
    for peer in peers:
        pl.semaphore_signal(barrier, inc=1, device_id=peer, device_id_type=MESH_IDS)
    pl.semaphore_wait(barrier, len(peers))


def push(source, target, sent, landed, peer):
    return pltpu.make_async_remote_copy(
        src_ref=source, dst_ref=target, send_sem=sent, recv_sem=landed,
        device_id=peer, device_id_type=MESH_IDS,
    )


def others(axis, count):
    me = lax.axis_index(axis)
    return [lax.rem(me + step, count) for step in range(1, count)]


def row_block(ref, index, rows):
    return ref.at[pl.ds(pl.multiple_of(index * rows, rows), rows)]


def team_gather_kernel(reps, tps, x_ref, out_ref, own_sem, sent, landed):
    rep, core = lax.axis_index("rep"), lax.axis_index("tp")
    rows = x_ref.shape[0]
    rep_peers, tp_peers = others("rep", reps), others("tp", tps)
    greet([{"rep": peer} for peer in rep_peers] + [{"tp": peer} for peer in tp_peers])
    mine = row_block(out_ref, rep * tps + core, rows)
    flights = []
    for step, peer in enumerate(rep_peers):
        copy = push(x_ref, mine, sent.at[step + 1, 0], landed.at[step + 1, 0], {"rep": peer})
        copy.start()
        flights.append(copy)
    own = pltpu.make_async_copy(x_ref, mine, own_sem)
    own.start()
    local = []
    for slot, peer in enumerate(tp_peers):
        copy = push(x_ref, mine, sent.at[0, slot + 1], landed.at[0, slot + 1], {"tp": peer})
        copy.start()
        local.append(copy)
    for step in range(1, reps):
        flights[step - 1].wait_recv()
        source = lax.rem(rep + reps - step, reps)
        block = row_block(out_ref, source * tps + core, rows)
        for slot, peer in enumerate(tp_peers):
            copy = push(block, block, sent.at[step, slot + 1], landed.at[step, slot + 1], {"tp": peer})
            copy.start()
            local.append(copy)
    for copy in flights:
        copy.wait_send()
    for copy in local:
        copy.wait()
    own.wait()


def team_gather(values):
    reps, tps = lax.axis_size("rep"), lax.axis_size("tp")
    rows, width = values.shape
    return pl.pallas_call(
        functools.partial(team_gather_kernel, reps, tps),
        out_shape=jax.ShapeDtypeStruct((rows * reps * tps, width), values.dtype),
        in_specs=[pl.BlockSpec(memory_space=pltpu.VMEM)],
        out_specs=pl.BlockSpec(memory_space=pltpu.VMEM),
        scratch_shapes=[
            pltpu.SemaphoreType.DMA,
            pltpu.SemaphoreType.DMA((reps, tps)),
            pltpu.SemaphoreType.DMA((reps, tps)),
        ],
        compiler_params=pltpu.CompilerParams(collective_id=0, has_side_effects=True),
        cost_estimate=pl.CostEstimate(flops=0, bytes_accessed=80_000_000, transcendentals=0),
        name="team_gather",
    )(values)


def team_sum_kernel(reps, tps, part_ref, out_ref, got, stage, last, sent, landed, sent_far, landed_far):
    rep, core = lax.axis_index("rep"), lax.axis_index("tp")
    rows = out_ref.shape[0]
    step_rows = 16
    rep_peers, tp_peers = others("rep", reps), others("tp", tps)
    greet([{"rep": peer} for peer in rep_peers] + [{"tp": peer} for peer in tp_peers])
    near = []
    for slot, peer in enumerate(tp_peers):
        for group in range(reps):
            copy = push(
                row_block(part_ref, group * tps + peer, rows), got.at[slot, group],
                sent.at[slot, group], landed.at[slot, group], {"tp": peer},
            )
            copy.start()
            near.append(copy)
    for copy in near:
        copy.wait()

    def total(group, start):
        base = pl.multiple_of((group * tps + core) * rows + start, step_rows)
        value = part_ref[pl.ds(base, step_rows)].astype(F32)
        for slot in range(tps - 1):
            value += got[slot, group, pl.ds(start, step_rows)].astype(F32)
        return value

    far = []
    for step, peer in enumerate(rep_peers):

        def fill(index, carry):
            start = pl.multiple_of(index * step_rows, step_rows)
            stage[step, pl.ds(start, step_rows)] = total(peer, start).astype(BF16)
            return carry

        lax.fori_loop(0, rows // step_rows, fill, 0)
        copy = push(stage.at[step], last.at[step], sent_far.at[step], landed_far.at[step], {"rep": peer})
        copy.start()
        far.append(copy)
    for copy in far:
        copy.wait()

    def finish(index, carry):
        start = pl.multiple_of(index * step_rows, step_rows)
        value = total(rep, start)
        for step in range(reps - 1):
            value += last[step, pl.ds(start, step_rows)].astype(F32)
        out_ref[pl.ds(start, step_rows)] = value
        return carry

    lax.fori_loop(0, rows // step_rows, finish, 0)


def team_sum(parts):
    reps, tps = lax.axis_size("rep"), lax.axis_size("tp")
    rows, width = parts.shape[0] // (reps * tps), parts.shape[1]
    return pl.pallas_call(
        functools.partial(team_sum_kernel, reps, tps),
        out_shape=jax.ShapeDtypeStruct((rows, width), F32),
        in_specs=[pl.BlockSpec(memory_space=pltpu.VMEM)],
        out_specs=pl.BlockSpec(memory_space=pltpu.VMEM),
        scratch_shapes=[
            pltpu.VMEM((tps - 1, reps, rows, width), BF16),
            pltpu.VMEM((reps - 1, rows, width), BF16),
            pltpu.VMEM((reps - 1, rows, width), BF16),
            pltpu.SemaphoreType.DMA((tps - 1, reps)),
            pltpu.SemaphoreType.DMA((tps - 1, reps)),
            pltpu.SemaphoreType.DMA((reps - 1,)),
            pltpu.SemaphoreType.DMA((reps - 1,)),
        ],
        compiler_params=pltpu.CompilerParams(collective_id=1, has_side_effects=True),
        cost_estimate=pl.CostEstimate(flops=0, bytes_accessed=80_000_000, transcendentals=0),
        name="team_sum",
    )(parts)


def shard_gather_kernel(shards, x_ref, out_ref, own_sem, sent, landed, sent_pass, landed_pass):
    me = lax.axis_index("fs")
    rows = x_ref.shape[0]
    pairs = shards // 2
    pair, parity = me // 2, lax.rem(me, 2)
    partner = {"fs": pair * 2 + 1 - parity}
    peers = [{"fs": lax.rem(pair + step, pairs) * 2 + parity} for step in range(1, pairs)]
    greet([partner] + peers)
    mine = row_block(out_ref, me, rows)
    passed = [push(x_ref, mine, sent_pass.at[0], landed_pass.at[0], partner)]
    passed[0].start()
    direct = []
    for step, peer in enumerate(peers):
        copy = push(x_ref, mine, sent.at[step], landed.at[step], peer)
        copy.start()
        direct.append(copy)
    own = pltpu.make_async_copy(x_ref, mine, own_sem)
    own.start()
    for step in range(1, pairs):
        direct[step - 1].wait_recv()
        block = row_block(out_ref, lax.rem(pair + pairs - step, pairs) * 2 + parity, rows)
        copy = push(block, block, sent_pass.at[step], landed_pass.at[step], partner)
        copy.start()
        passed.append(copy)
    for copy in direct:
        copy.wait_send()
    for copy in passed:
        copy.wait()
    own.wait()


def shard_gather(values, collective_id):
    shards = lax.axis_size("fs")
    rows, width = values.shape
    return pl.pallas_call(
        functools.partial(shard_gather_kernel, shards),
        out_shape=jax.ShapeDtypeStruct((rows * shards, width), values.dtype),
        in_specs=[pl.BlockSpec(memory_space=pltpu.VMEM)],
        out_specs=pl.BlockSpec(memory_space=pltpu.VMEM),
        scratch_shapes=[
            pltpu.SemaphoreType.DMA,
            pltpu.SemaphoreType.DMA((shards // 2,)),
            pltpu.SemaphoreType.DMA((shards // 2,)),
            pltpu.SemaphoreType.DMA((shards // 2,)),
            pltpu.SemaphoreType.DMA((shards // 2,)),
        ],
        compiler_params=pltpu.CompilerParams(collective_id=collective_id, has_side_effects=True),
        cost_estimate=pl.CostEstimate(flops=0, bytes_accessed=200_000_000, transcendentals=0),
        name="shard_gather",
    )(values)


def on_device(
    tokens, gain_mix_pre, gain_mix_post, gain_mlp_pre, gain_mlp_post,
    x_weight, gate_weight, x_scale, gate_scale, conv_weight, recur_map, input_map,
    decay_param, out_weight, out_scale, up_weight, up_scale, down_weight, down_scale,
):
    reps = lax.axis_size("rep")
    rep = lax.axis_index("rep")

    def part(values, axis):
        size = values.shape[axis] // reps
        return lax.dynamic_slice_in_dim(values, rep * size, size, axis)

    length = tokens.shape[1]
    share_rows = length // lax.axis_size("tp")
    offset_row = lax.axis_index("tp") * share_rows
    resid_share = lax.dynamic_slice_in_dim(tokens[0], offset_row, share_rows, 0).astype(F32)
    normed_share = unit_rows(resid_share).astype(BF16)

    pre = gain_mix_pre[:, None]
    branch_rows = jnp.concatenate(
        [(part(x_weight, 1) * pre).astype(BF16), (part(gate_weight, 1) * pre).astype(BF16)], axis=1
    )
    branch_rows, out_weight = lax.optimization_barrier((branch_rows, out_weight))
    branch_full = lax.all_gather(branch_rows, "fs", axis=0, tiled=True)
    post = jnp.stack([gain_mix_post, gain_mlp_post])
    post_high = post.astype(BF16)
    post_low = (post - post_high.astype(F32)).astype(BF16)
    pad_rows = jnp.zeros((12, post.shape[1]), BF16)
    out_cols = jnp.concatenate(
        [(part(out_weight, 0) * out_scale).astype(BF16), post_high, post_low, pad_rows], axis=0
    )
    out_cols, down_weight = lax.optimization_barrier((out_cols, down_weight))
    out_all = lax.all_gather(out_cols, "fs", axis=1, tiled=True)
    down_full = lax.all_gather((part(down_weight, 0) * down_scale).astype(BF16), "fs", axis=1, tiled=True)
    up_rows = (part(up_weight, 1) * gain_mlp_pre[:, None]).astype(BF16)
    normed = team_gather(normed_share)
    normed, up_rows = lax.optimization_barrier((normed, up_rows))
    up_full = shard_gather(up_rows, 2)
    normed, up_full = lax.optimization_barrier((normed, up_full))

    scales = jnp.concatenate([part(x_scale, 0), part(gate_scale, 0)])
    branches = (jnp.dot(normed, branch_full, preferred_element_type=F32) * scales).astype(BF16)
    width = branches.shape[1] // 2

    def dense(block_map):
        rows = lax.broadcasted_iota(jnp.int32, (width, LANES), 0)
        columns = lax.broadcasted_iota(jnp.int32, (width, LANES), 1)
        spread = jnp.tile(part(block_map, 0), (1, LANES // BLOCK))
        return jnp.where(rows % LANES // BLOCK == columns // BLOCK, spread, 0).astype(BF16)

    rate = -DECAY_SCALE * jax.nn.softplus(-part(decay_param, 0))
    mixed = mixer(
        branches, part(conv_weight, 1), dense(recur_map), dense(input_map), rate[None], reps
    )
    out_full = out_all[:width]
    gains = out_all[width : width + 2].astype(F32) + out_all[width + 2 : width + 4].astype(F32)
    mix_share = team_sum(jnp.dot(mixed, out_full, preferred_element_type=F32).astype(BF16))
    hidden_state = (resid_share + unit_rows(mix_share) * gains[0]).astype(BF16)
    mlp_input = team_gather(unit_rows(hidden_state.astype(F32)).astype(BF16))
    up_proj = jnp.dot(mlp_input, up_full, preferred_element_type=F32)
    activated = jnp.square(jax.nn.relu(up_proj * part(up_scale, 0))).astype(BF16)
    mlp_share = team_sum(jnp.dot(activated, down_full, preferred_element_type=F32).astype(BF16))
    return (hidden_state.astype(F32) + unit_rows(mlp_share) * gains[1]).astype(BF16)[None]


WEIGHTS = 4
PIECE = 256
CUTS = 2


def log_decay_and_drive(conv, logits, rate):
    lanes = conv.shape[1]
    log_decay = jax.nn.sigmoid(logits[:, :lanes]) * rate
    decay = jnp.exp(log_decay)
    z = -2.0 * log_decay
    series = z * (1.0 - z * (1 / 2) * (1.0 - z * (1 / 3) * (1.0 - z * (1 / 4) * (1.0 - z * (1 / 5)))))
    power = jnp.where(z < 0.1, series, 1.0 - decay * decay)
    return decay, jnp.sqrt(power) * jax.nn.sigmoid(logits[:, lanes:]) * conv.astype(F32)


def mixer_group(x_branch, gate, taps, maps, rate):
    length, count = x_branch.shape[0], taps.shape[0]
    total = taps[count - 1 : count, :] * x_branch
    for tap in range(count - 1):
        total += taps[tap : tap + 1, :] * shifted(x_branch, count - 1 - tap, 0.0)
    conv = total.astype(BF16)
    logits = lax.dot_general(conv, maps, (((1,), (1,)), ((), ())), preferred_element_type=F32)
    decay, state = log_decay_and_drive(conv, logits, rate)
    distance = 1
    while distance < length:
        state = state + decay * shifted(state, distance, 0.0)
        decay = decay * shifted(decay, distance, 1.0)
        distance *= 2
    return (state * jax.nn.gelu(gate)).astype(BF16)


def softplus_of_negative(values):
    small = jnp.exp(-jnp.abs(values))
    series = jnp.zeros_like(small)
    for term in range(8, 0, -1):
        series = small * (1.0 / term - series)
    return jnp.maximum(-values, 0.0) + jnp.where(small < 0.1, series, jnp.log(1.0 + small))


def aligned(start, unit):
    return pl.multiple_of(start, unit)


def layer_kernel(shards, *refs):
    count = 14
    sources, raws, out = refs[:count], refs[count : count + 5], refs[count + 5]
    copies = refs[count + 6 : 2 * count + 6]
    load_sem = refs[2 * count + 6]
    loads = [
        pltpu.make_async_copy(source, copy, load_sem.at[at])
        for at, (source, copy) in enumerate(zip(sources, copies, strict=True))
    ]
    layer_body(shards, loads, *copies, *raws, out, *refs[2 * count + 7 :])


def layer_body(
    shards, loads, tokens, mix_pre, mix_post, mlp_pre, mlp_post, out_scale, down_scale,
    x_scale, gate_scale, up_scale, conv_weight, recur_map, input_map, decay_param,
    x_weight, gate_weight, out_weight, up_weight, down_weight, out,
    b_full, o_full, u_full, d_full, b_give, o_give, u_give, d_give,
    x_raw, gate_raw, o_raw, u_raw, d_raw, gains_full, gain_rows, scales, maps, rate,
    tok_got, normed, branches, mixed, mlp_in, active, hidden, result,
    give, got_near, keep, total, stage, got_far,
    raw_sem, y_sent, y_land, z_sent, z_land, zf_sent, x_sent, x_land, g_sent, g_land,
    t_sent, t_land, n_sent, n_land, f_sent, f_land, m_sent, m_land, mn_sent, mn_land, mf_sent, mf_land, out_sem,
):
    lines = shards // 2
    others = lines - 1
    rep, me, core = lax.axis_index("rep"), lax.axis_index("fs"), lax.axis_index("tp")
    z, y = me // 2, lax.rem(me, 2)
    x_peer, core_peer, y_peer = {"rep": 1 - rep}, {"tp": 1 - core}, {"fs": z * 2 + 1 - y}
    upper = z // (lines // 2)
    depth = z + upper * (lines - 1 - 2 * z)
    inner = (depth + lines - 1) // lines

    def unfold(place):
        return place + upper * (lines - 1 - 2 * place)

    def early(k):
        return 1 - (k + 2 * lines - 2 * depth) // (2 * lines)

    def other(k):
        near = depth + (1 - 2 * lax.rem(k, 2)) * (k // 2 + 1)
        return unfold(k + 1 + early(k) * (near - k - 1))

    seq, width = tokens.shape
    share = seq // 2
    columns = branches.shape[1]
    channels = columns // 2
    units = active.shape[1]
    gives = (b_give, o_give, u_give, d_give)
    fulls = (b_full, o_full, u_full, d_full)

    raw_copies = [
        pltpu.make_async_copy(x_weight, x_raw, raw_sem.at[0]),
        pltpu.make_async_copy(gate_weight, gate_raw, raw_sem.at[1]),
        pltpu.make_async_copy(out_weight, o_raw, raw_sem.at[2]),
        pltpu.make_async_copy(up_weight, u_raw, raw_sem.at[3]),
        pltpu.make_async_copy(down_weight, d_raw, raw_sem.at[4]),
    ]
    for copy in raw_copies[:2] + loads[1:] + raw_copies[2:] + loads[:1]:
        copy.start()
    token_copy = loads[0]
    peers = [{"fs": lax.rem(me + step, shards)} for step in range(1, shards)] + [x_peer, core_peer]
    barrier = pltpu.get_barrier_semaphore()
    for peer in peers:
        pl.semaphore_signal(barrier, inc=1, device_id=peer, device_id_type=MESH_IDS)
    for copy in loads[1:]:
        copy.wait()
    for row, gain in enumerate((mix_pre, mix_post, mlp_pre, mlp_post)):
        gains_full[me, row : row + 1, :] = gain[...]
    chunk = 32

    def cast(count, move):
        def body(index, carry):
            move(aligned(index * chunk, chunk))
            return carry

        lax.fori_loop(0, count // chunk, body, 0)

    def branch_rows(start):
        rows = pl.ds(start, chunk)
        home = pl.ds(aligned(me * b_give.shape[0] + start, chunk), chunk)
        for at, raw in enumerate((x_raw, gate_raw)):
            place = pl.ds(at * channels, channels)
            b_full[home, place] = raw[rows, pl.ds(aligned(y * channels, LANES), channels)].astype(BF16)
            b_give[rows, place] = raw[rows, pl.ds(aligned((1 - y) * channels, LANES), channels)].astype(BF16)

    def up_rows_cast(start):
        rows = pl.ds(start, chunk)
        home = pl.ds(aligned(me * u_give.shape[0] + start, chunk), chunk)
        u_full[home, :] = u_raw[rows, pl.ds(aligned(y * units, LANES), units)].astype(BF16)
        u_give[rows, :] = u_raw[rows, pl.ds(aligned((1 - y) * units, LANES), units)].astype(BF16)

    def column_rows(full, spare, raw, scale):
        size = spare.shape[0]

        def move(start):
            home = pl.ds(aligned(me * size + start, chunk), chunk)
            full[home, :] = (raw[pl.ds(aligned(y * size + start, chunk), chunk), :] * scale[...]).astype(BF16)
            rows = pl.ds(start, chunk)
            spare[rows, :] = (raw[pl.ds(aligned((1 - y) * size + start, chunk), chunk), :] * scale[...]).astype(BF16)

        return move

    def half(w, slot, side, cut):
        rows = gives[w].shape[0]
        size = rows // (2 * CUTS)
        return fulls[w].at[pl.ds(aligned(slot * rows + (side * CUTS + cut) * size, 32), size)]

    def whole(w, slot):
        rows = gives[w].shape[0]
        return fulls[w].at[pl.ds(aligned(slot * rows, 64), rows)]

    def y_copy(w):
        return push(gives[w], whole(w, me), y_sent.at[w], y_land.at[w], y_peer)

    def y_arrival(w):
        block = whole(w, z * 2 + 1 - y)
        return push(block, block, y_sent.at[w], y_land.at[w], y_peer)

    def z_copy(w, kind, way, cut):
        slot = z * 2 + lax.rem(y + kind, 2)
        block = half(w, slot, rep, cut)
        target = unfold(depth + 1 - 2 * way)
        return push(block, block, z_sent.at[w, kind, way, cut], z_land.at[w, slot, cut], {"fs": target * 2 + y})

    def start_z(w, kind):
        for cut in range(CUTS):

            @pl.when(inner == 1)
            def _():
                z_copy(w, kind, 1, cut).start()

            z_copy(w, kind, 0, cut).start()

    def item_slot(kind, k):
        return other(k) * 2 + lax.rem(y + kind, 2)

    def zf_copy(w, kind, k, cut):
        slot = item_slot(kind, k)
        block = half(w, slot, rep, cut)
        target = unfold(depth - 1 + 2 * early(k) * lax.rem(k, 2))
        return push(block, block, zf_sent.at[w, kind, k, cut], z_land.at[w, slot, cut], {"fs": target * 2 + y})

    def x_copy(w, kind, k, cut):
        slot = item_slot(kind, k)
        block = half(w, slot, rep, cut)
        return push(block, block, x_sent.at[w, kind, k, cut], x_land.at[w, slot, cut], x_peer)

    def serve(w, item):
        kind, k = item // others, lax.rem(item, others)
        slot = item_slot(kind, k)
        for cut in range(CUTS):
            block = half(w, slot, rep, cut)
            push(block, block, x_sent.at[w, kind, k, cut], z_land.at[w, slot, cut], x_peer).wait_recv()

            @pl.when(inner == 1)
            def _():
                zf_copy(w, kind, k, cut).start()

            x_copy(w, kind, k, cut).start()

    def x_arrival(w, item):
        slot = item_slot(item // others, lax.rem(item, others))
        for cut in range(CUTS):
            block = half(w, slot, 1 - rep, cut)
            push(block, block, x_sent.at[w, 0, 0, cut], x_land.at[w, slot, cut], x_peer).wait_recv()

    items = 2 * others

    def all_x_arrivals(w):
        def body(index, carry):
            x_arrival(w, index)
            return carry

        lax.fori_loop(0, items, body, 0)

    def when(condition, act):
        pl.when(condition)(act)

    mine = pl.ds(aligned(core * share, 64), share)
    t_near = push(tokens.at[mine], tok_got.at[mine], t_sent.at[0], t_land.at[0], y_peer)
    t_pass = push(tok_got.at[mine], tok_got.at[mine], t_sent.at[1], t_land.at[1], core_peer)

    def gain_copy(step):
        block = gains_full.at[me]
        return push(block, block, g_sent.at[step - 1], g_land.at[me], {"fs": lax.rem(me + step, shards)})

    raw_copies[0].wait()
    raw_copies[1].wait()
    cast(b_give.shape[0], branch_rows)
    pl.semaphore_wait(barrier, len(peers))
    for step in range(1, shards):
        gain_copy(step).start()
    y_copy(0).start()
    start_z(0, 0)
    raw_copies[2].wait()
    cast(o_give.shape[0], column_rows(o_full, o_give, o_raw, out_scale))
    raw_copies[3].wait()
    cast(u_give.shape[0], up_rows_cast)
    raw_copies[4].wait()
    cast(d_give.shape[0], column_rows(d_full, d_give, d_raw, down_scale))
    y_copy(1).start()
    token_copy.wait()
    t_near.start()
    y_copy(2).start()
    y_copy(3).start()

    part = pl.ds(aligned(y * channels, LANES), channels)
    scales[:, :channels] = x_scale[:, part]
    scales[:, channels:] = gate_scale[:, part]
    rate[...] = -DECAY_SCALE * softplus_of_negative(decay_param[:, part])
    block_rows = recur_map.shape[0]
    groups = channels // LANES
    same = (
        lax.broadcasted_iota(jnp.int32, (LANES, LANES), 0) // block_rows
        == lax.broadcasted_iota(jnp.int32, (LANES, LANES), 1) // block_rows
    )
    for group in range(groups):
        lanes = pl.ds(aligned(y * channels + group * LANES, LANES), LANES)
        for at, block_map in enumerate((recur_map, input_map)):
            spread = jnp.concatenate([block_map[:, lanes].astype(F32)] * (LANES // block_rows), axis=0)
            first = (group * 2 + at) * LANES
            maps[first : first + LANES, :] = jnp.where(same, spread, 0.0).astype(BF16)

    for step in range(1, shards):
        source = lax.rem(me + step, shards)
        block = gains_full.at[source]
        push(block, block, g_sent.at[step - 1], g_land.at[source], y_peer).wait_recv()
    piece_cols = width // shards
    for block in range(shards):
        gain_rows[:, block * piece_cols : (block + 1) * piece_cols] = gains_full[block]

    rows = 16

    def normalize(source, base):
        def body(index, carry):
            start = aligned(index * rows, rows)
            values = source[pl.ds(start, rows), :].astype(F32)
            values = unit_rows(values) * gain_rows[0:1, :]
            normed[pl.ds(aligned(base + start, rows), rows), :] = values.astype(BF16)
            return carry

        lax.fori_loop(0, seq // rows, body, 0)

    is_inner, is_end = inner == 1, inner == 0

    def start_other(w):
        y_arrival(w).wait_recv()
        start_z(w, 1)

    serve(0, 0)
    serve(0, 1)
    start_other(0)
    when(is_end, lambda: start_z(1, 0))
    normalize(tokens, 0)
    serve(0, 2)

    @pl.when(is_end)
    def _():
        start_other(1)
        start_z(2, 0)

    serve(0, 3)
    serve(0, 4)
    when(is_inner, lambda: start_z(1, 0))
    serve(0, 5)
    serve(1, 0)
    serve(1, 1)

    @pl.when(is_inner)
    def _():
        start_other(1)
        start_z(2, 0)
        serve(1, 2)
        serve(1, 3)
        serve(1, 4)

    all_x_arrivals(0)

    col_tiles = columns // PIECE

    def pass_tokens():
        t_near.wait_recv()
        t_pass.start()

    def branch_step(index, carry):
        row = aligned((index // col_tiles) * seq, 64)
        col = aligned(lax.rem(index, col_tiles) * PIECE, PIECE)
        value = jnp.dot(normed[pl.ds(row, seq), :], b_full[:, pl.ds(col, PIECE)], preferred_element_type=F32)
        branches[pl.ds(row, seq), pl.ds(col, PIECE)] = (value * scales[:, pl.ds(col, PIECE)]).astype(BF16)
        when(index == 0, pass_tokens)
        when(is_inner & (index == 1), lambda: serve(1, 5))

        @pl.when(is_end & (lax.rem(index, 2) == 0))
        def _():
            serve(1, 2 + index // 2)

        return carry

    lax.fori_loop(0, col_tiles, branch_step, 0)
    t_pass.wait_recv()
    normalize(tok_got, seq)
    when(is_end, lambda: start_other(2))
    lax.fori_loop(col_tiles, 2 * col_tiles, branch_step, 0)

    def up_second():
        serve(2, 1)
        start_other(2)

    def mixer_step(index, carry):
        row = aligned((index // groups) * seq, 64)
        group = lax.rem(index, groups)
        col = aligned(group * LANES, LANES)
        lanes = pl.ds(col, LANES)
        mixed[pl.ds(row, seq), lanes] = mixer_group(
            branches[pl.ds(row, seq), lanes].astype(F32),
            branches[pl.ds(row, seq), pl.ds(aligned(channels + col, LANES), LANES)].astype(F32),
            conv_weight[:, pl.ds(aligned(y * channels + col, LANES), LANES)],
            maps[pl.ds(aligned(group * 2 * LANES, LANES), 2 * LANES), :], rate[:, lanes],
        )
        when(is_inner & (index == 3), lambda: serve(2, 0))
        when(is_inner & (index == 4), up_second)
        when(is_end & (index == 1), lambda: serve(2, 0))
        when(is_end & (index == 5), lambda: serve(2, 1))
        return carry

    lax.fori_loop(0, 2 * groups, mixer_step, 0)

    def block_of(index, flip=0):
        item = index - 2
        safe = lax.rem(item + items, items)
        far = item_slot(safe // others + flip, lax.rem(safe, others))
        near = z * 2 + lax.rem(y + index + flip, 2)
        late = (index + shards - 2) // shards
        return near + late * (far - near)

    def near_copy(phase, block):
        return push(give.at[block], got_near.at[block], n_sent.at[phase, block], n_land.at[phase, block], core_peer)

    def far_copy(phase, block):
        return push(stage.at[block], got_far.at[block], f_sent.at[phase, block], f_land.at[phase, block], y_peer)

    def project(phase, w, lhs, lag, before):
        depth_rows = gives[w].shape[0]

        def combine(index):
            block = block_of(index)
            near_copy(phase, block).wait_recv()
            stage[block] = (keep[block] + got_near[block, 1].astype(F32)).astype(BF16)
            total[block] += got_near[block, 0].astype(F32)
            far_copy(phase, block).start()

        def body(index, carry):
            before(index)
            block = block_of(index)
            weight = fulls[w][pl.ds(aligned(block * depth_rows, 64), depth_rows), :]
            for side in range(2):
                left = lhs[pl.ds(aligned(side * seq + (1 - core) * share, 64), share), :]
                give[block, side] = jnp.dot(left, weight, preferred_element_type=F32).astype(BF16)
            own = lhs[pl.ds(aligned(core * share, 64), share), :]
            total[block] = jnp.dot(own, weight, preferred_element_type=F32)
            near_copy(phase, block).start()
            own = lhs[pl.ds(aligned(seq + core * share, 64), share), :]
            keep[block] = jnp.dot(own, weight, preferred_element_type=F32)
            when(index > 0, lambda: combine(index - 1))
            if lag < shards:
                when(index >= lag, lambda: add_far(phase, index - lag))
            return carry

        lax.fori_loop(0, shards, body, 0)
        combine(shards - 1)

    def add_far(phase, index):
        block = block_of(index, 1)
        far_copy(phase, block).wait_recv()
        total[block] += got_far[block].astype(F32)

    def collect(phase, lag, between):
        def body(index, carry):
            add_far(phase, index)
            between(index)
            return carry

        lax.fori_loop(shards - lag, shards, body, 0)

        def drain(index, carry):
            far_copy(phase, index).wait_send()
            near_copy(phase, index).wait_send()
            return carry

        lax.fori_loop(0, shards, drain, 0)

    def during_project(index):
        when(is_inner & (index == 3), lambda: serve(2, 2))
        when(is_end & (index == 3), lambda: start_z(3, 0))

    def last_up():
        serve(2, 5)
        start_z(3, 0)

    def during_sum(index):
        when(is_inner & (index == 0), lambda: serve(2, 3))
        when(is_inner & (index == 1), lambda: serve(2, 4))
        when(is_inner & (index == 4), last_up)
        when(is_end & (index == 0), lambda: serve(2, 2))
        when(is_end & (index == 1), lambda: serve(2, 3))
        when(is_end & (index == 3), lambda: start_other(3))
        when(is_end & (index == 4), lambda: serve(2, 4))

    all_x_arrivals(1)
    project(0, 1, mixed, shards, during_project)
    collect(0, shards, during_sum)

    def summed(start):
        values = [total[block, pl.ds(start, rows), :] for block in range(shards)]
        squares = sum(jnp.sum(value * value, axis=-1, keepdims=True) for value in values)
        return values, lax.rsqrt(squares * (1.0 / width) + EPSILON)

    pieces = m_sent.shape[0]
    piece_rows = share // pieces

    def piece(ref, base, index):
        return ref.at[pl.ds(aligned(base + index * piece_rows, 16), piece_rows)]

    def to_far(index):
        return push(
            piece(mlp_in, core * share, index), piece(mlp_in, seq + core * share, index),
            m_sent.at[index], m_land.at[index], y_peer,
        )

    def to_near(index):
        block = piece(mlp_in, core * share, index)
        return push(block, block, mn_sent.at[index], mn_land.at[index], core_peer)

    def onward(index):
        block = piece(mlp_in, seq + core * share, index)
        return push(block, block, mf_sent.at[index], mf_land.at[index], core_peer)

    def entry_piece(index, carry):
        def entry_rows(inner_index, inner_carry):
            start = aligned(index * piece_rows + inner_index * rows, rows)
            values, factor = summed(start)
            place = aligned(core * share + start, rows)
            squares = jnp.zeros((rows, 1), F32)
            kept = []
            for block in range(shards):
                cols = pl.ds(block * piece_cols, piece_cols)
                value = tokens[pl.ds(place, rows), cols].astype(F32) + values[block] * factor * gain_rows[1:2, cols]
                value = value.astype(BF16)
                hidden[pl.ds(start, rows), cols] = value
                value = value.astype(F32)
                kept.append(value)
                squares += jnp.sum(value * value, axis=-1, keepdims=True)
            scale = lax.rsqrt(squares * (1.0 / width) + EPSILON)
            for block in range(shards):
                cols = pl.ds(block * piece_cols, piece_cols)
                mlp_in[pl.ds(place, rows), cols] = (kept[block] * scale * gain_rows[2:3, cols]).astype(BF16)
            return inner_carry

        lax.fori_loop(0, piece_rows // rows, entry_rows, 0)
        to_far(index).start()
        to_near(index).start()
        return carry

    lax.fori_loop(0, pieces, entry_piece, 0)
    when(is_end, lambda: serve(2, 5))
    serve(3, 0)

    @pl.when(is_inner)
    def _():
        serve(3, 1)
        start_other(3)
        serve(3, 2)

    all_x_arrivals(2)

    def wait_near(index, carry):
        to_near(index).wait_recv()
        return carry

    lax.fori_loop(0, pieces, wait_near, 0)
    up_tiles = units // PIECE

    def up_rows(base):
        def body(index, carry):
            col = aligned(index * PIECE, PIECE)
            value = jnp.dot(mlp_in[pl.ds(base, seq), :], u_full[:, pl.ds(col, PIECE)], preferred_element_type=F32)
            value = jnp.maximum(value * up_scale[:, pl.ds(aligned(y * units + col, PIECE), PIECE)], 0.0)
            active[pl.ds(base, seq), pl.ds(col, PIECE)] = (value * value).astype(BF16)
            return carry

        lax.fori_loop(0, up_tiles, body, 0)

    up_rows(0)

    def pass_on(index, carry):
        to_far(index).wait_recv()
        onward(index).start()
        return carry

    lax.fori_loop(0, pieces, pass_on, 0)
    when(is_end, lambda: serve(3, 1))

    @pl.when(is_inner)
    def _():
        serve(3, 3)
        serve(3, 4)

    def wait_far(index, carry):
        onward(index).wait_recv()
        return carry

    lax.fori_loop(0, pieces, wait_far, 0)
    up_rows(seq)

    def before_down(index):
        when(is_inner & (index == 0), lambda: serve(3, 5))
        when(is_end & (index >= 2) & (index < items), lambda: serve(3, index))
        when(index >= 2, lambda: x_arrival(3, index - 2))

    project(1, 3, active, 3, before_down)
    collect(1, 3, lambda index: None)

    def out_copy(index):
        block = pl.ds(aligned(index * piece_rows, 16), piece_rows)
        return pltpu.make_async_copy(result.at[block], out.at[block], out_sem.at[index])

    def last_piece(index, carry):
        def last_rows(inner_index, inner_carry):
            start = aligned(index * piece_rows + inner_index * rows, rows)
            values, factor = summed(start)
            for block in range(shards):
                cols = pl.ds(block * piece_cols, piece_cols)
                value = hidden[pl.ds(start, rows), cols].astype(F32) + values[block] * factor * gain_rows[3:4, cols]
                result[pl.ds(start, rows), cols] = value.astype(BF16)
            return inner_carry

        lax.fori_loop(0, piece_rows // rows, last_rows, 0)
        out_copy(index).start()
        return carry

    lax.fori_loop(0, pieces, last_piece, 0)

    for w in range(WEIGHTS):
        y_copy(w).wait_send()
        for kind in range(2):
            for cut in range(CUTS):
                for k in range(others):
                    x_copy(w, kind, k, cut).wait_send()
                z_copy(w, kind, 0, cut).wait_send()

                @pl.when(inner == 1)
                def _():
                    z_copy(w, kind, 1, cut).wait_send()
                    for k in range(others):
                        zf_copy(w, kind, k, cut).wait_send()

    t_near.wait_send()
    t_pass.wait_send()
    for step in range(1, shards):
        gain_copy(step).wait_send()

    def drain(index, carry):
        to_far(index).wait_send()
        to_near(index).wait_send()
        onward(index).wait_send()
        out_copy(index).wait()
        return carry

    lax.fori_loop(0, pieces, drain, 0)


def on_device_paired(
    tokens, gain_mix_pre, gain_mix_post, gain_mlp_pre, gain_mlp_post,
    x_weight, gate_weight, x_scale, gate_scale, conv_weight, recur_map, input_map,
    decay_param, out_weight, out_scale, up_weight, up_scale, down_weight, down_scale,
):
    shards = lax.axis_size("fs")
    seq, width = tokens.shape[1:]
    share, lines, pieces = seq // 2, shards // 2, 4
    fan_in, channels, units = x_weight.shape[0], x_weight.shape[1] // 2, up_weight.shape[1] // 2
    piece_cols = width // shards
    dma = pltpu.SemaphoreType.DMA
    anywhere = pl.BlockSpec(memory_space=pl.ANY)
    part_shapes = ((fan_in, 2 * channels), (channels, piece_cols), (fan_in, units), (units, piece_cols))
    raws = (x_weight, gate_weight, out_weight, up_weight, down_weight)
    rows = [
        value[None] for value in (
            gain_mix_pre, gain_mix_post, gain_mlp_pre, gain_mlp_post, out_scale, down_scale,
            x_scale, gate_scale, up_scale,
        )
    ]
    inputs = (tokens[0], *rows, conv_weight, recur_map.T, input_map.T, decay_param[None])
    outcome = pl.pallas_call(
        functools.partial(layer_kernel, shards),
        out_shape=jax.ShapeDtypeStruct((share, width), BF16),
        in_specs=[anywhere] * (len(inputs) + len(raws)),
        out_specs=anywhere,
        scratch_shapes=[pltpu.VMEM(value.shape, value.dtype) for value in inputs]
        + [dma((len(inputs),))]
        + [pltpu.VMEM((shards * shape[0], shape[1]), BF16) for shape in part_shapes]
        + [pltpu.VMEM(shape, BF16) for shape in part_shapes]
        + [pltpu.VMEM(raw.shape, F32) for raw in raws]
        + [
            pltpu.VMEM((shards, 4, piece_cols), F32),
            pltpu.VMEM((4, width), F32),
            pltpu.VMEM((1, 2 * channels), F32),
            pltpu.VMEM((2 * channels, LANES), BF16),
            pltpu.VMEM((1, channels), F32),
            pltpu.VMEM((seq, width), BF16),
            pltpu.VMEM((2 * seq, width), BF16),
            pltpu.VMEM((2 * seq, 2 * channels), BF16),
            pltpu.VMEM((2 * seq, channels), BF16),
            pltpu.VMEM((2 * seq, width), BF16),
            pltpu.VMEM((2 * seq, units), BF16),
            pltpu.VMEM((share, width), BF16),
            pltpu.VMEM((share, width), BF16),
            pltpu.VMEM((shards, 2, share, piece_cols), BF16),
            pltpu.VMEM((shards, 2, share, piece_cols), BF16),
            pltpu.VMEM((shards, share, piece_cols), F32),
            pltpu.VMEM((shards, share, piece_cols), F32),
            pltpu.VMEM((shards, share, piece_cols), BF16),
            pltpu.VMEM((shards, share, piece_cols), BF16),
            dma((len(raws),)), dma((WEIGHTS,)), dma((WEIGHTS,)),
            dma((WEIGHTS, 2, 2, CUTS)), dma((WEIGHTS, shards, CUTS)), dma((WEIGHTS, 2, lines - 1, CUTS)),
            dma((WEIGHTS, 2, lines - 1, CUTS)), dma((WEIGHTS, shards, CUTS)),
            dma((shards - 1,)), dma((shards,)),
            dma((2,)), dma((2,)),
            dma((2, shards)), dma((2, shards)), dma((2, shards)), dma((2, shards)),
            *[dma((pieces,))] * 7,
        ],
        compiler_params=pltpu.CompilerParams(
            collective_id=4, has_side_effects=True, vmem_limit_bytes=67_000_000
        ),
        cost_estimate=pl.CostEstimate(flops=20_000_000_000, bytes_accessed=80_000_000, transcendentals=0),
        name="layer",
    )(*inputs, *raws)
    return outcome[None]


def solution(mesh):
    in_specs = (
        P(("rep", "fs"), None, None),
        P("fs"), P("fs"), P("fs"), P("fs"),
        P("fs", "tp"), P("fs", "tp"),
        P("tp"), P("tp"),
        P(None, "tp"), P("tp", None), P("tp", None), P("tp"),
        P("tp", "fs"), P("fs"),
        P("fs", "tp"), P("tp"),
        P("tp", "fs"), P("fs"),
    )
    out_specs = P(("rep", "fs"), "tp", None)
    paired = (
        mesh.shape["rep"] == 2 and mesh.shape["tp"] == 2
        and mesh.shape["fs"] % 4 == 0 and mesh.shape["fs"] > 4
    )
    return jax.shard_map(
        on_device_paired if paired else on_device, mesh=mesh, in_specs=in_specs, out_specs=out_specs, check_vma=False
    )
```

```python
import functools

import jax
import jax.numpy as jnp
from jax import lax
from jax.experimental import pallas as pl
from jax.experimental.pallas import tpu as pltpu
from jax.sharding import PartitionSpec as P

BLOCK = 32
LANES = 128
EPSILON = 1e-06
DECAY_SCALE = 8.0
F32 = jnp.float32
BF16 = jnp.bfloat16


def unit_rows(values):
    return values * lax.rsqrt(jnp.mean(values * values, axis=-1, keepdims=True) + EPSILON)


def shifted(values, distance, fill):
    head = jnp.full((distance, values.shape[1]), fill, values.dtype)
    return jnp.concatenate([head, values[: values.shape[0] - distance]], axis=0)


def mixer_kernel(x_ref, gate_ref, taps_ref, recur_ref, input_ref, rate_ref, mixed_ref):
    length = x_ref.shape[0]
    x_branch = x_ref[...].astype(F32)
    taps = taps_ref.shape[0]
    total = taps_ref[taps - 1 : taps, :] * x_branch
    for tap in range(taps - 1):
        total += taps_ref[tap : tap + 1, :] * shifted(x_branch, taps - 1 - tap, 0.0)
    conv = total.astype(BF16)
    recur = jax.nn.sigmoid(jnp.dot(conv, recur_ref[...], preferred_element_type=F32))
    gate_in = jax.nn.sigmoid(jnp.dot(conv, input_ref[...], preferred_element_type=F32))
    log_decay = recur * rate_ref[0:1, :]
    decay = jnp.exp(log_decay)
    z = -2.0 * log_decay
    series = z * (1.0 - z * (1 / 2) * (1.0 - z * (1 / 3) * (1.0 - z * (1 / 4) * (1.0 - z * (1 / 5)))))
    power = jnp.where(z < 0.1, series, 1.0 - decay * decay)
    state = jnp.sqrt(power) * gate_in * conv.astype(F32)
    distance = 1
    while distance < length:
        state = state + decay * shifted(state, distance, 0.0)
        decay = decay * shifted(decay, distance, 1.0)
        distance *= 2
    mixed_ref[...] = (state * jax.nn.gelu(gate_ref[...].astype(F32))).astype(BF16)


def mixer(branches, taps, recur_dense, input_dense, rate, sequences):
    rows, width = branches.shape[0], branches.shape[1] // 2
    length = rows // sequences
    groups = width // LANES
    return pl.pallas_call(
        mixer_kernel,
        grid=(sequences, groups),
        in_specs=[
            pl.BlockSpec((length, LANES), lambda s, g: (s, g)),
            pl.BlockSpec((length, LANES), lambda s, g: (s, g + groups)),
            pl.BlockSpec((taps.shape[0], LANES), lambda s, g: (0, g)),
            pl.BlockSpec((LANES, LANES), lambda s, g: (g, 0)),
            pl.BlockSpec((LANES, LANES), lambda s, g: (g, 0)),
            pl.BlockSpec((1, LANES), lambda s, g: (0, g)),
        ],
        out_specs=pl.BlockSpec((length, LANES), lambda s, g: (s, g)),
        out_shape=jax.ShapeDtypeStruct((rows, width), BF16),
        cost_estimate=pl.CostEstimate(
            flops=rows * width * 100, bytes_accessed=rows * width * 6, transcendentals=rows * width * 4
        ),
        name="mixer",
    )(branches, branches, taps, recur_dense, input_dense, rate)


MESH_IDS = pl.DeviceIdType.MESH


def greet(peers):
    barrier = pltpu.get_barrier_semaphore()
    for peer in peers:
        pl.semaphore_signal(barrier, inc=1, device_id=peer, device_id_type=MESH_IDS)
    pl.semaphore_wait(barrier, len(peers))


def push(source, target, sent, landed, peer):
    return pltpu.make_async_remote_copy(
        src_ref=source, dst_ref=target, send_sem=sent, recv_sem=landed,
        device_id=peer, device_id_type=MESH_IDS,
    )


def others(axis, count):
    me = lax.axis_index(axis)
    return [lax.rem(me + step, count) for step in range(1, count)]


def row_block(ref, index, rows):
    return ref.at[pl.ds(pl.multiple_of(index * rows, rows), rows)]


def team_gather_kernel(reps, tps, x_ref, out_ref, own_sem, sent, landed):
    rep, core = lax.axis_index("rep"), lax.axis_index("tp")
    rows = x_ref.shape[0]
    rep_peers, tp_peers = others("rep", reps), others("tp", tps)
    greet([{"rep": peer} for peer in rep_peers] + [{"tp": peer} for peer in tp_peers])
    mine = row_block(out_ref, rep * tps + core, rows)
    flights = []
    for step, peer in enumerate(rep_peers):
        copy = push(x_ref, mine, sent.at[step + 1, 0], landed.at[step + 1, 0], {"rep": peer})
        copy.start()
        flights.append(copy)
    own = pltpu.make_async_copy(x_ref, mine, own_sem)
    own.start()
    local = []
    for slot, peer in enumerate(tp_peers):
        copy = push(x_ref, mine, sent.at[0, slot + 1], landed.at[0, slot + 1], {"tp": peer})
        copy.start()
        local.append(copy)
    for step in range(1, reps):
        flights[step - 1].wait_recv()
        source = lax.rem(rep + reps - step, reps)
        block = row_block(out_ref, source * tps + core, rows)
        for slot, peer in enumerate(tp_peers):
            copy = push(block, block, sent.at[step, slot + 1], landed.at[step, slot + 1], {"tp": peer})
            copy.start()
            local.append(copy)
    for copy in flights:
        copy.wait_send()
    for copy in local:
        copy.wait()
    own.wait()


def team_gather(values):
    reps, tps = lax.axis_size("rep"), lax.axis_size("tp")
    rows, width = values.shape
    return pl.pallas_call(
        functools.partial(team_gather_kernel, reps, tps),
        out_shape=jax.ShapeDtypeStruct((rows * reps * tps, width), values.dtype),
        in_specs=[pl.BlockSpec(memory_space=pltpu.VMEM)],
        out_specs=pl.BlockSpec(memory_space=pltpu.VMEM),
        scratch_shapes=[
            pltpu.SemaphoreType.DMA,
            pltpu.SemaphoreType.DMA((reps, tps)),
            pltpu.SemaphoreType.DMA((reps, tps)),
        ],
        compiler_params=pltpu.CompilerParams(collective_id=0, has_side_effects=True),
        cost_estimate=pl.CostEstimate(flops=0, bytes_accessed=80_000_000, transcendentals=0),
        name="team_gather",
    )(values)


def team_sum_kernel(reps, tps, part_ref, out_ref, got, stage, last, sent, landed, sent_far, landed_far):
    rep, core = lax.axis_index("rep"), lax.axis_index("tp")
    rows = out_ref.shape[0]
    step_rows = 16
    rep_peers, tp_peers = others("rep", reps), others("tp", tps)
    greet([{"rep": peer} for peer in rep_peers] + [{"tp": peer} for peer in tp_peers])
    near = []
    for slot, peer in enumerate(tp_peers):
        for group in range(reps):
            copy = push(
                row_block(part_ref, group * tps + peer, rows), got.at[slot, group],
                sent.at[slot, group], landed.at[slot, group], {"tp": peer},
            )
            copy.start()
            near.append(copy)
    for copy in near:
        copy.wait()

    def total(group, start):
        base = pl.multiple_of((group * tps + core) * rows + start, step_rows)
        value = part_ref[pl.ds(base, step_rows)].astype(F32)
        for slot in range(tps - 1):
            value += got[slot, group, pl.ds(start, step_rows)].astype(F32)
        return value

    far = []
    for step, peer in enumerate(rep_peers):

        def fill(index, carry):
            start = pl.multiple_of(index * step_rows, step_rows)
            stage[step, pl.ds(start, step_rows)] = total(peer, start).astype(BF16)
            return carry

        lax.fori_loop(0, rows // step_rows, fill, 0)
        copy = push(stage.at[step], last.at[step], sent_far.at[step], landed_far.at[step], {"rep": peer})
        copy.start()
        far.append(copy)
    for copy in far:
        copy.wait()

    def finish(index, carry):
        start = pl.multiple_of(index * step_rows, step_rows)
        value = total(rep, start)
        for step in range(reps - 1):
            value += last[step, pl.ds(start, step_rows)].astype(F32)
        out_ref[pl.ds(start, step_rows)] = value
        return carry

    lax.fori_loop(0, rows // step_rows, finish, 0)


def team_sum(parts):
    reps, tps = lax.axis_size("rep"), lax.axis_size("tp")
    rows, width = parts.shape[0] // (reps * tps), parts.shape[1]
    return pl.pallas_call(
        functools.partial(team_sum_kernel, reps, tps),
        out_shape=jax.ShapeDtypeStruct((rows, width), F32),
        in_specs=[pl.BlockSpec(memory_space=pltpu.VMEM)],
        out_specs=pl.BlockSpec(memory_space=pltpu.VMEM),
        scratch_shapes=[
            pltpu.VMEM((tps - 1, reps, rows, width), BF16),
            pltpu.VMEM((reps - 1, rows, width), BF16),
            pltpu.VMEM((reps - 1, rows, width), BF16),
            pltpu.SemaphoreType.DMA((tps - 1, reps)),
            pltpu.SemaphoreType.DMA((tps - 1, reps)),
            pltpu.SemaphoreType.DMA((reps - 1,)),
            pltpu.SemaphoreType.DMA((reps - 1,)),
        ],
        compiler_params=pltpu.CompilerParams(collective_id=1, has_side_effects=True),
        cost_estimate=pl.CostEstimate(flops=0, bytes_accessed=80_000_000, transcendentals=0),
        name="team_sum",
    )(parts)


def shard_gather_kernel(shards, x_ref, out_ref, own_sem, sent, landed, sent_pass, landed_pass):
    me = lax.axis_index("fs")
    rows = x_ref.shape[0]
    pairs = shards // 2
    pair, parity = me // 2, lax.rem(me, 2)
    partner = {"fs": pair * 2 + 1 - parity}
    peers = [{"fs": lax.rem(pair + step, pairs) * 2 + parity} for step in range(1, pairs)]
    greet([partner] + peers)
    mine = row_block(out_ref, me, rows)
    passed = [push(x_ref, mine, sent_pass.at[0], landed_pass.at[0], partner)]
    passed[0].start()
    direct = []
    for step, peer in enumerate(peers):
        copy = push(x_ref, mine, sent.at[step], landed.at[step], peer)
        copy.start()
        direct.append(copy)
    own = pltpu.make_async_copy(x_ref, mine, own_sem)
    own.start()
    for step in range(1, pairs):
        direct[step - 1].wait_recv()
        block = row_block(out_ref, lax.rem(pair + pairs - step, pairs) * 2 + parity, rows)
        copy = push(block, block, sent_pass.at[step], landed_pass.at[step], partner)
        copy.start()
        passed.append(copy)
    for copy in direct:
        copy.wait_send()
    for copy in passed:
        copy.wait()
    own.wait()


def shard_gather(values, collective_id):
    shards = lax.axis_size("fs")
    rows, width = values.shape
    return pl.pallas_call(
        functools.partial(shard_gather_kernel, shards),
        out_shape=jax.ShapeDtypeStruct((rows * shards, width), values.dtype),
        in_specs=[pl.BlockSpec(memory_space=pltpu.VMEM)],
        out_specs=pl.BlockSpec(memory_space=pltpu.VMEM),
        scratch_shapes=[
            pltpu.SemaphoreType.DMA,
            pltpu.SemaphoreType.DMA((shards // 2,)),
            pltpu.SemaphoreType.DMA((shards // 2,)),
            pltpu.SemaphoreType.DMA((shards // 2,)),
            pltpu.SemaphoreType.DMA((shards // 2,)),
        ],
        compiler_params=pltpu.CompilerParams(collective_id=collective_id, has_side_effects=True),
        cost_estimate=pl.CostEstimate(flops=0, bytes_accessed=200_000_000, transcendentals=0),
        name="shard_gather",
    )(values)


def on_device(
    tokens, gain_mix_pre, gain_mix_post, gain_mlp_pre, gain_mlp_post,
    x_weight, gate_weight, x_scale, gate_scale, conv_weight, recur_map, input_map,
    decay_param, out_weight, out_scale, up_weight, up_scale, down_weight, down_scale,
):
    reps = lax.axis_size("rep")
    rep = lax.axis_index("rep")

    def part(values, axis):
        size = values.shape[axis] // reps
        return lax.dynamic_slice_in_dim(values, rep * size, size, axis)

    length = tokens.shape[1]
    share_rows = length // lax.axis_size("tp")
    offset_row = lax.axis_index("tp") * share_rows
    resid_share = lax.dynamic_slice_in_dim(tokens[0], offset_row, share_rows, 0).astype(F32)
    normed_share = unit_rows(resid_share).astype(BF16)

    pre = gain_mix_pre[:, None]
    branch_rows = jnp.concatenate(
        [(part(x_weight, 1) * pre).astype(BF16), (part(gate_weight, 1) * pre).astype(BF16)], axis=1
    )
    branch_rows, out_weight = lax.optimization_barrier((branch_rows, out_weight))
    branch_full = lax.all_gather(branch_rows, "fs", axis=0, tiled=True)
    post = jnp.stack([gain_mix_post, gain_mlp_post])
    post_high = post.astype(BF16)
    post_low = (post - post_high.astype(F32)).astype(BF16)
    pad_rows = jnp.zeros((12, post.shape[1]), BF16)
    out_cols = jnp.concatenate(
        [(part(out_weight, 0) * out_scale).astype(BF16), post_high, post_low, pad_rows], axis=0
    )
    out_cols, down_weight = lax.optimization_barrier((out_cols, down_weight))
    out_all = lax.all_gather(out_cols, "fs", axis=1, tiled=True)
    down_full = lax.all_gather((part(down_weight, 0) * down_scale).astype(BF16), "fs", axis=1, tiled=True)
    up_rows = (part(up_weight, 1) * gain_mlp_pre[:, None]).astype(BF16)
    normed = team_gather(normed_share)
    normed, up_rows = lax.optimization_barrier((normed, up_rows))
    up_full = shard_gather(up_rows, 2)
    normed, up_full = lax.optimization_barrier((normed, up_full))

    scales = jnp.concatenate([part(x_scale, 0), part(gate_scale, 0)])
    branches = (jnp.dot(normed, branch_full, preferred_element_type=F32) * scales).astype(BF16)
    width = branches.shape[1] // 2

    def dense(block_map):
        rows = lax.broadcasted_iota(jnp.int32, (width, LANES), 0)
        columns = lax.broadcasted_iota(jnp.int32, (width, LANES), 1)
        spread = jnp.tile(part(block_map, 0), (1, LANES // BLOCK))
        return jnp.where(rows % LANES // BLOCK == columns // BLOCK, spread, 0).astype(BF16)

    rate = -DECAY_SCALE * jax.nn.softplus(-part(decay_param, 0))
    mixed = mixer(
        branches, part(conv_weight, 1), dense(recur_map), dense(input_map), rate[None], reps
    )
    out_full = out_all[:width]
    gains = out_all[width : width + 2].astype(F32) + out_all[width + 2 : width + 4].astype(F32)
    mix_share = team_sum(jnp.dot(mixed, out_full, preferred_element_type=F32).astype(BF16))
    hidden_state = (resid_share + unit_rows(mix_share) * gains[0]).astype(BF16)
    mlp_input = team_gather(unit_rows(hidden_state.astype(F32)).astype(BF16))
    up_proj = jnp.dot(mlp_input, up_full, preferred_element_type=F32)
    activated = jnp.square(jax.nn.relu(up_proj * part(up_scale, 0))).astype(BF16)
    mlp_share = team_sum(jnp.dot(activated, down_full, preferred_element_type=F32).astype(BF16))
    return (hidden_state.astype(F32) + unit_rows(mlp_share) * gains[1]).astype(BF16)[None]


WEIGHTS = 4
PIECE = 256
CUTS = (2, 2, 2, 4)


def log_decay_and_drive(conv, logits, rate):
    lanes = conv.shape[1]
    log_decay = jax.nn.sigmoid(logits[:, :lanes]) * rate
    decay = jnp.exp(log_decay)
    z = -2.0 * log_decay
    series = z * (1.0 - z * (1 / 2) * (1.0 - z * (1 / 3) * (1.0 - z * (1 / 4) * (1.0 - z * (1 / 5)))))
    power = jnp.where(z < 0.1, series, 1.0 - decay * decay)
    return decay, jnp.sqrt(power) * jax.nn.sigmoid(logits[:, lanes:]) * conv.astype(F32)


def mixer_group(x_branch, gate, taps, maps, rate):
    length, count = x_branch.shape[0], taps.shape[0]
    total = taps[count - 1 : count, :] * x_branch
    for tap in range(count - 1):
        total += taps[tap : tap + 1, :] * shifted(x_branch, count - 1 - tap, 0.0)
    conv = total.astype(BF16)
    logits = lax.dot_general(conv, maps, (((1,), (1,)), ((), ())), preferred_element_type=F32)
    decay, state = log_decay_and_drive(conv, logits, rate)
    distance = 1
    while distance < length:
        state = state + decay * shifted(state, distance, 0.0)
        decay = decay * shifted(decay, distance, 1.0)
        distance *= 2
    return (state * jax.nn.gelu(gate)).astype(BF16)


def softplus_of_negative(values):
    small = jnp.exp(-jnp.abs(values))
    series = jnp.zeros_like(small)
    for term in range(8, 0, -1):
        series = small * (1.0 / term - series)
    return jnp.maximum(-values, 0.0) + jnp.where(small < 0.1, series, jnp.log(1.0 + small))


def aligned(start, unit):
    return pl.multiple_of(start, unit)


def layer_kernel(shards, *refs):
    count = 14
    sources, raws, out = refs[:count], refs[count : count + 5], refs[count + 5]
    copies = refs[count + 6 : 2 * count + 6]
    load_sem = refs[2 * count + 6]
    loads = [
        pltpu.make_async_copy(source, copy, load_sem.at[at])
        for at, (source, copy) in enumerate(zip(sources, copies, strict=True))
    ]
    layer_body(shards, loads, *copies, *raws, out, *refs[2 * count + 7 :])


def layer_body(
    shards, loads, tokens, mix_pre, mix_post, mlp_pre, mlp_post, out_scale, down_scale,
    x_scale, gate_scale, up_scale, conv_weight, recur_map, input_map, decay_param,
    x_weight, gate_weight, out_weight, up_weight, down_weight, out,
    b_full, o_full, u_full, d_full, b_give, o_give, u_give, d_give,
    x_raw, gate_raw, o_raw, u_raw, d_raw, gains_full, gain_rows, scales, maps, rate,
    tok_got, normed, branches, mixed, mlp_in, active, hidden, result,
    give, got_near, keep, total, stage, got_far,
    raw_sem, y_sent, y_land, z_sent, z_land, zf_sent, x_sent, x_land, g_sent, g_land,
    t_sent, t_land, n_sent, n_land, f_sent, f_land, m_sent, m_land, mn_sent, mn_land, mf_sent, mf_land, out_sem,
):
    lines = shards // 2
    others = lines - 1
    rep, me, core = lax.axis_index("rep"), lax.axis_index("fs"), lax.axis_index("tp")
    z, y = me // 2, lax.rem(me, 2)
    x_peer, core_peer, y_peer = {"rep": 1 - rep}, {"tp": 1 - core}, {"fs": z * 2 + 1 - y}
    upper = z // (lines // 2)
    depth = z + upper * (lines - 1 - 2 * z)
    inner = (depth + lines - 1) // lines

    def unfold(place):
        return place + upper * (lines - 1 - 2 * place)

    def early(k):
        return 1 - (k + 2 * lines - 2 * depth) // (2 * lines)

    def other(k):
        near = depth + (1 - 2 * lax.rem(k, 2)) * (k // 2 + 1)
        return unfold(k + 1 + early(k) * (near - k - 1))

    seq, width = tokens.shape
    share = seq // 2
    columns = branches.shape[1]
    channels = columns // 2
    units = active.shape[1]
    gives = (b_give, o_give, u_give, d_give)
    fulls = (b_full, o_full, u_full, d_full)

    raw_copies = [
        pltpu.make_async_copy(x_weight, x_raw, raw_sem.at[0]),
        pltpu.make_async_copy(gate_weight, gate_raw, raw_sem.at[1]),
        pltpu.make_async_copy(out_weight, o_raw, raw_sem.at[2]),
        pltpu.make_async_copy(up_weight, u_raw, raw_sem.at[3]),
        pltpu.make_async_copy(down_weight, d_raw, raw_sem.at[4]),
    ]
    for copy in raw_copies[:2] + loads[1:] + raw_copies[2:] + loads[:1]:
        copy.start()
    token_copy = loads[0]
    peers = [{"fs": lax.rem(me + step, shards)} for step in range(1, shards)] + [x_peer, core_peer]
    barrier = pltpu.get_barrier_semaphore()
    for peer in peers:
        pl.semaphore_signal(barrier, inc=1, device_id=peer, device_id_type=MESH_IDS)
    for copy in loads[1:]:
        copy.wait()
    for row, gain in enumerate((mix_pre, mix_post, mlp_pre, mlp_post)):
        gains_full[me, row : row + 1, :] = gain[...]
    chunk = 32

    def cast(count, move):
        def body(index, carry):
            move(aligned(index * chunk, chunk))
            return carry

        lax.fori_loop(0, count // chunk, body, 0)

    def branch_rows(start):
        rows = pl.ds(start, chunk)
        home = pl.ds(aligned(me * b_give.shape[0] + start, chunk), chunk)
        for at, raw in enumerate((x_raw, gate_raw)):
            place = pl.ds(at * channels, channels)
            b_full[home, place] = raw[rows, pl.ds(aligned(y * channels, LANES), channels)].astype(BF16)
            b_give[rows, place] = raw[rows, pl.ds(aligned((1 - y) * channels, LANES), channels)].astype(BF16)

    def up_rows_cast(start):
        rows = pl.ds(start, chunk)
        home = pl.ds(aligned(me * u_give.shape[0] + start, chunk), chunk)
        u_full[home, :] = u_raw[rows, pl.ds(aligned(y * units, LANES), units)].astype(BF16)
        u_give[rows, :] = u_raw[rows, pl.ds(aligned((1 - y) * units, LANES), units)].astype(BF16)

    def column_rows(full, spare, raw, scale):
        size = spare.shape[0]

        def move(start):
            home = pl.ds(aligned(me * size + start, chunk), chunk)
            full[home, :] = (raw[pl.ds(aligned(y * size + start, chunk), chunk), :] * scale[...]).astype(BF16)
            rows = pl.ds(start, chunk)
            spare[rows, :] = (raw[pl.ds(aligned((1 - y) * size + start, chunk), chunk), :] * scale[...]).astype(BF16)

        return move

    def half(w, slot, side, cut):
        rows = gives[w].shape[0]
        size = rows // (2 * CUTS[w])
        return fulls[w].at[pl.ds(aligned(slot * rows + (side * CUTS[w] + cut) * size, 32), size)]

    def whole(w, slot):
        rows = gives[w].shape[0]
        return fulls[w].at[pl.ds(aligned(slot * rows, 64), rows)]

    def y_copy(w):
        return push(gives[w], whole(w, me), y_sent.at[w], y_land.at[w], y_peer)

    def y_arrival(w):
        block = whole(w, z * 2 + 1 - y)
        return push(block, block, y_sent.at[w], y_land.at[w], y_peer)

    def z_copy(w, kind, way, cut):
        slot = z * 2 + lax.rem(y + kind, 2)
        block = half(w, slot, rep, cut)
        target = unfold(depth + 1 - 2 * way)
        return push(block, block, z_sent.at[w, way], z_land.at[w, slot, cut], {"fs": target * 2 + y})

    def start_z(w, kind):
        for cut in range(CUTS[w]):

            @pl.when(inner == 1)
            def _():
                z_copy(w, kind, 1, cut).start()

            z_copy(w, kind, 0, cut).start()

    def item_slot(kind, k):
        return other(k) * 2 + lax.rem(y + kind, 2)

    def zf_copy(w, kind, k, cut):
        slot = item_slot(kind, k)
        block = half(w, slot, rep, cut)
        target = unfold(depth - 1 + 2 * early(k) * lax.rem(k, 2))
        return push(block, block, zf_sent.at[w], z_land.at[w, slot, cut], {"fs": target * 2 + y})

    def x_copy(w, kind, k, cut):
        slot = item_slot(kind, k)
        block = half(w, slot, rep, cut)
        return push(block, block, x_sent.at[w], x_land.at[w, slot], x_peer)

    def serve(w, item, cuts=None):
        kind, k = item // others, lax.rem(item, others)
        slot = item_slot(kind, k)
        for cut in range(CUTS[w]) if cuts is None else cuts:
            block = half(w, slot, rep, cut)
            push(block, block, x_sent.at[w], z_land.at[w, slot, cut], x_peer).wait_recv()

            @pl.when(inner == 1)
            def _():
                zf_copy(w, kind, k, cut).start()

            x_copy(w, kind, k, cut).start()

    def x_arrival(w, item):
        slot = item_slot(item // others, lax.rem(item, others))
        rows = gives[w].shape[0]
        block = fulls[w].at[pl.ds(aligned(slot * rows + (1 - rep) * (rows // 2), 64), rows // 2)]
        push(block, block, x_sent.at[w], x_land.at[w, slot], x_peer).wait_recv()

    items = 2 * others

    def all_x_arrivals(w):
        def body(index, carry):
            x_arrival(w, index)
            return carry

        lax.fori_loop(0, items, body, 0)

    def when(condition, act):
        pl.when(condition)(act)

    mine = pl.ds(aligned(core * share, 64), share)
    t_near = push(tokens.at[mine], tok_got.at[mine], t_sent.at[0], t_land.at[0], y_peer)
    t_pass = push(tok_got.at[mine], tok_got.at[mine], t_sent.at[1], t_land.at[1], core_peer)

    def gain_copy(step):
        block = gains_full.at[me]
        return push(block, block, g_sent, g_land.at[me], {"fs": lax.rem(me + step, shards)})

    raw_copies[0].wait()
    raw_copies[1].wait()
    cast(b_give.shape[0], branch_rows)
    pl.semaphore_wait(barrier, len(peers))
    for step in range(1, shards):
        gain_copy(step).start()
    y_copy(0).start()
    start_z(0, 0)
    raw_copies[2].wait()
    cast(o_give.shape[0], column_rows(o_full, o_give, o_raw, out_scale))
    raw_copies[3].wait()
    cast(u_give.shape[0], up_rows_cast)
    raw_copies[4].wait()
    cast(d_give.shape[0], column_rows(d_full, d_give, d_raw, down_scale))
    y_copy(1).start()
    token_copy.wait()
    t_near.start()
    y_copy(2).start()
    y_copy(3).start()

    part = pl.ds(aligned(y * channels, LANES), channels)
    scales[:, :channels] = x_scale[:, part]
    scales[:, channels:] = gate_scale[:, part]
    rate[...] = -DECAY_SCALE * softplus_of_negative(decay_param[:, part])
    block_rows = recur_map.shape[0]
    groups = channels // LANES
    same = (
        lax.broadcasted_iota(jnp.int32, (LANES, LANES), 0) // block_rows
        == lax.broadcasted_iota(jnp.int32, (LANES, LANES), 1) // block_rows
    )
    for group in range(groups):
        lanes = pl.ds(aligned(y * channels + group * LANES, LANES), LANES)
        for at, block_map in enumerate((recur_map, input_map)):
            spread = jnp.concatenate([block_map[:, lanes].astype(F32)] * (LANES // block_rows), axis=0)
            first = (group * 2 + at) * LANES
            maps[first : first + LANES, :] = jnp.where(same, spread, 0.0).astype(BF16)

    for step in range(1, shards):
        source = lax.rem(me + step, shards)
        block = gains_full.at[source]
        push(block, block, g_sent, g_land.at[source], y_peer).wait_recv()
    piece_cols = width // shards
    for block in range(shards):
        gain_rows[:, block * piece_cols : (block + 1) * piece_cols] = gains_full[block]

    rows = 16

    def normalize(source, base):
        def body(index, carry):
            start = aligned(index * rows, rows)
            values = source[pl.ds(start, rows), :].astype(F32)
            values = unit_rows(values) * gain_rows[0:1, :]
            normed[pl.ds(aligned(base + start, rows), rows), :] = values.astype(BF16)
            return carry

        lax.fori_loop(0, seq // rows, body, 0)

    is_inner, is_end = inner == 1, inner == 0

    def start_other(w):
        y_arrival(w).wait_recv()
        start_z(w, 1)

    serve(0, 0)
    serve(0, 1)
    when(is_inner, lambda: serve(0, 2))
    start_other(0)
    when(is_end, lambda: start_z(1, 0))
    normalize(tokens, 0)
    when(is_end, lambda: serve(0, 2))

    @pl.when(is_end)
    def _():
        start_other(1)
        start_z(2, 0)

    serve(0, 3)
    serve(0, 4)
    serve(0, 5)
    when(is_inner, lambda: start_z(1, 0))
    serve(1, 0)
    serve(1, 1)

    @pl.when(is_inner)
    def _():
        start_other(1)
        serve(1, 2)
        serve(1, 3)
        serve(1, 4)

    all_x_arrivals(0)

    col_tiles = columns // PIECE

    def last_out():
        serve(1, 5)
        start_z(2, 0)

    def pass_tokens():
        t_near.wait_recv()
        t_pass.start()

    def branch_step(index, carry):
        row = aligned((index // col_tiles) * seq, 64)
        col = aligned(lax.rem(index, col_tiles) * PIECE, PIECE)
        value = jnp.dot(normed[pl.ds(row, seq), :], b_full[:, pl.ds(col, PIECE)], preferred_element_type=F32)
        branches[pl.ds(row, seq), pl.ds(col, PIECE)] = (value * scales[:, pl.ds(col, PIECE)]).astype(BF16)
        when(index == 0, pass_tokens)
        when(is_inner & (index == 1), last_out)

        when(is_end & (index == 0), lambda: serve(1, 3))
        when(is_end & (index == 2), lambda: serve(1, 2))
        when(is_end & (index == 6), lambda: serve(2, 0))
        when(is_end & (index == 7), lambda: start_other(2))

        return carry

    lax.fori_loop(0, col_tiles, branch_step, 0)
    t_pass.wait_recv()
    normalize(tok_got, seq)

    @pl.when(is_end)
    def _():
        serve(1, 4)
        serve(1, 5)

    lax.fori_loop(col_tiles, 2 * col_tiles, branch_step, 0)

    def up_second():
        serve(2, 1)
        start_other(2)

    def mixer_step(index, carry):
        row = aligned((index // groups) * seq, 64)
        group = lax.rem(index, groups)
        col = aligned(group * LANES, LANES)
        lanes = pl.ds(col, LANES)
        mixed[pl.ds(row, seq), lanes] = mixer_group(
            branches[pl.ds(row, seq), lanes].astype(F32),
            branches[pl.ds(row, seq), pl.ds(aligned(channels + col, LANES), LANES)].astype(F32),
            conv_weight[:, pl.ds(aligned(y * channels + col, LANES), LANES)],
            maps[pl.ds(aligned(group * 2 * LANES, LANES), 2 * LANES), :], rate[:, lanes],
        )
        when(is_inner & (index == 3), lambda: serve(2, 0))
        when(is_inner & (index == 4), up_second)
        when(is_end & (index == 2 * groups - 1), lambda: serve(2, 1))
        return carry

    lax.fori_loop(0, 2 * groups, mixer_step, 0)

    def arrival(item):
        gap = item - others + 1
        swapped = 1 - (gap * (gap - 1) + 63) // 64
        return item + swapped * (2 * others - 1 - 2 * item)

    def block_of(index, flip=0):
        item = index - 2
        safe = arrival(lax.rem(item + items, items))
        far = item_slot(safe // others + flip, lax.rem(safe, others))
        near = z * 2 + lax.rem(y + index + flip, 2)
        late = (index + shards - 2) // shards
        return near + late * (far - near)

    def near_copy(phase, block):
        return push(give.at[block], got_near.at[block], n_sent.at[phase], n_land.at[block], core_peer)

    def far_copy(phase, block):
        return push(stage.at[block], got_far.at[block], f_sent.at[phase], f_land.at[block], y_peer)

    def project(phase, w, lhs, lag, before, after):
        depth_rows = gives[w].shape[0]

        def combine(index):
            block = block_of(index)
            near_copy(phase, block).wait_recv()
            stage[block] = (keep[block] + got_near[block, 1].astype(F32)).astype(BF16)
            total[block] += got_near[block, 0].astype(F32)
            far_copy(phase, block).start()

        def body(index, carry):
            before(index)
            block = block_of(index)
            weight = fulls[w][pl.ds(aligned(block * depth_rows, 64), depth_rows), :]
            for side in range(2):
                left = lhs[pl.ds(aligned(side * seq + (1 - core) * share, 64), share), :]
                give[block, side] = jnp.dot(left, weight, preferred_element_type=F32).astype(BF16)
            own = lhs[pl.ds(aligned(core * share, 64), share), :]
            total[block] = jnp.dot(own, weight, preferred_element_type=F32)
            near_copy(phase, block).start()
            own = lhs[pl.ds(aligned(seq + core * share, 64), share), :]
            keep[block] = jnp.dot(own, weight, preferred_element_type=F32)
            when(index > 0, lambda: combine(index - 1))
            if lag < shards:
                when(index >= lag, lambda: add_far(phase, index - lag))
            after(index)
            return carry

        lax.fori_loop(0, shards, body, 0)
        combine(shards - 1)

    def add_far(phase, index):
        block = block_of(index, 1)
        far_copy(phase, block).wait_recv()
        total[block] += got_far[block].astype(F32)

    def collect(phase, lag, between):
        def body(index, carry):
            add_far(phase, index)
            between(index)
            return carry

        lax.fori_loop(shards - lag, shards, body, 0)

        push(stage, stage, f_sent.at[phase], f_land.at[0], y_peer).wait_send()
        push(give, give, n_sent.at[phase], n_land.at[0], core_peer).wait_send()

    def during_project(index):
        when(is_inner & (index == 6), lambda: serve(2, 2))
        when(is_end & (index == 0), lambda: start_z(3, 0))
        when(is_end & (index == 6), lambda: serve(2, 3))

    def last_up():
        serve(2, 5)
        start_z(3, 0)

    def during_sum(index):
        when(is_inner & (index == 1), lambda: serve(2, 3))
        when(is_inner & (index == 2), lambda: serve(2, 4))
        when(is_inner & (index == 5), last_up)
        when(is_end & (index == 0), lambda: start_other(3))
        when(is_end & (index == 1), lambda: serve(2, 2))
        when(is_end & (index == 3), lambda: serve(2, 4))

    all_x_arrivals(1)
    project(0, 1, mixed, shards, during_project, lambda index: None)
    collect(0, shards, during_sum)

    def summed(start):
        values = [total[block, pl.ds(start, rows), :] for block in range(shards)]
        squares = sum(jnp.sum(value * value, axis=-1, keepdims=True) for value in values)
        return values, lax.rsqrt(squares * (1.0 / width) + EPSILON)

    pieces = m_land.shape[0]
    piece_rows = share // pieces

    def piece(ref, base, index):
        return ref.at[pl.ds(aligned(base + index * piece_rows, 16), piece_rows)]

    def to_far(index):
        return push(
            piece(mlp_in, core * share, index), piece(mlp_in, seq + core * share, index),
            m_sent, m_land.at[index], y_peer,
        )

    def to_near(index):
        block = piece(mlp_in, core * share, index)
        return push(block, block, mn_sent, mn_land.at[index], core_peer)

    def onward(index):
        block = piece(mlp_in, seq + core * share, index)
        return push(block, block, mf_sent, mf_land.at[index], core_peer)

    def entry_piece(index, carry):
        def entry_rows(inner_index, inner_carry):
            start = aligned(index * piece_rows + inner_index * rows, rows)
            values, factor = summed(start)
            place = aligned(core * share + start, rows)
            squares = jnp.zeros((rows, 1), F32)
            kept = []
            for block in range(shards):
                cols = pl.ds(block * piece_cols, piece_cols)
                value = tokens[pl.ds(place, rows), cols].astype(F32) + values[block] * factor * gain_rows[1:2, cols]
                value = value.astype(BF16)
                hidden[pl.ds(start, rows), cols] = value
                value = value.astype(F32)
                kept.append(value)
                squares += jnp.sum(value * value, axis=-1, keepdims=True)
            scale = lax.rsqrt(squares * (1.0 / width) + EPSILON)
            for block in range(shards):
                cols = pl.ds(block * piece_cols, piece_cols)
                mlp_in[pl.ds(place, rows), cols] = (kept[block] * scale * gain_rows[2:3, cols]).astype(BF16)
            return inner_carry

        lax.fori_loop(0, piece_rows // rows, entry_rows, 0)
        to_far(index).start()
        to_near(index).start()
        return carry

    when(is_end, lambda: serve(2, 5, (0,)))
    lax.fori_loop(0, pieces, entry_piece, 0)
    when(is_end, lambda: serve(2, 5, range(1, CUTS[2])))
    serve(3, 0)

    @pl.when(is_inner)
    def _():
        serve(3, 1)
        start_other(3)
        serve(3, 2)

    all_x_arrivals(2)

    def wait_near(index, carry):
        to_near(index).wait_recv()
        return carry

    lax.fori_loop(0, pieces, wait_near, 0)
    up_tiles = units // PIECE

    def up_rows(base):
        def body(index, carry):
            col = aligned(index * PIECE, PIECE)
            value = jnp.dot(mlp_in[pl.ds(base, seq), :], u_full[:, pl.ds(col, PIECE)], preferred_element_type=F32)
            value = jnp.maximum(value * up_scale[:, pl.ds(aligned(y * units + col, PIECE), PIECE)], 0.0)
            active[pl.ds(base, seq), pl.ds(col, PIECE)] = (value * value).astype(BF16)
            return carry

        lax.fori_loop(0, up_tiles, body, 0)

    up_rows(0)
    when(is_end, lambda: serve(3, 1))

    def pass_on(index, carry):
        to_far(index).wait_recv()
        onward(index).start()
        return carry

    lax.fori_loop(0, pieces, pass_on, 0)
    when(is_end, lambda: serve(3, 3, (0, 1)))

    @pl.when(is_inner)
    def _():
        serve(3, 3)
        serve(3, 4)

    def wait_far(index, carry):
        onward(index).wait_recv()
        return carry

    lax.fori_loop(0, pieces, wait_far, 0)
    up_rows(seq)

    def before_down(index):
        when(is_inner & (index == 0), lambda: serve(3, 5))
        when(index >= 2, lambda: x_arrival(3, arrival(index - 2)))

    def after_down(index):
        when(is_end & (index >= 2) & (index < items - 1), lambda: serve(3, arrival(index + 1)))

    when(is_end, lambda: serve(3, 3, range(2, CUTS[3])))
    project(1, 3, active, 3, before_down, after_down)
    collect(1, 3, lambda index: None)

    def out_copy(index):
        block = pl.ds(aligned(index * piece_rows, 16), piece_rows)
        return pltpu.make_async_copy(result.at[block], out.at[block], out_sem.at[index])

    def last_piece(index, carry):
        def last_rows(inner_index, inner_carry):
            start = aligned(index * piece_rows + inner_index * rows, rows)
            values, factor = summed(start)
            for block in range(shards):
                cols = pl.ds(block * piece_cols, piece_cols)
                value = hidden[pl.ds(start, rows), cols].astype(F32) + values[block] * factor * gain_rows[3:4, cols]
                result[pl.ds(start, rows), cols] = value.astype(BF16)
            return inner_carry

        lax.fori_loop(0, piece_rows // rows, last_rows, 0)
        out_copy(index).start()
        return carry

    lax.fori_loop(0, pieces, last_piece, 0)

    for w in range(WEIGHTS):
        y_copy(w).wait_send()
        sent = fulls[w].at[pl.ds(0, others * gives[w].shape[0])]
        own = fulls[w].at[pl.ds(0, gives[w].shape[0])]
        push(sent, sent, x_sent.at[w], x_land.at[w, 0], x_peer).wait_send()
        push(own, own, z_sent.at[w, 0], x_land.at[w, 0], x_peer).wait_send()

        @pl.when(inner == 1)
        def _():
            push(own, own, z_sent.at[w, 1], x_land.at[w, 0], x_peer).wait_send()
            push(sent, sent, zf_sent.at[w], x_land.at[w, 0], x_peer).wait_send()

    t_near.wait_send()
    t_pass.wait_send()
    most = gains_full.at[pl.ds(0, shards - 1)]
    push(most, most, g_sent, g_land.at[0], y_peer).wait_send()

    def drain(index, carry):
        out_copy(index).wait()
        return carry

    lax.fori_loop(0, pieces, drain, 0)
    block = mlp_in.at[pl.ds(0, share)]
    for sent in (m_sent, mn_sent, mf_sent):
        push(block, block, sent, m_land.at[0], y_peer).wait_send()


def on_device_paired(
    tokens, gain_mix_pre, gain_mix_post, gain_mlp_pre, gain_mlp_post,
    x_weight, gate_weight, x_scale, gate_scale, conv_weight, recur_map, input_map,
    decay_param, out_weight, out_scale, up_weight, up_scale, down_weight, down_scale,
):
    shards = lax.axis_size("fs")
    seq, width = tokens.shape[1:]
    share, lines, pieces = seq // 2, shards // 2, 4
    fan_in, channels, units = x_weight.shape[0], x_weight.shape[1] // 2, up_weight.shape[1] // 2
    piece_cols = width // shards
    dma = pltpu.SemaphoreType.DMA
    anywhere = pl.BlockSpec(memory_space=pl.ANY)
    part_shapes = ((fan_in, 2 * channels), (channels, piece_cols), (fan_in, units), (units, piece_cols))
    raws = (x_weight, gate_weight, out_weight, up_weight, down_weight)
    rows = [
        value[None] for value in (
            gain_mix_pre, gain_mix_post, gain_mlp_pre, gain_mlp_post, out_scale, down_scale,
            x_scale, gate_scale, up_scale,
        )
    ]
    inputs = (tokens[0], *rows, conv_weight, recur_map.T, input_map.T, decay_param[None])
    outcome = pl.pallas_call(
        functools.partial(layer_kernel, shards),
        out_shape=jax.ShapeDtypeStruct((share, width), BF16),
        in_specs=[anywhere] * (len(inputs) + len(raws)),
        out_specs=anywhere,
        scratch_shapes=[pltpu.VMEM(value.shape, value.dtype) for value in inputs]
        + [dma((len(inputs),))]
        + [pltpu.VMEM((shards * shape[0], shape[1]), BF16) for shape in part_shapes]
        + [pltpu.VMEM(shape, BF16) for shape in part_shapes]
        + [pltpu.VMEM(raw.shape, F32) for raw in raws]
        + [
            pltpu.VMEM((shards, 4, piece_cols), F32),
            pltpu.VMEM((4, width), F32),
            pltpu.VMEM((1, 2 * channels), F32),
            pltpu.VMEM((2 * channels, LANES), BF16),
            pltpu.VMEM((1, channels), F32),
            pltpu.VMEM((seq, width), BF16),
            pltpu.VMEM((2 * seq, width), BF16),
            pltpu.VMEM((2 * seq, 2 * channels), BF16),
            pltpu.VMEM((2 * seq, channels), BF16),
            pltpu.VMEM((2 * seq, width), BF16),
            pltpu.VMEM((2 * seq, units), BF16),
            pltpu.VMEM((share, width), BF16),
            pltpu.VMEM((share, width), BF16),
            pltpu.VMEM((shards, 2, share, piece_cols), BF16),
            pltpu.VMEM((shards, 2, share, piece_cols), BF16),
            pltpu.VMEM((shards, share, piece_cols), F32),
            pltpu.VMEM((shards, share, piece_cols), F32),
            pltpu.VMEM((shards, share, piece_cols), BF16),
            pltpu.VMEM((shards, share, piece_cols), BF16),
            dma((len(raws),)), dma((WEIGHTS,)), dma((WEIGHTS,)),
            dma((WEIGHTS, 2)), dma((WEIGHTS, shards, max(CUTS))), dma((WEIGHTS,)),
            dma((WEIGHTS,)), dma((WEIGHTS, shards)),
            dma, dma((shards,)),
            dma((2,)), dma((2,)),
            dma((2,)), dma((shards,)), dma((2,)), dma((shards,)),
            dma, dma((pieces,)), dma, dma((pieces,)), dma, dma((pieces,)), dma((pieces,)),
        ],
        compiler_params=pltpu.CompilerParams(
            collective_id=4, has_side_effects=True, vmem_limit_bytes=67_000_000
        ),
        cost_estimate=pl.CostEstimate(flops=20_000_000_000, bytes_accessed=80_000_000, transcendentals=0),
        name="layer",
    )(*inputs, *raws)
    return outcome[None]


def solution(mesh):
    in_specs = (
        P(("rep", "fs"), None, None),
        P("fs"), P("fs"), P("fs"), P("fs"),
        P("fs", "tp"), P("fs", "tp"),
        P("tp"), P("tp"),
        P(None, "tp"), P("tp", None), P("tp", None), P("tp"),
        P("tp", "fs"), P("fs"),
        P("fs", "tp"), P("tp"),
        P("tp", "fs"), P("fs"),
    )
    out_specs = P(("rep", "fs"), "tp", None)
    paired = (
        mesh.shape["rep"] == 2 and mesh.shape["tp"] == 2
        and mesh.shape["fs"] % 4 == 0 and mesh.shape["fs"] > 4
    )
    return jax.shard_map(
        on_device_paired if paired else on_device, mesh=mesh, in_specs=in_specs, out_specs=out_specs, check_vma=False
    )
```

```python
import functools

import jax
import jax.numpy as jnp
from jax import lax
from jax.experimental import pallas as pl
from jax.experimental.pallas import tpu as pltpu
from jax.sharding import PartitionSpec as P

BLOCK = 32
LANES = 128
EPSILON = 1e-06
DECAY_SCALE = 8.0
F32 = jnp.float32
BF16 = jnp.bfloat16


def unit_rows(values):
    return values * lax.rsqrt(jnp.mean(values * values, axis=-1, keepdims=True) + EPSILON)


def shifted(values, distance, fill):
    head = jnp.full((distance, values.shape[1]), fill, values.dtype)
    return jnp.concatenate([head, values[: values.shape[0] - distance]], axis=0)


def mixer_kernel(x_ref, gate_ref, taps_ref, recur_ref, input_ref, rate_ref, mixed_ref):
    length = x_ref.shape[0]
    x_branch = x_ref[...].astype(F32)
    taps = taps_ref.shape[0]
    total = taps_ref[taps - 1 : taps, :] * x_branch
    for tap in range(taps - 1):
        total += taps_ref[tap : tap + 1, :] * shifted(x_branch, taps - 1 - tap, 0.0)
    conv = total.astype(BF16)
    recur = jax.nn.sigmoid(jnp.dot(conv, recur_ref[...], preferred_element_type=F32))
    gate_in = jax.nn.sigmoid(jnp.dot(conv, input_ref[...], preferred_element_type=F32))
    log_decay = recur * rate_ref[0:1, :]
    decay = jnp.exp(log_decay)
    z = -2.0 * log_decay
    series = z * (1.0 - z * (1 / 2) * (1.0 - z * (1 / 3) * (1.0 - z * (1 / 4) * (1.0 - z * (1 / 5)))))
    power = jnp.where(z < 0.1, series, 1.0 - decay * decay)
    state = jnp.sqrt(power) * gate_in * conv.astype(F32)
    distance = 1
    while distance < length:
        state = state + decay * shifted(state, distance, 0.0)
        decay = decay * shifted(decay, distance, 1.0)
        distance *= 2
    mixed_ref[...] = (state * jax.nn.gelu(gate_ref[...].astype(F32))).astype(BF16)


def mixer(branches, taps, recur_dense, input_dense, rate, sequences):
    rows, width = branches.shape[0], branches.shape[1] // 2
    length = rows // sequences
    groups = width // LANES
    return pl.pallas_call(
        mixer_kernel,
        grid=(sequences, groups),
        in_specs=[
            pl.BlockSpec((length, LANES), lambda s, g: (s, g)),
            pl.BlockSpec((length, LANES), lambda s, g: (s, g + groups)),
            pl.BlockSpec((taps.shape[0], LANES), lambda s, g: (0, g)),
            pl.BlockSpec((LANES, LANES), lambda s, g: (g, 0)),
            pl.BlockSpec((LANES, LANES), lambda s, g: (g, 0)),
            pl.BlockSpec((1, LANES), lambda s, g: (0, g)),
        ],
        out_specs=pl.BlockSpec((length, LANES), lambda s, g: (s, g)),
        out_shape=jax.ShapeDtypeStruct((rows, width), BF16),
        cost_estimate=pl.CostEstimate(
            flops=rows * width * 100, bytes_accessed=rows * width * 6, transcendentals=rows * width * 4
        ),
        name="mixer",
    )(branches, branches, taps, recur_dense, input_dense, rate)


MESH_IDS = pl.DeviceIdType.MESH


def greet(peers):
    barrier = pltpu.get_barrier_semaphore()
    for peer in peers:
        pl.semaphore_signal(barrier, inc=1, device_id=peer, device_id_type=MESH_IDS)
    pl.semaphore_wait(barrier, len(peers))


def push(source, target, sent, landed, peer):
    return pltpu.make_async_remote_copy(
        src_ref=source, dst_ref=target, send_sem=sent, recv_sem=landed,
        device_id=peer, device_id_type=MESH_IDS,
    )


def others(axis, count):
    me = lax.axis_index(axis)
    return [lax.rem(me + step, count) for step in range(1, count)]


def row_block(ref, index, rows):
    return ref.at[pl.ds(pl.multiple_of(index * rows, rows), rows)]


def team_gather_kernel(reps, tps, x_ref, out_ref, own_sem, sent, landed):
    rep, core = lax.axis_index("rep"), lax.axis_index("tp")
    rows = x_ref.shape[0]
    rep_peers, tp_peers = others("rep", reps), others("tp", tps)
    greet([{"rep": peer} for peer in rep_peers] + [{"tp": peer} for peer in tp_peers])
    mine = row_block(out_ref, rep * tps + core, rows)
    flights = []
    for step, peer in enumerate(rep_peers):
        copy = push(x_ref, mine, sent.at[step + 1, 0], landed.at[step + 1, 0], {"rep": peer})
        copy.start()
        flights.append(copy)
    own = pltpu.make_async_copy(x_ref, mine, own_sem)
    own.start()
    local = []
    for slot, peer in enumerate(tp_peers):
        copy = push(x_ref, mine, sent.at[0, slot + 1], landed.at[0, slot + 1], {"tp": peer})
        copy.start()
        local.append(copy)
    for step in range(1, reps):
        flights[step - 1].wait_recv()
        source = lax.rem(rep + reps - step, reps)
        block = row_block(out_ref, source * tps + core, rows)
        for slot, peer in enumerate(tp_peers):
            copy = push(block, block, sent.at[step, slot + 1], landed.at[step, slot + 1], {"tp": peer})
            copy.start()
            local.append(copy)
    for copy in flights:
        copy.wait_send()
    for copy in local:
        copy.wait()
    own.wait()


def team_gather(values):
    reps, tps = lax.axis_size("rep"), lax.axis_size("tp")
    rows, width = values.shape
    return pl.pallas_call(
        functools.partial(team_gather_kernel, reps, tps),
        out_shape=jax.ShapeDtypeStruct((rows * reps * tps, width), values.dtype),
        in_specs=[pl.BlockSpec(memory_space=pltpu.VMEM)],
        out_specs=pl.BlockSpec(memory_space=pltpu.VMEM),
        scratch_shapes=[
            pltpu.SemaphoreType.DMA,
            pltpu.SemaphoreType.DMA((reps, tps)),
            pltpu.SemaphoreType.DMA((reps, tps)),
        ],
        compiler_params=pltpu.CompilerParams(collective_id=0, has_side_effects=True),
        cost_estimate=pl.CostEstimate(flops=0, bytes_accessed=80_000_000, transcendentals=0),
        name="team_gather",
    )(values)


def team_sum_kernel(reps, tps, part_ref, out_ref, got, stage, last, sent, landed, sent_far, landed_far):
    rep, core = lax.axis_index("rep"), lax.axis_index("tp")
    rows = out_ref.shape[0]
    step_rows = 16
    rep_peers, tp_peers = others("rep", reps), others("tp", tps)
    greet([{"rep": peer} for peer in rep_peers] + [{"tp": peer} for peer in tp_peers])
    near = []
    for slot, peer in enumerate(tp_peers):
        for group in range(reps):
            copy = push(
                row_block(part_ref, group * tps + peer, rows), got.at[slot, group],
                sent.at[slot, group], landed.at[slot, group], {"tp": peer},
            )
            copy.start()
            near.append(copy)
    for copy in near:
        copy.wait()

    def total(group, start):
        base = pl.multiple_of((group * tps + core) * rows + start, step_rows)
        value = part_ref[pl.ds(base, step_rows)].astype(F32)
        for slot in range(tps - 1):
            value += got[slot, group, pl.ds(start, step_rows)].astype(F32)
        return value

    far = []
    for step, peer in enumerate(rep_peers):

        def fill(index, carry):
            start = pl.multiple_of(index * step_rows, step_rows)
            stage[step, pl.ds(start, step_rows)] = total(peer, start).astype(BF16)
            return carry

        lax.fori_loop(0, rows // step_rows, fill, 0)
        copy = push(stage.at[step], last.at[step], sent_far.at[step], landed_far.at[step], {"rep": peer})
        copy.start()
        far.append(copy)
    for copy in far:
        copy.wait()

    def finish(index, carry):
        start = pl.multiple_of(index * step_rows, step_rows)
        value = total(rep, start)
        for step in range(reps - 1):
            value += last[step, pl.ds(start, step_rows)].astype(F32)
        out_ref[pl.ds(start, step_rows)] = value
        return carry

    lax.fori_loop(0, rows // step_rows, finish, 0)


def team_sum(parts):
    reps, tps = lax.axis_size("rep"), lax.axis_size("tp")
    rows, width = parts.shape[0] // (reps * tps), parts.shape[1]
    return pl.pallas_call(
        functools.partial(team_sum_kernel, reps, tps),
        out_shape=jax.ShapeDtypeStruct((rows, width), F32),
        in_specs=[pl.BlockSpec(memory_space=pltpu.VMEM)],
        out_specs=pl.BlockSpec(memory_space=pltpu.VMEM),
        scratch_shapes=[
            pltpu.VMEM((tps - 1, reps, rows, width), BF16),
            pltpu.VMEM((reps - 1, rows, width), BF16),
            pltpu.VMEM((reps - 1, rows, width), BF16),
            pltpu.SemaphoreType.DMA((tps - 1, reps)),
            pltpu.SemaphoreType.DMA((tps - 1, reps)),
            pltpu.SemaphoreType.DMA((reps - 1,)),
            pltpu.SemaphoreType.DMA((reps - 1,)),
        ],
        compiler_params=pltpu.CompilerParams(collective_id=1, has_side_effects=True),
        cost_estimate=pl.CostEstimate(flops=0, bytes_accessed=80_000_000, transcendentals=0),
        name="team_sum",
    )(parts)


def shard_gather_kernel(shards, x_ref, out_ref, own_sem, sent, landed, sent_pass, landed_pass):
    me = lax.axis_index("fs")
    rows = x_ref.shape[0]
    pairs = shards // 2
    pair, parity = me // 2, lax.rem(me, 2)
    partner = {"fs": pair * 2 + 1 - parity}
    peers = [{"fs": lax.rem(pair + step, pairs) * 2 + parity} for step in range(1, pairs)]
    greet([partner] + peers)
    mine = row_block(out_ref, me, rows)
    passed = [push(x_ref, mine, sent_pass.at[0], landed_pass.at[0], partner)]
    passed[0].start()
    direct = []
    for step, peer in enumerate(peers):
        copy = push(x_ref, mine, sent.at[step], landed.at[step], peer)
        copy.start()
        direct.append(copy)
    own = pltpu.make_async_copy(x_ref, mine, own_sem)
    own.start()
    for step in range(1, pairs):
        direct[step - 1].wait_recv()
        block = row_block(out_ref, lax.rem(pair + pairs - step, pairs) * 2 + parity, rows)
        copy = push(block, block, sent_pass.at[step], landed_pass.at[step], partner)
        copy.start()
        passed.append(copy)
    for copy in direct:
        copy.wait_send()
    for copy in passed:
        copy.wait()
    own.wait()


def shard_gather(values, collective_id):
    shards = lax.axis_size("fs")
    rows, width = values.shape
    return pl.pallas_call(
        functools.partial(shard_gather_kernel, shards),
        out_shape=jax.ShapeDtypeStruct((rows * shards, width), values.dtype),
        in_specs=[pl.BlockSpec(memory_space=pltpu.VMEM)],
        out_specs=pl.BlockSpec(memory_space=pltpu.VMEM),
        scratch_shapes=[
            pltpu.SemaphoreType.DMA,
            pltpu.SemaphoreType.DMA((shards // 2,)),
            pltpu.SemaphoreType.DMA((shards // 2,)),
            pltpu.SemaphoreType.DMA((shards // 2,)),
            pltpu.SemaphoreType.DMA((shards // 2,)),
        ],
        compiler_params=pltpu.CompilerParams(collective_id=collective_id, has_side_effects=True),
        cost_estimate=pl.CostEstimate(flops=0, bytes_accessed=200_000_000, transcendentals=0),
        name="shard_gather",
    )(values)


def on_device(
    tokens, gain_mix_pre, gain_mix_post, gain_mlp_pre, gain_mlp_post,
    x_weight, gate_weight, x_scale, gate_scale, conv_weight, recur_map, input_map,
    decay_param, out_weight, out_scale, up_weight, up_scale, down_weight, down_scale,
):
    reps = lax.axis_size("rep")
    rep = lax.axis_index("rep")

    def part(values, axis):
        size = values.shape[axis] // reps
        return lax.dynamic_slice_in_dim(values, rep * size, size, axis)

    length = tokens.shape[1]
    share_rows = length // lax.axis_size("tp")
    offset_row = lax.axis_index("tp") * share_rows
    resid_share = lax.dynamic_slice_in_dim(tokens[0], offset_row, share_rows, 0).astype(F32)
    normed_share = unit_rows(resid_share).astype(BF16)

    pre = gain_mix_pre[:, None]
    branch_rows = jnp.concatenate(
        [(part(x_weight, 1) * pre).astype(BF16), (part(gate_weight, 1) * pre).astype(BF16)], axis=1
    )
    branch_rows, out_weight = lax.optimization_barrier((branch_rows, out_weight))
    branch_full = lax.all_gather(branch_rows, "fs", axis=0, tiled=True)
    post = jnp.stack([gain_mix_post, gain_mlp_post])
    post_high = post.astype(BF16)
    post_low = (post - post_high.astype(F32)).astype(BF16)
    pad_rows = jnp.zeros((12, post.shape[1]), BF16)
    out_cols = jnp.concatenate(
        [(part(out_weight, 0) * out_scale).astype(BF16), post_high, post_low, pad_rows], axis=0
    )
    out_cols, down_weight = lax.optimization_barrier((out_cols, down_weight))
    out_all = lax.all_gather(out_cols, "fs", axis=1, tiled=True)
    down_full = lax.all_gather((part(down_weight, 0) * down_scale).astype(BF16), "fs", axis=1, tiled=True)
    up_rows = (part(up_weight, 1) * gain_mlp_pre[:, None]).astype(BF16)
    normed = team_gather(normed_share)
    normed, up_rows = lax.optimization_barrier((normed, up_rows))
    up_full = shard_gather(up_rows, 2)
    normed, up_full = lax.optimization_barrier((normed, up_full))

    scales = jnp.concatenate([part(x_scale, 0), part(gate_scale, 0)])
    branches = (jnp.dot(normed, branch_full, preferred_element_type=F32) * scales).astype(BF16)
    width = branches.shape[1] // 2

    def dense(block_map):
        rows = lax.broadcasted_iota(jnp.int32, (width, LANES), 0)
        columns = lax.broadcasted_iota(jnp.int32, (width, LANES), 1)
        spread = jnp.tile(part(block_map, 0), (1, LANES // BLOCK))
        return jnp.where(rows % LANES // BLOCK == columns // BLOCK, spread, 0).astype(BF16)

    rate = -DECAY_SCALE * jax.nn.softplus(-part(decay_param, 0))
    mixed = mixer(
        branches, part(conv_weight, 1), dense(recur_map), dense(input_map), rate[None], reps
    )
    out_full = out_all[:width]
    gains = out_all[width : width + 2].astype(F32) + out_all[width + 2 : width + 4].astype(F32)
    mix_share = team_sum(jnp.dot(mixed, out_full, preferred_element_type=F32).astype(BF16))
    hidden_state = (resid_share + unit_rows(mix_share) * gains[0]).astype(BF16)
    mlp_input = team_gather(unit_rows(hidden_state.astype(F32)).astype(BF16))
    up_proj = jnp.dot(mlp_input, up_full, preferred_element_type=F32)
    activated = jnp.square(jax.nn.relu(up_proj * part(up_scale, 0))).astype(BF16)
    mlp_share = team_sum(jnp.dot(activated, down_full, preferred_element_type=F32).astype(BF16))
    return (hidden_state.astype(F32) + unit_rows(mlp_share) * gains[1]).astype(BF16)[None]


WEIGHTS = 4
PIECE = 256
CUTS = (2, 1, 4, 4)


def log_decay_and_drive(conv, logits, rate):
    lanes = conv.shape[1]
    log_decay = jax.nn.sigmoid(logits[:, :lanes]) * rate
    decay = jnp.exp(log_decay)
    z = -2.0 * log_decay
    series = z * (1.0 - z * (1 / 2) * (1.0 - z * (1 / 3) * (1.0 - z * (1 / 4) * (1.0 - z * (1 / 5)))))
    power = jnp.where(z < 0.1, series, 1.0 - decay * decay)
    return decay, jnp.sqrt(power) * jax.nn.sigmoid(logits[:, lanes:]) * conv.astype(F32)


def mixer_group(x_branch, gate, taps, maps, rate):
    length, count = x_branch.shape[0], taps.shape[0]
    total = taps[count - 1 : count, :] * x_branch
    for tap in range(count - 1):
        total += taps[tap : tap + 1, :] * shifted(x_branch, count - 1 - tap, 0.0)
    conv = total.astype(BF16)
    logits = lax.dot_general(conv, maps, (((1,), (1,)), ((), ())), preferred_element_type=F32)
    decay, state = log_decay_and_drive(conv, logits, rate)
    distance = 1
    while distance < length:
        state = state + decay * shifted(state, distance, 0.0)
        decay = decay * shifted(decay, distance, 1.0)
        distance *= 2
    return (state * jax.nn.gelu(gate)).astype(BF16)


def softplus_of_negative(values):
    small = jnp.exp(-jnp.abs(values))
    series = jnp.zeros_like(small)
    for term in range(8, 0, -1):
        series = small * (1.0 / term - series)
    return jnp.maximum(-values, 0.0) + jnp.where(small < 0.1, series, jnp.log(1.0 + small))


def aligned(start, unit):
    return pl.multiple_of(start, unit)


def arrival_item(item, others):
    gap = item - others + 1
    swapped = 1 - (gap * (gap - 1) + 63) // 64
    return item + swapped * (2 * others - 1 - 2 * item)


def far_lag(shards):
    others = shards // 2 - 1

    def place(index):
        if index < 2:
            return 1 - index
        kind, k = divmod(arrival_item(index - 2, others), others)
        return arrival_item((1 - kind) * others + k, others) + 2

    return next(lag for lag in range(1, shards + 1) if all(place(i) < i + lag for i in range(shards - lag)))


def layer_kernel(shards, *refs):
    count = 14
    sources, raws, outs = refs[:count], refs[count : count + 5], refs[count + 5 : count + 9]
    copies = refs[count + 9 : 2 * count + 9]
    load_sem = refs[2 * count + 9]
    loads = [
        pltpu.make_async_copy(source, copy, load_sem.at[at])
        for at, (source, copy) in enumerate(zip(sources, copies, strict=True))
    ]
    layer_body(shards, loads, *copies, *raws, *outs, *refs[2 * count + 10 :])


def layer_body(
    shards, loads, tokens, mix_pre, mix_post, mlp_pre, mlp_post, out_scale, down_scale,
    x_scale, gate_scale, up_scale, conv_weight, recur_map, input_map, decay_param,
    x_weight, gate_weight, out_weight, up_weight, down_weight, out_total, out_factor, out_hidden, out_gain,
    b_full, o_full, u_full, d_full, b_give, o_give, u_give, d_give,
    x_raw, gate_raw, o_raw, u_raw, d_raw, gains_full, gain_rows, scales, maps, rate,
    tok_got, normed, branches, mixed, mlp_in, active, hidden, lane_squares,
    give, got_near, keep, total, stage, got_far,
    raw_sem, y_sent, y_land, z_sent, b_land, o_land, u_land, d_land, zf_sent, x_sent, x_land, g_sent, g_land,
    t_sent, t_land, n_sent, n_land, f_sent, f_land, m_sent, m_land, mn_sent, mn_land, mf_sent, mf_land, out_sem,
):
    lines = shards // 2
    others = lines - 1
    rep, me, core = lax.axis_index("rep"), lax.axis_index("fs"), lax.axis_index("tp")
    z, y = me // 2, lax.rem(me, 2)
    x_peer, core_peer, y_peer = {"rep": 1 - rep}, {"tp": 1 - core}, {"fs": z * 2 + 1 - y}
    upper = z // (lines // 2)
    depth = z + upper * (lines - 1 - 2 * z)
    inner = (depth + lines - 1) // lines

    def unfold(place):
        return place + upper * (lines - 1 - 2 * place)

    def early(k):
        return 1 - (k + 2 * lines - 2 * depth) // (2 * lines)

    def other(k):
        near = depth + (1 - 2 * lax.rem(k, 2)) * (k // 2 + 1)
        return unfold(k + 1 + early(k) * (near - k - 1))

    seq, width = tokens.shape
    share = seq // 2
    columns = branches.shape[1]
    channels = columns // 2
    units = active.shape[1]
    gives = (b_give, o_give, u_give, d_give)
    fulls = (b_full, o_full, u_full, d_full)
    z_land = (b_land, o_land, u_land, d_land)

    raw_copies = [
        pltpu.make_async_copy(x_weight, x_raw, raw_sem.at[0]),
        pltpu.make_async_copy(gate_weight, gate_raw, raw_sem.at[1]),
        pltpu.make_async_copy(out_weight, o_raw, raw_sem.at[2]),
        pltpu.make_async_copy(up_weight, u_raw, raw_sem.at[3]),
        pltpu.make_async_copy(down_weight, d_raw, raw_sem.at[4]),
    ]
    for copy in raw_copies[:2] + loads[1:] + raw_copies[2:] + loads[:1]:
        copy.start()
    token_copy = loads[0]
    peers = [{"fs": lax.rem(me + step, shards)} for step in range(1, shards)] + [x_peer, core_peer]
    barrier = pltpu.get_barrier_semaphore()
    for peer in peers:
        pl.semaphore_signal(barrier, inc=1, device_id=peer, device_id_type=MESH_IDS)
    for copy in loads[1:]:
        copy.wait()
    for row, gain in enumerate((mix_pre, mix_post, mlp_pre, mlp_post)):
        gains_full[me, row : row + 1, :] = gain[...]
    chunk = 32

    def cast(count, move):
        def body(index, carry):
            move(aligned(index * chunk, chunk))
            return carry

        lax.fori_loop(0, count // chunk, body, 0)

    def branch_rows(start):
        rows = pl.ds(start, chunk)
        home = pl.ds(aligned(me * b_give.shape[0] + start, chunk), chunk)
        for at, raw in enumerate((x_raw, gate_raw)):
            place = pl.ds(at * channels, channels)
            b_full[home, place] = raw[rows, pl.ds(aligned(y * channels, LANES), channels)].astype(BF16)
            b_give[rows, place] = raw[rows, pl.ds(aligned((1 - y) * channels, LANES), channels)].astype(BF16)

    def up_rows_cast(start):
        rows = pl.ds(start, chunk)
        home = pl.ds(aligned(me * u_give.shape[0] + start, chunk), chunk)
        u_full[home, :] = u_raw[rows, pl.ds(aligned(y * units, LANES), units)].astype(BF16)
        u_give[rows, :] = u_raw[rows, pl.ds(aligned((1 - y) * units, LANES), units)].astype(BF16)

    def column_rows(full, spare, raw, scale):
        size = spare.shape[0]

        def move(start):
            home = pl.ds(aligned(me * size + start, chunk), chunk)
            full[home, :] = (raw[pl.ds(aligned(y * size + start, chunk), chunk), :] * scale[...]).astype(BF16)
            rows = pl.ds(start, chunk)
            spare[rows, :] = (raw[pl.ds(aligned((1 - y) * size + start, chunk), chunk), :] * scale[...]).astype(BF16)

        return move

    def half(w, slot, side, cut):
        rows = gives[w].shape[0]
        size = rows // (2 * CUTS[w])
        return fulls[w].at[pl.ds(aligned(slot * rows + (side * CUTS[w] + cut) * size, 32), size)]

    def whole(w, slot):
        rows = gives[w].shape[0]
        return fulls[w].at[pl.ds(aligned(slot * rows, 64), rows)]

    def y_copy(w):
        return push(gives[w], whole(w, me), y_sent.at[w], y_land.at[w], y_peer)

    def y_arrival(w):
        block = whole(w, z * 2 + 1 - y)
        return push(block, block, y_sent.at[w], y_land.at[w], y_peer)

    def z_copy(w, kind, way, cut):
        slot = z * 2 + lax.rem(y + kind, 2)
        block = half(w, slot, rep, cut)
        target = unfold(depth + 1 - 2 * way)
        return push(block, block, z_sent.at[w, way], z_land[w].at[slot, cut], {"fs": target * 2 + y})

    def start_z(w, kind):
        for cut in range(CUTS[w]):

            @pl.when(inner == 1)
            def _():
                z_copy(w, kind, 1, cut).start()

            z_copy(w, kind, 0, cut).start()

    def item_slot(kind, k):
        return other(k) * 2 + lax.rem(y + kind, 2)

    def zf_copy(w, kind, k, cut):
        slot = item_slot(kind, k)
        block = half(w, slot, rep, cut)
        target = unfold(depth - 1 + 2 * early(k) * lax.rem(k, 2))
        return push(block, block, zf_sent.at[w], z_land[w].at[slot, cut], {"fs": target * 2 + y})

    def x_copy(w, kind, k, cut):
        slot = item_slot(kind, k)
        block = half(w, slot, rep, cut)
        return push(block, block, x_sent.at[w], x_land.at[w, slot], x_peer)

    def serve(w, item, cuts=None):
        kind, k = item // others, lax.rem(item, others)
        slot = item_slot(kind, k)
        for cut in range(CUTS[w]) if cuts is None else cuts:
            block = half(w, slot, rep, cut)
            push(block, block, x_sent.at[w], z_land[w].at[slot, cut], x_peer).wait_recv()

            @pl.when(inner == 1)
            def _():
                zf_copy(w, kind, k, cut).start()

            x_copy(w, kind, k, cut).start()

    def x_arrival(w, item):
        slot = item_slot(item // others, lax.rem(item, others))
        rows = gives[w].shape[0]
        block = fulls[w].at[pl.ds(aligned(slot * rows + (1 - rep) * (rows // 2), 64), rows // 2)]
        push(block, block, x_sent.at[w], x_land.at[w, slot], x_peer).wait_recv()

    items = 2 * others

    def all_x_arrivals(w):
        def body(index, carry):
            x_arrival(w, index)
            return carry

        lax.fori_loop(0, items, body, 0)

    def when(condition, act):
        pl.when(condition)(act)

    mine = pl.ds(aligned(core * share, 64), share)
    t_near = push(tokens.at[mine], tok_got.at[mine], t_sent.at[0], t_land.at[0], y_peer)
    t_pass = push(tok_got.at[mine], tok_got.at[mine], t_sent.at[1], t_land.at[1], core_peer)

    def gain_copy(step):
        block = gains_full.at[me]
        return push(block, block, g_sent, g_land.at[me], {"fs": lax.rem(me + step, shards)})

    raw_copies[0].wait()
    raw_copies[1].wait()
    cast(b_give.shape[0], branch_rows)
    pl.semaphore_wait(barrier, len(peers))
    for step in range(1, shards):
        gain_copy(step).start()
    y_copy(0).start()
    start_z(0, 0)
    raw_copies[2].wait()
    cast(o_give.shape[0], column_rows(o_full, o_give, o_raw, out_scale))
    raw_copies[3].wait()
    cast(u_give.shape[0], up_rows_cast)
    raw_copies[4].wait()
    cast(d_give.shape[0], column_rows(d_full, d_give, d_raw, down_scale))
    y_copy(1).start()
    token_copy.wait()
    t_near.start()
    y_copy(2).start()
    y_copy(3).start()

    part = pl.ds(aligned(y * channels, LANES), channels)
    scales[:, :channels] = x_scale[:, part]
    scales[:, channels:] = gate_scale[:, part]
    rate[...] = -DECAY_SCALE * softplus_of_negative(decay_param[:, part])
    block_rows = recur_map.shape[0]
    groups = channels // LANES
    same = (
        lax.broadcasted_iota(jnp.int32, (LANES, LANES), 0) // block_rows
        == lax.broadcasted_iota(jnp.int32, (LANES, LANES), 1) // block_rows
    )
    for group in range(groups):
        lanes = pl.ds(aligned(y * channels + group * LANES, LANES), LANES)
        for at, block_map in enumerate((recur_map, input_map)):
            spread = jnp.concatenate([block_map[:, lanes].astype(F32)] * (LANES // block_rows), axis=0)
            first = (group * 2 + at) * LANES
            maps[first : first + LANES, :] = jnp.where(same, spread, 0.0).astype(BF16)

    for step in range(1, shards):
        source = lax.rem(me + step, shards)
        block = gains_full.at[source]
        push(block, block, g_sent, g_land.at[source], y_peer).wait_recv()
    piece_cols = width // shards
    for block in range(shards):
        gain_rows[:, block * piece_cols : (block + 1) * piece_cols] = gains_full[block]

    gain_out = pltpu.make_async_copy(gain_rows.at[pl.ds(3, 1)], out_gain, out_sem.at[shards + 1])
    gain_out.start()
    rows = 16

    def normalize(source, base):
        def body(index, carry):
            start = aligned(index * rows, rows)
            values = source[pl.ds(start, rows), :].astype(F32)
            values = unit_rows(values) * gain_rows[0:1, :]
            normed[pl.ds(aligned(base + start, rows), rows), :] = values.astype(BF16)
            return carry

        lax.fori_loop(0, seq // rows, body, 0)

    is_inner, is_end = inner == 1, inner == 0

    def start_other(w):
        y_arrival(w).wait_recv()
        start_z(w, 1)

    serve(0, 0)
    serve(0, 1)
    when(is_inner, lambda: serve(0, 2))
    start_other(0)
    when(is_end, lambda: start_z(1, 0))
    normalize(tokens, 0)
    when(is_end, lambda: serve(0, 2))

    @pl.when(is_end)
    def _():
        start_other(1)
        start_z(2, 0)

    serve(0, 3)
    serve(0, 4)
    serve(0, 5)
    when(is_inner, lambda: start_z(1, 0))
    serve(1, 0)
    serve(1, 1)

    @pl.when(is_inner)
    def _():
        start_other(1)
        serve(1, 2)
        serve(1, 3)
        serve(1, 4)

    all_x_arrivals(0)

    col_tiles = columns // PIECE

    def last_out():
        serve(1, 5)
        start_z(2, 0)

    def pass_tokens():
        t_near.wait_recv()
        t_pass.start()

    def branch_step(index, carry):
        row = aligned((index // col_tiles) * seq, 64)
        col = aligned(lax.rem(index, col_tiles) * PIECE, PIECE)
        value = jnp.dot(normed[pl.ds(row, seq), :], b_full[:, pl.ds(col, PIECE)], preferred_element_type=F32)
        branches[pl.ds(row, seq), pl.ds(col, PIECE)] = (value * scales[:, pl.ds(col, PIECE)]).astype(BF16)
        when(index == 0, pass_tokens)
        when(is_inner & (index == 1), last_out)

        when(is_end & (index == 0), lambda: serve(1, 3))
        when(is_end & (index == 2), lambda: serve(1, 2))
        when(is_end & (index == 6), lambda: serve(2, 0))
        when(is_end & (index == 7), lambda: start_other(2))

        return carry

    lax.fori_loop(0, col_tiles, branch_step, 0)
    t_pass.wait_recv()
    normalize(tok_got, seq)

    @pl.when(is_end)
    def _():
        serve(1, 4)
        serve(1, 5)

    lax.fori_loop(col_tiles, 2 * col_tiles, branch_step, 0)

    def up_second():
        serve(2, 1)
        start_other(2)

    def mixer_step(index, carry):
        row = aligned((index // groups) * seq, 64)
        group = lax.rem(index, groups)
        col = aligned(group * LANES, LANES)
        lanes = pl.ds(col, LANES)
        mixed[pl.ds(row, seq), lanes] = mixer_group(
            branches[pl.ds(row, seq), lanes].astype(F32),
            branches[pl.ds(row, seq), pl.ds(aligned(channels + col, LANES), LANES)].astype(F32),
            conv_weight[:, pl.ds(aligned(y * channels + col, LANES), LANES)],
            maps[pl.ds(aligned(group * 2 * LANES, LANES), 2 * LANES), :], rate[:, lanes],
        )
        when(is_inner & (index == 3), lambda: serve(2, 0))
        when(is_inner & (index == 4), up_second)
        when(is_end & (lax.rem(index, 2) == 1), lambda: serve(2, 1, (index // 2,)))
        return carry

    lax.fori_loop(0, 2 * groups, mixer_step, 0)

    def arrival(item):
        return arrival_item(item, others)

    def block_of(index, flip=0):
        item = index - 2
        safe = arrival(lax.rem(item + items, items))
        far = item_slot(safe // others + flip, lax.rem(safe, others))
        near = z * 2 + lax.rem(y + index + flip, 2)
        late = (index + shards - 2) // shards
        return near + late * (far - near)

    def near_copy(phase, block):
        return push(give.at[block], got_near.at[block], n_sent.at[phase], n_land.at[block], core_peer)

    def far_copy(phase, block):
        return push(stage.at[block], got_far.at[block], f_sent.at[phase], f_land.at[block], y_peer)

    def out_copy(block):
        cols = pl.ds(aligned(block * piece_cols, LANES), piece_cols)
        return pltpu.make_async_copy(total.at[block], out_total.at[:, cols], out_sem.at[block])

    def project(phase, w, lhs, lag, before, after):
        depth_rows = gives[w].shape[0]

        def combine(index):
            block = block_of(index)
            near_copy(phase, block).wait_recv()
            stage[block] = (keep[block] + got_near[block, 1].astype(F32)).astype(BF16)
            total[block] += got_near[block, 0].astype(F32)
            far_copy(phase, block).start()

        def body(index, carry):
            if phase == 1:
                when(index > 0, lambda: combine(index - 1))
            before(index)
            block = block_of(index)
            weight = fulls[w][pl.ds(aligned(block * depth_rows, 64), depth_rows), :]
            for side in range(2):
                left = lhs[pl.ds(aligned(side * seq + (1 - core) * share, 64), share), :]
                give[block, side] = jnp.dot(left, weight, preferred_element_type=F32).astype(BF16)
            own = lhs[pl.ds(aligned(core * share, 64), share), :]
            total[block] = jnp.dot(own, weight, preferred_element_type=F32)
            near_copy(phase, block).start()
            own = lhs[pl.ds(aligned(seq + core * share, 64), share), :]
            keep[block] = jnp.dot(own, weight, preferred_element_type=F32)
            if phase == 0:
                when(index > 0, lambda: combine(index - 1))
            if lag < shards:
                when(index >= lag, lambda: add_far(phase, index - lag))
            after(index)
            return carry

        lax.fori_loop(0, shards, body, 0)
        combine(shards - 1)

    def add_far(phase, index):
        block = block_of(index, 1)
        far_copy(phase, block).wait_recv()
        value = total[block] + got_far[block].astype(F32)
        total[block] = value
        if phase == 1:
            lane_squares[...] += sum(
                jnp.square(value[:, at : at + LANES]) for at in range(0, piece_cols, LANES)
            )
            out_copy(block).start()

    def collect(phase, lag, between):
        def body(index, carry):
            add_far(phase, index)
            between(index)
            return carry

        lax.fori_loop(shards - lag, shards, body, 0)

        push(stage, stage, f_sent.at[phase], f_land.at[0], y_peer).wait_send()
        push(give, give, n_sent.at[phase], n_land.at[0], core_peer).wait_send()

    def during_project(index):
        when(is_inner & (index == 6), lambda: serve(2, 2))
        when(is_end & (index == 0), lambda: start_z(3, 0))
        when(is_end & (lax.rem(index, 2) == 1), lambda: serve(2, 3, (index // 2,)))

    def last_up():
        serve(2, 5)
        start_z(3, 0)

    def during_sum(index):
        when(is_inner & (index == 1), lambda: serve(2, 3))
        when(is_inner & (index == 2), lambda: serve(2, 4))
        when(is_inner & (index == 5), last_up)
        when(is_end & (index == 0), lambda: start_other(3))
        when(is_end & (index >= 1) & (index < 5), lambda: serve(2, 2, (index - 1,)))
        when(is_end & (index == 5), lambda: serve(2, 4, (0, 1)))
        when(is_end & (index >= 6), lambda: serve(2, 4, (index - 4,)))

    all_x_arrivals(1)
    project(0, 1, mixed, shards, during_project, lambda index: None)
    collect(0, shards, during_sum)

    def summed(start):
        values = [total[block, pl.ds(start, rows), :] for block in range(shards)]
        squares = sum(jnp.sum(value * value, axis=-1, keepdims=True) for value in values)
        return values, lax.rsqrt(squares * (1.0 / width) + EPSILON)

    pieces = m_land.shape[0]
    piece_rows = share // pieces

    def piece(ref, base, index):
        return ref.at[pl.ds(aligned(base + index * piece_rows, 16), piece_rows)]

    def to_far(index):
        return push(
            piece(mlp_in, core * share, index), piece(mlp_in, seq + core * share, index),
            m_sent, m_land.at[index], y_peer,
        )

    def to_near(index):
        block = piece(mlp_in, core * share, index)
        return push(block, block, mn_sent, mn_land.at[index], core_peer)

    def onward(index):
        block = piece(mlp_in, seq + core * share, index)
        return push(block, block, mf_sent, mf_land.at[index], core_peer)

    def entry_piece(index, carry):
        def entry_rows(inner_index, inner_carry):
            start = aligned(index * piece_rows + inner_index * rows, rows)
            values, factor = summed(start)
            place = aligned(core * share + start, rows)
            squares = jnp.zeros((rows, 1), F32)
            kept = []
            for block in range(shards):
                cols = pl.ds(block * piece_cols, piece_cols)
                value = tokens[pl.ds(place, rows), cols].astype(F32) + values[block] * factor * gain_rows[1:2, cols]
                value = value.astype(BF16)
                hidden[pl.ds(start, rows), cols] = value
                value = value.astype(F32)
                kept.append(value)
                squares += jnp.sum(value * value, axis=-1, keepdims=True)
            scale = lax.rsqrt(squares * (1.0 / width) + EPSILON)
            for block in range(shards):
                cols = pl.ds(block * piece_cols, piece_cols)
                mlp_in[pl.ds(place, rows), cols] = (kept[block] * scale * gain_rows[2:3, cols]).astype(BF16)
            return inner_carry

        lax.fori_loop(0, piece_rows // rows, entry_rows, 0)
        to_far(index).start()
        to_near(index).start()
        return carry

    when(is_end, lambda: serve(2, 5, (0,)))
    lax.fori_loop(0, pieces, entry_piece, 0)
    hidden_out = pltpu.make_async_copy(hidden, out_hidden, out_sem.at[shards + 2])
    hidden_out.start()
    lane_squares[...] = jnp.zeros_like(lane_squares)
    when(is_end, lambda: serve(2, 5, range(1, CUTS[2])))
    serve(3, 0)

    @pl.when(is_inner)
    def _():
        serve(3, 1)
        start_other(3)
        serve(3, 2)

    all_x_arrivals(2)

    def wait_near(index, carry):
        to_near(index).wait_recv()
        return carry

    lax.fori_loop(0, pieces, wait_near, 0)
    up_tiles = units // PIECE

    def up_rows(base):
        def body(index, carry):
            col = aligned(index * PIECE, PIECE)
            value = jnp.dot(mlp_in[pl.ds(base, seq), :], u_full[:, pl.ds(col, PIECE)], preferred_element_type=F32)
            value = jnp.maximum(value * up_scale[:, pl.ds(aligned(y * units + col, PIECE), PIECE)], 0.0)
            active[pl.ds(base, seq), pl.ds(col, PIECE)] = (value * value).astype(BF16)
            return carry

        lax.fori_loop(0, up_tiles, body, 0)

    up_rows(0)
    when(is_end, lambda: serve(3, 1))

    def pass_on(index, carry):
        to_far(index).wait_recv()
        onward(index).start()
        return carry

    lax.fori_loop(0, pieces, pass_on, 0)
    when(is_end, lambda: serve(3, 3, (0, 1)))

    @pl.when(is_inner)
    def _():
        serve(3, 3)
        serve(3, 4)

    def wait_far(index, carry):
        onward(index).wait_recv()
        return carry

    lax.fori_loop(0, pieces, wait_far, 0)
    up_rows(seq)

    def before_down(index):
        when(is_inner & (index == 0), lambda: serve(3, 5))
        when(index >= 2, lambda: x_arrival(3, arrival(index - 2)))

    def after_down(index):
        when(is_end & (index >= 2) & (index < items - 2), lambda: serve(3, arrival(index + 1)))
        when(is_end & (index == items - 1), lambda: serve(3, items - 1, (0, 1)))
        when(is_end & (index == items), lambda: serve(3, items - 1, range(2, CUTS[3])))

    when(is_end, lambda: serve(3, 3, range(2, CUTS[3])))
    lag = far_lag(shards)
    project(1, 3, active, lag, before_down, after_down)
    collect(1, lag, lambda index: None)

    squares = jnp.sum(lane_squares[...], axis=-1, keepdims=True)
    lane_squares[...] = jnp.broadcast_to(lax.rsqrt(squares * (1.0 / width) + EPSILON), lane_squares.shape)
    factor_copy = pltpu.make_async_copy(lane_squares, out_factor, out_sem.at[shards])
    factor_copy.start()

    for w in range(WEIGHTS):
        y_copy(w).wait_send()
        sent = fulls[w].at[pl.ds(0, others * gives[w].shape[0])]
        own = fulls[w].at[pl.ds(0, gives[w].shape[0])]
        push(sent, sent, x_sent.at[w], x_land.at[w, 0], x_peer).wait_send()
        push(own, own, z_sent.at[w, 0], x_land.at[w, 0], x_peer).wait_send()

        @pl.when(inner == 1)
        def _():
            push(own, own, z_sent.at[w, 1], x_land.at[w, 0], x_peer).wait_send()
            push(sent, sent, zf_sent.at[w], x_land.at[w, 0], x_peer).wait_send()

    t_near.wait_send()
    t_pass.wait_send()
    most = gains_full.at[pl.ds(0, shards - 1)]
    push(most, most, g_sent, g_land.at[0], y_peer).wait_send()

    block = mlp_in.at[pl.ds(0, share)]
    for sent in (m_sent, mn_sent, mf_sent):
        push(block, block, sent, m_land.at[0], y_peer).wait_send()

    def drain(index, carry):
        out_copy(index).wait()
        return carry

    lax.fori_loop(0, shards, drain, 0)
    gain_out.wait()
    hidden_out.wait()
    factor_copy.wait()


def finish_kernel(total, factor, hidden, gain, out, total_in, factor_in, hidden_in, gain_in, result, row_sem, sem, out_sem):
    pieces = out_sem.shape[0]
    size = total.shape[0] // pieces
    near = [pltpu.make_async_copy(factor, factor_in, row_sem.at[0]), pltpu.make_async_copy(gain, gain_in, row_sem.at[1])]
    loads, stores = [], []
    for index in range(pieces):
        block = pl.ds(index * size, size)
        loads.append([
            pltpu.make_async_copy(total.at[block], total_in.at[block], sem.at[0, index]),
            pltpu.make_async_copy(hidden.at[block], hidden_in.at[block], sem.at[1, index]),
        ])
        stores.append(pltpu.make_async_copy(result.at[block], out.at[block], out_sem.at[index]))
    for copy in near + sum(loads, []):
        copy.start()
    for copy in near:
        copy.wait()
    for index in range(pieces):
        block = pl.ds(index * size, size)
        for copy in loads[index]:
            copy.wait()
        scaled = total_in[block, :] * factor_in[block, :1] * gain_in[...]
        result[block, :] = (hidden_in[block, :].astype(F32) + scaled).astype(BF16)
        stores[index].start()
    for copy in stores:
        copy.wait()


def on_device_paired(
    tokens, gain_mix_pre, gain_mix_post, gain_mlp_pre, gain_mlp_post,
    x_weight, gate_weight, x_scale, gate_scale, conv_weight, recur_map, input_map,
    decay_param, out_weight, out_scale, up_weight, up_scale, down_weight, down_scale,
):
    shards = lax.axis_size("fs")
    seq, width = tokens.shape[1:]
    share, lines, pieces = seq // 2, shards // 2, 4
    fan_in, channels, units = x_weight.shape[0], x_weight.shape[1] // 2, up_weight.shape[1] // 2
    piece_cols = width // shards
    dma = pltpu.SemaphoreType.DMA
    anywhere = pl.BlockSpec(memory_space=pl.ANY)
    part_shapes = ((fan_in, 2 * channels), (channels, piece_cols), (fan_in, units), (units, piece_cols))
    raws = (x_weight, gate_weight, out_weight, up_weight, down_weight)
    rows = [
        value[None] for value in (
            gain_mix_pre, gain_mix_post, gain_mlp_pre, gain_mlp_post, out_scale, down_scale,
            x_scale, gate_scale, up_scale,
        )
    ]
    inputs = (tokens[0], *rows, conv_weight, recur_map.T, input_map.T, decay_param[None])
    total, factor, hidden, gain = pl.pallas_call(
        functools.partial(layer_kernel, shards),
        out_shape=(
            jax.ShapeDtypeStruct((share, width), F32),
            jax.ShapeDtypeStruct((share, LANES), F32),
            jax.ShapeDtypeStruct((share, width), BF16),
            jax.ShapeDtypeStruct((1, width), F32),
        ),
        in_specs=[anywhere] * (len(inputs) + len(raws)),
        out_specs=(anywhere,) * 4,
        scratch_shapes=[pltpu.VMEM(value.shape, value.dtype) for value in inputs]
        + [dma((len(inputs),))]
        + [pltpu.VMEM((shards * shape[0], shape[1]), BF16) for shape in part_shapes]
        + [pltpu.VMEM(shape, BF16) for shape in part_shapes]
        + [pltpu.VMEM(raw.shape, F32) for raw in raws]
        + [
            pltpu.VMEM((shards, 4, piece_cols), F32),
            pltpu.VMEM((4, width), F32),
            pltpu.VMEM((1, 2 * channels), F32),
            pltpu.VMEM((2 * channels, LANES), BF16),
            pltpu.VMEM((1, channels), F32),
            pltpu.VMEM((seq, width), BF16),
            pltpu.VMEM((2 * seq, width), BF16),
            pltpu.VMEM((2 * seq, 2 * channels), BF16),
            pltpu.VMEM((2 * seq, channels), BF16),
            pltpu.VMEM((2 * seq, width), BF16),
            pltpu.VMEM((2 * seq, units), BF16),
            pltpu.VMEM((share, width), BF16),
            pltpu.VMEM((share, LANES), F32),
            pltpu.VMEM((shards, 2, share, piece_cols), BF16),
            pltpu.VMEM((shards, 2, share, piece_cols), BF16),
            pltpu.VMEM((shards, share, piece_cols), F32),
            pltpu.VMEM((shards, share, piece_cols), F32),
            pltpu.VMEM((shards, share, piece_cols), BF16),
            pltpu.VMEM((shards, share, piece_cols), BF16),
            dma((len(raws),)), dma((WEIGHTS,)), dma((WEIGHTS,)),
            dma((WEIGHTS, 2)), *[dma((shards, cuts)) for cuts in CUTS], dma((WEIGHTS,)),
            dma((WEIGHTS,)), dma((WEIGHTS, shards)),
            dma, dma((shards,)),
            dma((2,)), dma((2,)),
            dma((2,)), dma((shards,)), dma((2,)), dma((shards,)),
            dma, dma((pieces,)), dma, dma((pieces,)), dma, dma((pieces,)), dma((shards + 3,)),
        ],
        compiler_params=pltpu.CompilerParams(
            collective_id=4, has_side_effects=True, vmem_limit_bytes=67_000_000
        ),
        cost_estimate=pl.CostEstimate(flops=20_000_000_000, bytes_accessed=80_000_000, transcendentals=0),
        name="layer",
    )(*inputs, *raws)
    finals = (total, factor, hidden, gain)
    return pl.pallas_call(
        finish_kernel,
        in_specs=[anywhere] * len(finals),
        out_specs=anywhere,
        out_shape=jax.ShapeDtypeStruct((share, width), BF16),
        scratch_shapes=[pltpu.VMEM(value.shape, value.dtype) for value in finals]
        + [pltpu.VMEM((share, width), BF16), dma((2,)), dma((2, pieces)), dma((pieces,))],
        name="finish",
    )(*finals)[None]


def solution(mesh):
    in_specs = (
        P(("rep", "fs"), None, None),
        P("fs"), P("fs"), P("fs"), P("fs"),
        P("fs", "tp"), P("fs", "tp"),
        P("tp"), P("tp"),
        P(None, "tp"), P("tp", None), P("tp", None), P("tp"),
        P("tp", "fs"), P("fs"),
        P("fs", "tp"), P("tp"),
        P("tp", "fs"), P("fs"),
    )
    out_specs = P(("rep", "fs"), "tp", None)
    paired = (
        mesh.shape["rep"] == 2 and mesh.shape["tp"] == 2
        and mesh.shape["fs"] % 4 == 0 and 4 < mesh.shape["fs"] < 16
    )
    return jax.shard_map(
        on_device_paired if paired else on_device, mesh=mesh, in_specs=in_specs, out_specs=out_specs, check_vma=False
    )
```

```python
import functools

import jax
import jax.numpy as jnp
from jax import lax
from jax.experimental import pallas as pl
from jax.experimental.pallas import tpu as pltpu
from jax.sharding import PartitionSpec as P

BLOCK = 32
LANES = 128
EPSILON = 1e-06
DECAY_SCALE = 8.0
F32 = jnp.float32
BF16 = jnp.bfloat16


def unit_rows(values):
    return values * lax.rsqrt(jnp.mean(values * values, axis=-1, keepdims=True) + EPSILON)


def shifted(values, distance, fill):
    head = jnp.full((distance, values.shape[1]), fill, values.dtype)
    return jnp.concatenate([head, values[: values.shape[0] - distance]], axis=0)


def mixer_kernel(x_ref, gate_ref, taps_ref, recur_ref, input_ref, rate_ref, mixed_ref):
    length = x_ref.shape[0]
    x_branch = x_ref[...].astype(F32)
    taps = taps_ref.shape[0]
    total = taps_ref[taps - 1 : taps, :] * x_branch
    for tap in range(taps - 1):
        total += taps_ref[tap : tap + 1, :] * shifted(x_branch, taps - 1 - tap, 0.0)
    conv = total.astype(BF16)
    recur = jax.nn.sigmoid(jnp.dot(conv, recur_ref[...], preferred_element_type=F32))
    gate_in = jax.nn.sigmoid(jnp.dot(conv, input_ref[...], preferred_element_type=F32))
    log_decay = recur * rate_ref[0:1, :]
    decay = jnp.exp(log_decay)
    z = -2.0 * log_decay
    series = z * (1.0 - z * (1 / 2) * (1.0 - z * (1 / 3) * (1.0 - z * (1 / 4) * (1.0 - z * (1 / 5)))))
    power = jnp.where(z < 0.1, series, 1.0 - decay * decay)
    state = jnp.sqrt(power) * gate_in * conv.astype(F32)
    distance = 1
    while distance < length:
        state = state + decay * shifted(state, distance, 0.0)
        decay = decay * shifted(decay, distance, 1.0)
        distance *= 2
    mixed_ref[...] = (state * jax.nn.gelu(gate_ref[...].astype(F32))).astype(BF16)


def mixer(branches, taps, recur_dense, input_dense, rate, sequences):
    rows, width = branches.shape[0], branches.shape[1] // 2
    length = rows // sequences
    groups = width // LANES
    return pl.pallas_call(
        mixer_kernel,
        grid=(sequences, groups),
        in_specs=[
            pl.BlockSpec((length, LANES), lambda s, g: (s, g)),
            pl.BlockSpec((length, LANES), lambda s, g: (s, g + groups)),
            pl.BlockSpec((taps.shape[0], LANES), lambda s, g: (0, g)),
            pl.BlockSpec((LANES, LANES), lambda s, g: (g, 0)),
            pl.BlockSpec((LANES, LANES), lambda s, g: (g, 0)),
            pl.BlockSpec((1, LANES), lambda s, g: (0, g)),
        ],
        out_specs=pl.BlockSpec((length, LANES), lambda s, g: (s, g)),
        out_shape=jax.ShapeDtypeStruct((rows, width), BF16),
        cost_estimate=pl.CostEstimate(
            flops=rows * width * 100, bytes_accessed=rows * width * 6, transcendentals=rows * width * 4
        ),
        name="mixer",
    )(branches, branches, taps, recur_dense, input_dense, rate)


MESH_IDS = pl.DeviceIdType.MESH


def greet(peers):
    barrier = pltpu.get_barrier_semaphore()
    for peer in peers:
        pl.semaphore_signal(barrier, inc=1, device_id=peer, device_id_type=MESH_IDS)
    pl.semaphore_wait(barrier, len(peers))


def push(source, target, sent, landed, peer):
    return pltpu.make_async_remote_copy(
        src_ref=source, dst_ref=target, send_sem=sent, recv_sem=landed,
        device_id=peer, device_id_type=MESH_IDS,
    )


def others(axis, count):
    me = lax.axis_index(axis)
    return [lax.rem(me + step, count) for step in range(1, count)]


def row_block(ref, index, rows):
    return ref.at[pl.ds(pl.multiple_of(index * rows, rows), rows)]


def team_gather_kernel(reps, tps, x_ref, out_ref, own_sem, sent, landed):
    rep, core = lax.axis_index("rep"), lax.axis_index("tp")
    rows = x_ref.shape[0]
    rep_peers, tp_peers = others("rep", reps), others("tp", tps)
    greet([{"rep": peer} for peer in rep_peers] + [{"tp": peer} for peer in tp_peers])
    mine = row_block(out_ref, rep * tps + core, rows)
    flights = []
    for step, peer in enumerate(rep_peers):
        copy = push(x_ref, mine, sent.at[step + 1, 0], landed.at[step + 1, 0], {"rep": peer})
        copy.start()
        flights.append(copy)
    own = pltpu.make_async_copy(x_ref, mine, own_sem)
    own.start()
    local = []
    for slot, peer in enumerate(tp_peers):
        copy = push(x_ref, mine, sent.at[0, slot + 1], landed.at[0, slot + 1], {"tp": peer})
        copy.start()
        local.append(copy)
    for step in range(1, reps):
        flights[step - 1].wait_recv()
        source = lax.rem(rep + reps - step, reps)
        block = row_block(out_ref, source * tps + core, rows)
        for slot, peer in enumerate(tp_peers):
            copy = push(block, block, sent.at[step, slot + 1], landed.at[step, slot + 1], {"tp": peer})
            copy.start()
            local.append(copy)
    for copy in flights:
        copy.wait_send()
    for copy in local:
        copy.wait()
    own.wait()


def team_gather(values):
    reps, tps = lax.axis_size("rep"), lax.axis_size("tp")
    rows, width = values.shape
    return pl.pallas_call(
        functools.partial(team_gather_kernel, reps, tps),
        out_shape=jax.ShapeDtypeStruct((rows * reps * tps, width), values.dtype),
        in_specs=[pl.BlockSpec(memory_space=pltpu.VMEM)],
        out_specs=pl.BlockSpec(memory_space=pltpu.VMEM),
        scratch_shapes=[
            pltpu.SemaphoreType.DMA,
            pltpu.SemaphoreType.DMA((reps, tps)),
            pltpu.SemaphoreType.DMA((reps, tps)),
        ],
        compiler_params=pltpu.CompilerParams(collective_id=0, has_side_effects=True),
        cost_estimate=pl.CostEstimate(flops=0, bytes_accessed=80_000_000, transcendentals=0),
        name="team_gather",
    )(values)


def team_sum_kernel(reps, tps, part_ref, out_ref, got, stage, last, sent, landed, sent_far, landed_far):
    rep, core = lax.axis_index("rep"), lax.axis_index("tp")
    rows = out_ref.shape[0]
    step_rows = 16
    rep_peers, tp_peers = others("rep", reps), others("tp", tps)
    greet([{"rep": peer} for peer in rep_peers] + [{"tp": peer} for peer in tp_peers])
    near = []
    for slot, peer in enumerate(tp_peers):
        for group in range(reps):
            copy = push(
                row_block(part_ref, group * tps + peer, rows), got.at[slot, group],
                sent.at[slot, group], landed.at[slot, group], {"tp": peer},
            )
            copy.start()
            near.append(copy)
    for copy in near:
        copy.wait()

    def total(group, start):
        base = pl.multiple_of((group * tps + core) * rows + start, step_rows)
        value = part_ref[pl.ds(base, step_rows)].astype(F32)
        for slot in range(tps - 1):
            value += got[slot, group, pl.ds(start, step_rows)].astype(F32)
        return value

    far = []
    for step, peer in enumerate(rep_peers):

        def fill(index, carry):
            start = pl.multiple_of(index * step_rows, step_rows)
            stage[step, pl.ds(start, step_rows)] = total(peer, start).astype(BF16)
            return carry

        lax.fori_loop(0, rows // step_rows, fill, 0)
        copy = push(stage.at[step], last.at[step], sent_far.at[step], landed_far.at[step], {"rep": peer})
        copy.start()
        far.append(copy)
    for copy in far:
        copy.wait()

    def finish(index, carry):
        start = pl.multiple_of(index * step_rows, step_rows)
        value = total(rep, start)
        for step in range(reps - 1):
            value += last[step, pl.ds(start, step_rows)].astype(F32)
        out_ref[pl.ds(start, step_rows)] = value
        return carry

    lax.fori_loop(0, rows // step_rows, finish, 0)


def team_sum(parts):
    reps, tps = lax.axis_size("rep"), lax.axis_size("tp")
    rows, width = parts.shape[0] // (reps * tps), parts.shape[1]
    return pl.pallas_call(
        functools.partial(team_sum_kernel, reps, tps),
        out_shape=jax.ShapeDtypeStruct((rows, width), F32),
        in_specs=[pl.BlockSpec(memory_space=pltpu.VMEM)],
        out_specs=pl.BlockSpec(memory_space=pltpu.VMEM),
        scratch_shapes=[
            pltpu.VMEM((tps - 1, reps, rows, width), BF16),
            pltpu.VMEM((reps - 1, rows, width), BF16),
            pltpu.VMEM((reps - 1, rows, width), BF16),
            pltpu.SemaphoreType.DMA((tps - 1, reps)),
            pltpu.SemaphoreType.DMA((tps - 1, reps)),
            pltpu.SemaphoreType.DMA((reps - 1,)),
            pltpu.SemaphoreType.DMA((reps - 1,)),
        ],
        compiler_params=pltpu.CompilerParams(collective_id=1, has_side_effects=True),
        cost_estimate=pl.CostEstimate(flops=0, bytes_accessed=80_000_000, transcendentals=0),
        name="team_sum",
    )(parts)


def shard_gather_kernel(shards, x_ref, out_ref, own_sem, sent, landed, sent_pass, landed_pass):
    me = lax.axis_index("fs")
    rows = x_ref.shape[0]
    pairs = shards // 2
    pair, parity = me // 2, lax.rem(me, 2)
    partner = {"fs": pair * 2 + 1 - parity}
    peers = [{"fs": lax.rem(pair + step, pairs) * 2 + parity} for step in range(1, pairs)]
    greet([partner] + peers)
    mine = row_block(out_ref, me, rows)
    passed = [push(x_ref, mine, sent_pass.at[0], landed_pass.at[0], partner)]
    passed[0].start()
    direct = []
    for step, peer in enumerate(peers):
        copy = push(x_ref, mine, sent.at[step], landed.at[step], peer)
        copy.start()
        direct.append(copy)
    own = pltpu.make_async_copy(x_ref, mine, own_sem)
    own.start()
    for step in range(1, pairs):
        direct[step - 1].wait_recv()
        block = row_block(out_ref, lax.rem(pair + pairs - step, pairs) * 2 + parity, rows)
        copy = push(block, block, sent_pass.at[step], landed_pass.at[step], partner)
        copy.start()
        passed.append(copy)
    for copy in direct:
        copy.wait_send()
    for copy in passed:
        copy.wait()
    own.wait()


def shard_gather(values, collective_id):
    shards = lax.axis_size("fs")
    rows, width = values.shape
    return pl.pallas_call(
        functools.partial(shard_gather_kernel, shards),
        out_shape=jax.ShapeDtypeStruct((rows * shards, width), values.dtype),
        in_specs=[pl.BlockSpec(memory_space=pltpu.VMEM)],
        out_specs=pl.BlockSpec(memory_space=pltpu.VMEM),
        scratch_shapes=[
            pltpu.SemaphoreType.DMA,
            pltpu.SemaphoreType.DMA((shards // 2,)),
            pltpu.SemaphoreType.DMA((shards // 2,)),
            pltpu.SemaphoreType.DMA((shards // 2,)),
            pltpu.SemaphoreType.DMA((shards // 2,)),
        ],
        compiler_params=pltpu.CompilerParams(collective_id=collective_id, has_side_effects=True),
        cost_estimate=pl.CostEstimate(flops=0, bytes_accessed=200_000_000, transcendentals=0),
        name="shard_gather",
    )(values)


def on_device(
    tokens, gain_mix_pre, gain_mix_post, gain_mlp_pre, gain_mlp_post,
    x_weight, gate_weight, x_scale, gate_scale, conv_weight, recur_map, input_map,
    decay_param, out_weight, out_scale, up_weight, up_scale, down_weight, down_scale,
):
    reps = lax.axis_size("rep")
    rep = lax.axis_index("rep")

    def part(values, axis):
        size = values.shape[axis] // reps
        return lax.dynamic_slice_in_dim(values, rep * size, size, axis)

    length = tokens.shape[1]
    share_rows = length // lax.axis_size("tp")
    offset_row = lax.axis_index("tp") * share_rows
    resid_share = lax.dynamic_slice_in_dim(tokens[0], offset_row, share_rows, 0).astype(F32)
    normed_share = unit_rows(resid_share).astype(BF16)

    pre = gain_mix_pre[:, None]
    branch_rows = jnp.concatenate(
        [(part(x_weight, 1) * pre).astype(BF16), (part(gate_weight, 1) * pre).astype(BF16)], axis=1
    )
    branch_rows, out_weight = lax.optimization_barrier((branch_rows, out_weight))
    branch_full = lax.all_gather(branch_rows, "fs", axis=0, tiled=True)
    post = jnp.stack([gain_mix_post, gain_mlp_post])
    post_high = post.astype(BF16)
    post_low = (post - post_high.astype(F32)).astype(BF16)
    pad_rows = jnp.zeros((12, post.shape[1]), BF16)
    out_cols = jnp.concatenate(
        [(part(out_weight, 0) * out_scale).astype(BF16), post_high, post_low, pad_rows], axis=0
    )
    out_cols, down_weight = lax.optimization_barrier((out_cols, down_weight))
    out_all = lax.all_gather(out_cols, "fs", axis=1, tiled=True)
    down_full = lax.all_gather((part(down_weight, 0) * down_scale).astype(BF16), "fs", axis=1, tiled=True)
    up_rows = (part(up_weight, 1) * gain_mlp_pre[:, None]).astype(BF16)
    normed = team_gather(normed_share)
    normed, up_rows = lax.optimization_barrier((normed, up_rows))
    up_full = shard_gather(up_rows, 2)
    normed, up_full = lax.optimization_barrier((normed, up_full))

    scales = jnp.concatenate([part(x_scale, 0), part(gate_scale, 0)])
    branches = (jnp.dot(normed, branch_full, preferred_element_type=F32) * scales).astype(BF16)
    width = branches.shape[1] // 2

    def dense(block_map):
        rows = lax.broadcasted_iota(jnp.int32, (width, LANES), 0)
        columns = lax.broadcasted_iota(jnp.int32, (width, LANES), 1)
        spread = jnp.tile(part(block_map, 0), (1, LANES // BLOCK))
        return jnp.where(rows % LANES // BLOCK == columns // BLOCK, spread, 0).astype(BF16)

    rate = -DECAY_SCALE * jax.nn.softplus(-part(decay_param, 0))
    mixed = mixer(
        branches, part(conv_weight, 1), dense(recur_map), dense(input_map), rate[None], reps
    )
    out_full = out_all[:width]
    gains = out_all[width : width + 2].astype(F32) + out_all[width + 2 : width + 4].astype(F32)
    mix_share = team_sum(jnp.dot(mixed, out_full, preferred_element_type=F32).astype(BF16))
    hidden_state = (resid_share + unit_rows(mix_share) * gains[0]).astype(BF16)
    mlp_input = team_gather(unit_rows(hidden_state.astype(F32)).astype(BF16))
    up_proj = jnp.dot(mlp_input, up_full, preferred_element_type=F32)
    activated = jnp.square(jax.nn.relu(up_proj * part(up_scale, 0))).astype(BF16)
    mlp_share = team_sum(jnp.dot(activated, down_full, preferred_element_type=F32).astype(BF16))
    return (hidden_state.astype(F32) + unit_rows(mlp_share) * gains[1]).astype(BF16)[None]


WEIGHTS = 4
PIECE = 256
CUTS = (4, 1, 4, 4)


def log_decay_and_drive(conv, logits, rate):
    lanes = conv.shape[1]
    log_decay = jax.nn.sigmoid(logits[:, :lanes]) * rate
    decay = jnp.exp(log_decay)
    z = -2.0 * log_decay
    series = z * (1.0 - z * (1 / 2) * (1.0 - z * (1 / 3) * (1.0 - z * (1 / 4) * (1.0 - z * (1 / 5)))))
    power = jnp.where(z < 0.1, series, 1.0 - decay * decay)
    return decay, jnp.sqrt(power) * jax.nn.sigmoid(logits[:, lanes:]) * conv.astype(F32)


def mixer_group(x_branch, gate, taps, maps, rate):
    length, count = x_branch.shape[0], taps.shape[0]
    total = taps[count - 1 : count, :] * x_branch
    for tap in range(count - 1):
        total += taps[tap : tap + 1, :] * shifted(x_branch, count - 1 - tap, 0.0)
    conv = total.astype(BF16)
    logits = lax.dot_general(conv, maps, (((1,), (1,)), ((), ())), preferred_element_type=F32)
    decay, state = log_decay_and_drive(conv, logits, rate)
    distance = 1
    while distance < length:
        state = state + decay * shifted(state, distance, 0.0)
        decay = decay * shifted(decay, distance, 1.0)
        distance *= 2
    return (state * jax.nn.gelu(gate)).astype(BF16)


def softplus_of_negative(values):
    small = jnp.exp(-jnp.abs(values))
    series = jnp.zeros_like(small)
    for term in range(8, 0, -1):
        series = small * (1.0 / term - series)
    return jnp.maximum(-values, 0.0) + jnp.where(small < 0.1, series, jnp.log(1.0 + small))


def aligned(start, unit):
    return pl.multiple_of(start, unit)


def arrival_item(item, others):
    gap = item - others + 1
    swapped = 1 - (gap * (gap - 1) + 63) // 64
    return item + swapped * (2 * others - 1 - 2 * item)


def far_lag(shards):
    others = shards // 2 - 1

    def place(index):
        if index < 2:
            return 1 - index
        kind, k = divmod(arrival_item(index - 2, others), others)
        return arrival_item((1 - kind) * others + k, others) + 2

    return next(lag for lag in range(1, shards + 1) if all(place(i) < i + lag for i in range(shards - lag)))


def layer_kernel(shards, *refs):
    count = 14
    sources, raws, outs = refs[:count], refs[count : count + 5], refs[count + 5 : count + 9]
    copies = refs[count + 9 : 2 * count + 9]
    load_sem = refs[2 * count + 9]
    loads = [
        pltpu.make_async_copy(source, copy, load_sem.at[at])
        for at, (source, copy) in enumerate(zip(sources, copies, strict=True))
    ]
    layer_body(shards, loads, *copies, *raws, *outs, *refs[2 * count + 10 :])


def layer_body(
    shards, loads, tokens, mix_pre, mix_post, mlp_pre, mlp_post, out_scale, down_scale,
    x_scale, gate_scale, up_scale, conv_weight, recur_map, input_map, decay_param,
    x_weight, gate_weight, out_weight, up_weight, down_weight, out_total, out_factor, out_hidden, out_gain,
    b_full, o_full, u_full, d_full, b_give, o_give, u_give, d_give,
    x_raw, gate_raw, o_raw, u_raw, d_raw, gains_full, gain_rows, scales, maps, rate,
    tok_got, normed, branches, mixed, mlp_in, active, hidden, lane_squares,
    give, got_near, keep, total, stage, got_far,
    raw_sem, y_sent, y_land, z_sent, b_land, o_land, u_land, d_land, zf_sent, x_sent, x_land, g_sent, g_land,
    t_sent, t_land, n_sent, n_land, f_sent, f_land, m_sent, m_land, mn_sent, mn_land, mf_sent, mf_land, out_sem,
):
    lines = shards // 2
    others = lines - 1
    rep, me, core = lax.axis_index("rep"), lax.axis_index("fs"), lax.axis_index("tp")
    z, y = me // 2, lax.rem(me, 2)
    x_peer, core_peer, y_peer = {"rep": 1 - rep}, {"tp": 1 - core}, {"fs": z * 2 + 1 - y}
    upper = z // (lines // 2)
    depth = z + upper * (lines - 1 - 2 * z)
    inner = (depth + lines - 1) // lines

    def unfold(place):
        return place + upper * (lines - 1 - 2 * place)

    def early(k):
        return 1 - (k + 2 * lines - 2 * depth) // (2 * lines)

    def other(k):
        near = depth + (1 - 2 * lax.rem(k, 2)) * (k // 2 + 1)
        return unfold(k + 1 + early(k) * (near - k - 1))

    seq, width = tokens.shape
    share = seq // 2
    columns = branches.shape[1]
    channels = columns // 2
    units = active.shape[1]
    gives = (b_give, o_give, u_give, d_give)
    fulls = (b_full, o_full, u_full, d_full)
    z_land = (b_land, o_land, u_land, d_land)

    raw_copies = [
        pltpu.make_async_copy(x_weight, x_raw, raw_sem.at[0]),
        pltpu.make_async_copy(gate_weight, gate_raw, raw_sem.at[1]),
        pltpu.make_async_copy(out_weight, o_raw, raw_sem.at[2]),
        pltpu.make_async_copy(up_weight, u_raw, raw_sem.at[3]),
        pltpu.make_async_copy(down_weight, d_raw, raw_sem.at[4]),
    ]
    for copy in raw_copies[:2] + loads[1:] + raw_copies[2:] + loads[:1]:
        copy.start()
    token_copy = loads[0]
    peers = [{"fs": lax.rem(me + step, shards)} for step in range(1, shards)] + [x_peer, core_peer]
    barrier = pltpu.get_barrier_semaphore()
    for peer in peers:
        pl.semaphore_signal(barrier, inc=1, device_id=peer, device_id_type=MESH_IDS)
    for copy in loads[1:]:
        copy.wait()
    for row, gain in enumerate((mix_pre, mix_post, mlp_pre, mlp_post)):
        gains_full[me, row : row + 1, :] = gain[...]
    chunk = 32

    def cast(count, move):
        def body(index, carry):
            move(aligned(index * chunk, chunk))
            return carry

        lax.fori_loop(0, count // chunk, body, 0)

    def branch_rows(start):
        rows = pl.ds(start, chunk)
        home = pl.ds(aligned(me * b_give.shape[0] + start, chunk), chunk)
        for at, raw in enumerate((x_raw, gate_raw)):
            place = pl.ds(at * channels, channels)
            b_full[home, place] = raw[rows, pl.ds(aligned(y * channels, LANES), channels)].astype(BF16)
            b_give[rows, place] = raw[rows, pl.ds(aligned((1 - y) * channels, LANES), channels)].astype(BF16)

    def up_rows_cast(start):
        rows = pl.ds(start, chunk)
        home = pl.ds(aligned(me * u_give.shape[0] + start, chunk), chunk)
        u_full[home, :] = u_raw[rows, pl.ds(aligned(y * units, LANES), units)].astype(BF16)
        u_give[rows, :] = u_raw[rows, pl.ds(aligned((1 - y) * units, LANES), units)].astype(BF16)

    def column_rows(full, spare, raw, scale):
        size = spare.shape[0]

        def move(start):
            home = pl.ds(aligned(me * size + start, chunk), chunk)
            full[home, :] = (raw[pl.ds(aligned(y * size + start, chunk), chunk), :] * scale[...]).astype(BF16)
            rows = pl.ds(start, chunk)
            spare[rows, :] = (raw[pl.ds(aligned((1 - y) * size + start, chunk), chunk), :] * scale[...]).astype(BF16)

        return move

    def half(w, slot, side, cut):
        rows = gives[w].shape[0]
        size = rows // (2 * CUTS[w])
        return fulls[w].at[pl.ds(aligned(slot * rows + (side * CUTS[w] + cut) * size, 32), size)]

    def whole(w, slot):
        rows = gives[w].shape[0]
        return fulls[w].at[pl.ds(aligned(slot * rows, 64), rows)]

    def y_copy(w):
        return push(gives[w], whole(w, me), y_sent.at[w], y_land.at[w], y_peer)

    def y_arrival(w):
        block = whole(w, z * 2 + 1 - y)
        return push(block, block, y_sent.at[w], y_land.at[w], y_peer)

    def z_copy(w, kind, way, cut):
        slot = z * 2 + lax.rem(y + kind, 2)
        block = half(w, slot, rep, cut)
        target = unfold(depth + 1 - 2 * way)
        return push(block, block, z_sent.at[w, way], z_land[w].at[slot, cut], {"fs": target * 2 + y})

    def start_z(w, kind):
        for cut in range(CUTS[w]):

            @pl.when(inner == 1)
            def _():
                z_copy(w, kind, 1, cut).start()

            z_copy(w, kind, 0, cut).start()

    def item_slot(kind, k):
        return other(k) * 2 + lax.rem(y + kind, 2)

    def zf_copy(w, kind, k, cut):
        slot = item_slot(kind, k)
        block = half(w, slot, rep, cut)
        target = unfold(depth - 1 + 2 * early(k) * lax.rem(k, 2))
        return push(block, block, zf_sent.at[w], z_land[w].at[slot, cut], {"fs": target * 2 + y})

    def x_sem(w, slot):
        return x_land.at[w + slot if w == WEIGHTS - 1 else w]

    def x_copy(w, kind, k, cut):
        slot = item_slot(kind, k)
        block = half(w, slot, rep, cut)
        return push(block, block, x_sent.at[w], x_sem(w, slot), x_peer)

    def serve(w, item, cuts=None):
        kind, k = item // others, lax.rem(item, others)
        slot = item_slot(kind, k)
        for cut in range(CUTS[w]) if cuts is None else cuts:
            block = half(w, slot, rep, cut)
            push(block, block, x_sent.at[w], z_land[w].at[slot, cut], x_peer).wait_recv()

            @pl.when(inner == 1)
            def _():
                zf_copy(w, kind, k, cut).start()

            x_copy(w, kind, k, cut).start()

    def x_arrival(w, item):
        slot = item_slot(item // others, lax.rem(item, others))
        rows = gives[w].shape[0]
        block = fulls[w].at[pl.ds(aligned(slot * rows + (1 - rep) * (rows // 2), 64), rows // 2)]
        push(block, block, x_sent.at[w], x_sem(w, slot), x_peer).wait_recv()

    items = 2 * others

    def all_x_arrivals(w):
        block = fulls[w].at[pl.ds(0, others * gives[w].shape[0])]
        push(block, block, x_sent.at[w], x_land.at[w], x_peer).wait_recv()

    def when(condition, act):
        pl.when(condition)(act)

    mine = pl.ds(aligned(core * share, 64), share)
    t_near = push(tokens.at[mine], tok_got.at[mine], t_sent.at[0], t_land.at[0], y_peer)
    t_pass = push(tok_got.at[mine], tok_got.at[mine], t_sent.at[1], t_land.at[1], core_peer)

    def gain_copy(step):
        block = gains_full.at[me]
        return push(block, block, g_sent, g_land, {"fs": lax.rem(me + step, shards)})

    raw_copies[0].wait()
    raw_copies[1].wait()
    cast(b_give.shape[0], branch_rows)
    pl.semaphore_wait(barrier, len(peers))
    for step in range(1, shards):
        gain_copy(step).start()
    y_copy(0).start()
    start_z(0, 0)
    raw_copies[2].wait()
    cast(o_give.shape[0], column_rows(o_full, o_give, o_raw, out_scale))
    raw_copies[3].wait()
    cast(u_give.shape[0], up_rows_cast)
    raw_copies[4].wait()
    cast(d_give.shape[0], column_rows(d_full, d_give, d_raw, down_scale))
    y_copy(1).start()
    token_copy.wait()
    t_near.start()
    y_copy(2).start()
    y_copy(3).start()

    part = pl.ds(aligned(y * channels, LANES), channels)
    scales[:, :channels] = x_scale[:, part]
    scales[:, channels:] = gate_scale[:, part]
    rate[...] = -DECAY_SCALE * softplus_of_negative(decay_param[:, part])
    block_rows = recur_map.shape[0]
    groups = channels // LANES
    same = (
        lax.broadcasted_iota(jnp.int32, (LANES, LANES), 0) // block_rows
        == lax.broadcasted_iota(jnp.int32, (LANES, LANES), 1) // block_rows
    )
    for group in range(groups):
        lanes = pl.ds(aligned(y * channels + group * LANES, LANES), LANES)
        for at, block_map in enumerate((recur_map, input_map)):
            spread = jnp.concatenate([block_map[:, lanes].astype(F32)] * (LANES // block_rows), axis=0)
            first = (group * 2 + at) * LANES
            maps[first : first + LANES, :] = jnp.where(same, spread, 0.0).astype(BF16)

    most = gains_full.at[pl.ds(0, shards - 1)]
    push(most, most, g_sent, g_land, y_peer).wait_recv()
    piece_cols = width // shards
    for block in range(shards):
        gain_rows[:, block * piece_cols : (block + 1) * piece_cols] = gains_full[block]

    gain_out = pltpu.make_async_copy(gain_rows.at[pl.ds(3, 1)], out_gain, out_sem.at[shards + 1])
    gain_out.start()
    rows = 16

    def normalize(source, base, first, last):
        def body(index, carry):
            start = aligned(index * rows, rows)
            values = source[pl.ds(start, rows), :].astype(F32)
            values = unit_rows(values) * gain_rows[0:1, :]
            normed[pl.ds(aligned(base + start, rows), rows), :] = values.astype(BF16)
            return carry

        lax.fori_loop(first // rows, last // rows, body, 0)

    is_inner, is_end = inner == 1, inner == 0

    def start_other(w):
        y_arrival(w).wait_recv()
        start_z(w, 1)

    serve(0, 0)
    serve(0, 1)
    when(is_inner, lambda: serve(0, 2))
    start_other(0)
    when(is_end, lambda: start_z(1, 0))
    normalize(tokens, 0, 0, seq)
    when(is_end, lambda: serve(0, 2))

    @pl.when(is_end)
    def _():
        start_other(1)
        start_z(2, 0)

    serve(0, 3)
    serve(0, 4)
    serve(0, 5)
    when(is_inner, lambda: start_z(1, 0))
    serve(1, 0)
    serve(1, 1)

    @pl.when(is_inner)
    def _():
        start_other(1)
        serve(1, 2)
        serve(1, 3)
        serve(1, 4)

    all_x_arrivals(0)

    col_tiles = columns // PIECE

    def last_out():
        serve(1, 5)
        start_z(2, 0)

    def pass_tokens():
        t_near.wait_recv()
        t_pass.start()

    def branch_step(index, carry):
        row = aligned((index // col_tiles) * seq, 64)
        col = aligned(lax.rem(index, col_tiles) * PIECE, PIECE)
        value = jnp.dot(normed[pl.ds(row, seq), :], b_full[:, pl.ds(col, PIECE)], preferred_element_type=F32)
        branches[pl.ds(row, seq), pl.ds(col, PIECE)] = (value * scales[:, pl.ds(col, PIECE)]).astype(BF16)
        when(index == 0, pass_tokens)
        when(is_inner & (index == 1), last_out)

        when(is_end & (index == 0), lambda: serve(1, 3))
        when(is_end & (index == 2), lambda: serve(1, 2))
        when(is_end & (index == 6), lambda: serve(2, 0))
        when(is_end & (index == 7), lambda: start_other(2))

        return carry

    lax.fori_loop(0, col_tiles, branch_step, 0)
    t_pass.wait_recv()
    normalize(tok_got, seq, 0, share)
    when(is_end, lambda: serve(1, 4))
    normalize(tok_got, seq, share, seq)
    when(is_end, lambda: serve(1, 5))

    lax.fori_loop(col_tiles, 2 * col_tiles, branch_step, 0)

    def up_second():
        serve(2, 1)
        start_other(2)

    def mixer_step(index, carry):
        row = aligned((index // groups) * seq, 64)
        group = lax.rem(index, groups)
        col = aligned(group * LANES, LANES)
        lanes = pl.ds(col, LANES)
        mixed[pl.ds(row, seq), lanes] = mixer_group(
            branches[pl.ds(row, seq), lanes].astype(F32),
            branches[pl.ds(row, seq), pl.ds(aligned(channels + col, LANES), LANES)].astype(F32),
            conv_weight[:, pl.ds(aligned(y * channels + col, LANES), LANES)],
            maps[pl.ds(aligned(group * 2 * LANES, LANES), 2 * LANES), :], rate[:, lanes],
        )
        when(is_inner & (index == 3), lambda: serve(2, 0))
        when(is_inner & (index == 4), up_second)
        when(is_end & (lax.rem(index, 2) == 1), lambda: serve(2, 1, (index // 2,)))
        return carry

    lax.fori_loop(0, 2 * groups, mixer_step, 0)

    def arrival(item):
        return arrival_item(item, others)

    def block_of(index, flip=0):
        item = index - 2
        safe = arrival(lax.rem(item + items, items))
        far = item_slot(safe // others + flip, lax.rem(safe, others))
        near = z * 2 + lax.rem(y + index + flip, 2)
        late = (index + shards - 2) // shards
        return near + late * (far - near)

    def near_copy(phase, block, side):
        return push(
            give.at[block, side], got_near.at[block, side], n_sent.at[phase], n_land.at[block, side], core_peer
        )

    def far_copy(phase, block):
        return push(stage.at[block], got_far.at[block], f_sent.at[phase], f_land.at[block], y_peer)

    def out_copy(block):
        cols = pl.ds(aligned(block * piece_cols, LANES), piece_cols)
        return pltpu.make_async_copy(total.at[block], out_total.at[:, cols], out_sem.at[block])

    def project(phase, w, lhs, lag, before, after):
        depth_rows = gives[w].shape[0]

        def combine(index):
            block = block_of(index)
            near_copy(phase, block, 1).wait_recv()
            stage[block] = (keep[block] + got_near[block, 1].astype(F32)).astype(BF16)
            far_copy(phase, block).start()
            near_copy(phase, block, 0).wait_recv()
            total[block] += got_near[block, 0].astype(F32)

        def body(index, carry):
            if phase == 1:
                when(index > 0, lambda: combine(index - 1))
            before(index)
            block = block_of(index)
            weight = fulls[w][pl.ds(aligned(block * depth_rows, 64), depth_rows), :]
            for side, held in ((1, keep), (0, total)):
                left = lhs[pl.ds(aligned(side * seq + (1 - core) * share, 64), share), :]
                give[block, side] = jnp.dot(left, weight, preferred_element_type=F32).astype(BF16)
                left = lhs[pl.ds(aligned(side * seq + core * share, 64), share), :]
                held[block] = jnp.dot(left, weight, preferred_element_type=F32)
                near_copy(phase, block, side).start()
            if phase == 0:
                when(index > 0, lambda: combine(index - 1))
            if lag < shards:
                when(index >= lag, lambda: add_far(phase, index - lag))
            after(index)
            return carry

        lax.fori_loop(0, shards, body, 0)
        combine(shards - 1)

    def add_far(phase, index):
        block = block_of(index, 1)
        far_copy(phase, block).wait_recv()
        value = total[block] + got_far[block].astype(F32)
        total[block] = value
        if phase == 1:
            lane_squares[...] += sum(
                jnp.square(value[:, at : at + LANES]) for at in range(0, piece_cols, LANES)
            )
            out_copy(block).start()

    def collect(phase, lag, between):
        def body(index, carry):
            add_far(phase, index)
            between(index)
            return carry

        lax.fori_loop(shards - lag, shards, body, 0)

        push(stage, stage, f_sent.at[phase], f_land.at[0], y_peer).wait_send()
        push(give, give, n_sent.at[phase], n_land.at[0, 0], core_peer).wait_send()

    def during_project(index):
        when(is_inner & (index == 6), lambda: serve(2, 2))
        when(is_end & (index == 0), lambda: start_z(3, 0))
        when(is_end & (lax.rem(index, 2) == 1), lambda: serve(2, 3, (index // 2,)))

    def last_up():
        serve(2, 5)
        start_z(3, 0)

    def during_sum(index):
        when(is_inner & (index == 1), lambda: serve(2, 3))
        when(is_inner & (index == 2), lambda: serve(2, 4))
        when(is_inner & (index == 5), last_up)
        when(is_end & (index == 0), lambda: start_other(3))
        when(is_end & (index >= 1) & (index < 5), lambda: serve(2, 2, (index - 1,)))
        when(is_end & (index == 5), lambda: serve(2, 4, (0, 1)))
        when(is_end & (index >= 6), lambda: serve(2, 4, (index - 4,)))

    all_x_arrivals(1)
    project(0, 1, mixed, shards, during_project, lambda index: None)
    collect(0, shards, during_sum)

    def summed(start):
        values = [total[block, pl.ds(start, rows), :] for block in range(shards)]
        squares = sum(jnp.sum(value * value, axis=-1, keepdims=True) for value in values)
        return values, lax.rsqrt(squares * (1.0 / width) + EPSILON)

    pieces = m_land.shape[0]
    piece_rows = share // pieces

    def piece(ref, base, index):
        return ref.at[pl.ds(aligned(base + index * piece_rows, 16), piece_rows)]

    def to_far(index):
        return push(
            piece(mlp_in, core * share, index), piece(mlp_in, seq + core * share, index),
            m_sent, m_land.at[index], y_peer,
        )

    def to_near(index):
        block = piece(mlp_in, core * share, index)
        return push(block, block, mn_sent, mn_land, core_peer)

    def onward(index):
        block = piece(mlp_in, seq + core * share, index)
        return push(block, block, mf_sent, mf_land, core_peer)

    def entry_piece(index, carry):
        def entry_rows(inner_index, inner_carry):
            start = aligned(index * piece_rows + inner_index * rows, rows)
            values, factor = summed(start)
            place = aligned(core * share + start, rows)
            squares = jnp.zeros((rows, 1), F32)
            kept = []
            for block in range(shards):
                cols = pl.ds(block * piece_cols, piece_cols)
                value = tokens[pl.ds(place, rows), cols].astype(F32) + values[block] * factor * gain_rows[1:2, cols]
                value = value.astype(BF16)
                hidden[pl.ds(start, rows), cols] = value
                value = value.astype(F32)
                kept.append(value)
                squares += jnp.sum(value * value, axis=-1, keepdims=True)
            scale = lax.rsqrt(squares * (1.0 / width) + EPSILON)
            for block in range(shards):
                cols = pl.ds(block * piece_cols, piece_cols)
                mlp_in[pl.ds(place, rows), cols] = (kept[block] * scale * gain_rows[2:3, cols]).astype(BF16)
            return inner_carry

        lax.fori_loop(0, piece_rows // rows, entry_rows, 0)
        to_far(index).start()
        to_near(index).start()
        return carry

    when(is_end, lambda: serve(2, 5, (0,)))
    lax.fori_loop(0, pieces, entry_piece, 0)
    hidden_out = pltpu.make_async_copy(hidden, out_hidden, out_sem.at[shards + 2])
    hidden_out.start()
    lane_squares[...] = jnp.zeros_like(lane_squares)
    when(is_end, lambda: serve(2, 5, range(1, CUTS[2])))
    serve(3, 0)

    @pl.when(is_inner)
    def _():
        serve(3, 1)
        start_other(3)
        serve(3, 2)

    all_x_arrivals(2)

    peer_rows = mlp_in.at[pl.ds(0, share)]
    push(peer_rows, peer_rows, mn_sent, mn_land, core_peer).wait_recv()
    up_tiles = units // PIECE

    def up_rows(base, item):
        def body(index, carry):
            col = aligned(index * PIECE, PIECE)
            value = jnp.dot(mlp_in[pl.ds(base, seq), :], u_full[:, pl.ds(col, PIECE)], preferred_element_type=F32)
            value = jnp.maximum(value * up_scale[:, pl.ds(aligned(y * units + col, PIECE), PIECE)], 0.0)
            active[pl.ds(base, seq), pl.ds(col, PIECE)] = (value * value).astype(BF16)
            when(is_end & (index == 2), lambda: serve(3, item, (item - 1,)))
            return carry

        lax.fori_loop(0, up_tiles, body, 0)

    up_rows(0, 1)
    when(is_end, lambda: serve(3, 1, range(1, CUTS[3])))

    def pass_on(index, carry):
        to_far(index).wait_recv()
        onward(index).start()
        return carry

    lax.fori_loop(0, pieces, pass_on, 0)
    when(is_end, lambda: serve(3, 3, (0, 1)))

    @pl.when(is_inner)
    def _():
        serve(3, 3)
        serve(3, 4)

    push(peer_rows, peer_rows, mf_sent, mf_land, core_peer).wait_recv()
    up_rows(seq, 3)

    def before_down(index):
        when(is_inner & (index == 0), lambda: serve(3, 5))
        when(index >= 2, lambda: x_arrival(3, arrival(index - 2)))

    def after_down(index):
        when(is_end & (index < 2), lambda: serve(3, arrival(3), (index,)))
        when(is_end & (index == 2), lambda: serve(3, arrival(3), range(2, CUTS[3])))
        when(is_end & (index > 2) & (index < items - 2), lambda: serve(3, arrival(index + 1)))
        when(is_end & (index == items - 1), lambda: serve(3, items - 1, (0, 1)))
        when(is_end & (index == items), lambda: serve(3, items - 1, range(2, CUTS[3])))

    when(is_end, lambda: serve(3, 3, range(3, CUTS[3])))
    lag = far_lag(shards)
    project(1, 3, active, lag, before_down, after_down)
    collect(1, lag, lambda index: None)

    squares = jnp.sum(lane_squares[...], axis=-1, keepdims=True)
    lane_squares[...] = jnp.broadcast_to(lax.rsqrt(squares * (1.0 / width) + EPSILON), lane_squares.shape)
    factor_copy = pltpu.make_async_copy(lane_squares, out_factor, out_sem.at[shards])
    factor_copy.start()

    for w in range(WEIGHTS):
        y_copy(w).wait_send()
        sent = fulls[w].at[pl.ds(0, others * gives[w].shape[0])]
        own = fulls[w].at[pl.ds(0, gives[w].shape[0])]
        push(sent, sent, x_sent.at[w], x_land.at[w], x_peer).wait_send()
        push(own, own, z_sent.at[w, 0], x_land.at[w], x_peer).wait_send()

        @pl.when(inner == 1)
        def _():
            push(own, own, z_sent.at[w, 1], x_land.at[w], x_peer).wait_send()
            push(sent, sent, zf_sent.at[w], x_land.at[w], x_peer).wait_send()

    t_near.wait_send()
    t_pass.wait_send()
    push(most, most, g_sent, g_land, y_peer).wait_send()

    block = mlp_in.at[pl.ds(0, share)]
    for sent in (m_sent, mn_sent, mf_sent):
        push(block, block, sent, m_land.at[0], y_peer).wait_send()

    def drain(index, carry):
        out_copy(index).wait()
        return carry

    lax.fori_loop(0, shards, drain, 0)
    gain_out.wait()
    hidden_out.wait()
    factor_copy.wait()


def finish_kernel(total, factor, hidden, gain, out, total_in, factor_in, hidden_in, gain_in, result, row_sem, sem, out_sem):
    pieces = out_sem.shape[0]
    size = total.shape[0] // pieces
    near = [pltpu.make_async_copy(factor, factor_in, row_sem.at[0]), pltpu.make_async_copy(gain, gain_in, row_sem.at[1])]
    loads, stores = [], []
    for index in range(pieces):
        block = pl.ds(index * size, size)
        loads.append([
            pltpu.make_async_copy(total.at[block], total_in.at[block], sem.at[0, index]),
            pltpu.make_async_copy(hidden.at[block], hidden_in.at[block], sem.at[1, index]),
        ])
        stores.append(pltpu.make_async_copy(result.at[block], out.at[block], out_sem.at[index]))
    for copy in near + sum(loads, []):
        copy.start()
    for copy in near:
        copy.wait()
    for index in range(pieces):
        block = pl.ds(index * size, size)
        for copy in loads[index]:
            copy.wait()
        scaled = total_in[block, :] * factor_in[block, :1] * gain_in[...]
        result[block, :] = (hidden_in[block, :].astype(F32) + scaled).astype(BF16)
        stores[index].start()
    for copy in stores:
        copy.wait()


def on_device_paired(
    tokens, gain_mix_pre, gain_mix_post, gain_mlp_pre, gain_mlp_post,
    x_weight, gate_weight, x_scale, gate_scale, conv_weight, recur_map, input_map,
    decay_param, out_weight, out_scale, up_weight, up_scale, down_weight, down_scale,
):
    shards = lax.axis_size("fs")
    seq, width = tokens.shape[1:]
    share, lines, pieces = seq // 2, shards // 2, 4
    fan_in, channels, units = x_weight.shape[0], x_weight.shape[1] // 2, up_weight.shape[1] // 2
    piece_cols = width // shards
    dma = pltpu.SemaphoreType.DMA
    anywhere = pl.BlockSpec(memory_space=pl.ANY)
    part_shapes = ((fan_in, 2 * channels), (channels, piece_cols), (fan_in, units), (units, piece_cols))
    raws = (x_weight, gate_weight, out_weight, up_weight, down_weight)
    rows = [
        value[None] for value in (
            gain_mix_pre, gain_mix_post, gain_mlp_pre, gain_mlp_post, out_scale, down_scale,
            x_scale, gate_scale, up_scale,
        )
    ]
    inputs = (tokens[0], *rows, conv_weight, recur_map.T, input_map.T, decay_param[None])
    total, factor, hidden, gain = pl.pallas_call(
        functools.partial(layer_kernel, shards),
        out_shape=(
            jax.ShapeDtypeStruct((share, width), F32),
            jax.ShapeDtypeStruct((share, LANES), F32),
            jax.ShapeDtypeStruct((share, width), BF16),
            jax.ShapeDtypeStruct((1, width), F32),
        ),
        in_specs=[anywhere] * (len(inputs) + len(raws)),
        out_specs=(anywhere,) * 4,
        scratch_shapes=[pltpu.VMEM(value.shape, value.dtype) for value in inputs]
        + [dma((len(inputs),))]
        + [pltpu.VMEM((shards * shape[0], shape[1]), BF16) for shape in part_shapes]
        + [pltpu.VMEM(shape, BF16) for shape in part_shapes]
        + [pltpu.VMEM(raw.shape, F32) for raw in raws]
        + [
            pltpu.VMEM((shards, 4, piece_cols), F32),
            pltpu.VMEM((4, width), F32),
            pltpu.VMEM((1, 2 * channels), F32),
            pltpu.VMEM((2 * channels, LANES), BF16),
            pltpu.VMEM((1, channels), F32),
            pltpu.VMEM((seq, width), BF16),
            pltpu.VMEM((2 * seq, width), BF16),
            pltpu.VMEM((2 * seq, 2 * channels), BF16),
            pltpu.VMEM((2 * seq, channels), BF16),
            pltpu.VMEM((2 * seq, width), BF16),
            pltpu.VMEM((2 * seq, units), BF16),
            pltpu.VMEM((share, width), BF16),
            pltpu.VMEM((share, LANES), F32),
            pltpu.VMEM((shards, 2, share, piece_cols), BF16),
            pltpu.VMEM((shards, 2, share, piece_cols), BF16),
            pltpu.VMEM((shards, share, piece_cols), F32),
            pltpu.VMEM((shards, share, piece_cols), F32),
            pltpu.VMEM((shards, share, piece_cols), BF16),
            pltpu.VMEM((shards, share, piece_cols), BF16),
            dma((len(raws),)), dma((WEIGHTS,)), dma((WEIGHTS,)),
            dma((WEIGHTS, 2)), *[dma((shards, cuts)) for cuts in CUTS], dma((WEIGHTS,)),
            dma((WEIGHTS,)), dma((WEIGHTS - 1 + shards,)),
            dma, dma,
            dma((2,)), dma((2,)),
            dma((2,)), dma((shards, 2)), dma((2,)), dma((shards,)),
            dma, dma((pieces,)), dma, dma, dma, dma, dma((shards + 3,)),
        ],
        compiler_params=pltpu.CompilerParams(
            collective_id=4, has_side_effects=True, vmem_limit_bytes=67_000_000
        ),
        cost_estimate=pl.CostEstimate(flops=20_000_000_000, bytes_accessed=80_000_000, transcendentals=0),
        name="layer",
    )(*inputs, *raws)
    finals = (total, factor, hidden, gain)
    return pl.pallas_call(
        finish_kernel,
        in_specs=[anywhere] * len(finals),
        out_specs=anywhere,
        out_shape=jax.ShapeDtypeStruct((share, width), BF16),
        scratch_shapes=[pltpu.VMEM(value.shape, value.dtype) for value in finals]
        + [pltpu.VMEM((share, width), BF16), dma((2,)), dma((2, pieces)), dma((pieces,))],
        name="finish",
    )(*finals)[None]


def solution(mesh):
    in_specs = (
        P(("rep", "fs"), None, None),
        P("fs"), P("fs"), P("fs"), P("fs"),
        P("fs", "tp"), P("fs", "tp"),
        P("tp"), P("tp"),
        P(None, "tp"), P("tp", None), P("tp", None), P("tp"),
        P("tp", "fs"), P("fs"),
        P("fs", "tp"), P("tp"),
        P("tp", "fs"), P("fs"),
    )
    out_specs = P(("rep", "fs"), "tp", None)
    paired = (
        mesh.shape["rep"] == 2 and mesh.shape["tp"] == 2
        and mesh.shape["fs"] % 4 == 0 and 4 < mesh.shape["fs"] < 16
    )
    return jax.shard_map(
        on_device_paired if paired else on_device, mesh=mesh, in_specs=in_specs, out_specs=out_specs, check_vma=False
    )
```
